32 devices in a mesh: fs: 4 (over z), rep: 4 (over y, x), tp: 2 (over core).
Axes of the slice: x: 2, y: 2, z: 4, core: 2. Of those that a mesh axis runs over, the one named last changes fastest.
Arguments:
- saved_inputs: bfloat16 [12288, 2048], P(('fs', 'rep')), may hold values from -6 to 6
- query_cotangent: bfloat16 [12288, 1024], P(('fs', 'rep'), 'tp'), may hold values from -0.053955078 to 0.053955078
- value_cotangent: bfloat16 [12288, 2048], P(('fs', 'rep'), 'tp'), may hold values from -0.053955078 to 0.053955078
- query_weight: float32 [2048, 1024], P('fs', 'tp'), may hold values from -0.125 to 0.125
- value_weight: float32 [2048, 2048], P('fs', 'tp'), may hold values from -0.125 to 0.125
- query_factor: bfloat16 [2048, 256], P('fs'), as said below
- value_factor: bfloat16 [2048, 256], P('fs'), as said below
- query_first: float32 [256, 1024], P('rep', 'tp'), may hold values from -6 to 6
- query_second: float32 [256, 1024], P('rep', 'tp'), may hold values from 0.3 to 3
- value_first: float32 [256, 2048], P('rep', 'tp'), may hold values from -6 to 6
- value_second: float32 [256, 2048], P('rep', 'tp'), may hold values from 0.3 to 3
Outputs:
- query_direction: float32 [2048, 1024], P('fs', 'tp')
- value_direction: float32 [2048, 2048], P('fs', 'tp')
- query_master: float32 [2048, 1024], P('fs', 'tp')
- value_master: float32 [2048, 2048], P('fs', 'tp')
- query_first_new: float32 [256, 1024], P('rep', 'tp')
- query_second_new: float32 [256, 1024], P('rep', 'tp')
- value_first_new: float32 [256, 2048], P('rep', 'tp')
- value_second_new: float32 [256, 2048], P('rep', 'tp')
- query_copy: bfloat16 [2048, 1024], P(None, 'tp')
- value_copy: bfloat16 [2048, 2048], P(None, 'tp')
The draws below stay inside these ranges and needn't reach their ends.
Inputs may be any that keep to these rules, and one draw needn't show every extreme that they name: `query_factor`: A matrix of full rank. `value_factor`: A matrix of full rank.
All inputs are finite; a program needn't handle non-finite values.
Results may differ from the reference program's by a relative error of at most 0.012.
Values may be sent and summed in bfloat16 or wider, within the bound.
A program may use at most 128 MiB of HBM per device.

```python
import math
import jax
import jax.numpy as jnp
from jax import lax

D = 2048
QK = 1024
VW = 2048
RANK = 256
TOKENS = 12288


def factor_draw(key):
    first_key, second_key = jax.random.split(key)
    positions = jnp.arange(D, dtype=jnp.float32)
    trend = jnp.exp(math.log(3.0) * positions / D)
    spread = jnp.exp(jax.random.uniform(first_key, (D, 1), jnp.float32, 0.0, math.log(10.0)))
    base = jax.random.normal(second_key, (D, RANK), jnp.float32)
    return (base * spread * trend[:, None] * (0.3 / math.sqrt(D))).astype(jnp.bfloat16)


def draw_query_factor(key, part):
    return factor_draw(jax.random.fold_in(key, 11))


def draw_value_factor(key, part):
    return factor_draw(jax.random.fold_in(key, 23))


def block_levels(stream_key, extent, pieces, least, top_value):
    def one(dim, parts):
        heights = jax.random.uniform(jax.random.fold_in(jax.random.fold_in(stream_key, 6), dim), (parts,), jnp.float32, least / len(pieces), top_value / len(pieces))
        return jnp.repeat(jnp.exp(heights), extent[dim] // parts).reshape((-1,) + (1,) * (len(extent) - dim - 1))

    factor_of = one(*pieces[0])
    for cut in pieces[1:]:
        factor_of = factor_of * one(*cut)
    return factor_of


def normal_values(key, extent, scale, bound, pieces=(), held_as=jnp.bfloat16):
    array = scale * jax.random.normal(key, extent, jnp.float32)
    if pieces:
        array = array * block_levels(key, extent, pieces, -0.22, 0.18)
    return jnp.clip(array, -bound, bound).astype(held_as)


def setup_inputs(seed: int = 0) -> dict:
    keys = jax.random.split(jax.random.key(seed), 12)
    return {
        "saved_inputs": normal_values(keys[0], (TOKENS, D), 1.0, 6.0, ((0, 16),)),
        "query_cotangent": normal_values(keys[1], (TOKENS, QK), (TOKENS ** -0.5), 0.053955078, ((0, 16), (1, 2))),
        "value_cotangent": normal_values(keys[2], (TOKENS, VW), (TOKENS ** -0.5), 0.053955078, ((0, 16), (1, 2))),
        "query_weight": normal_values(keys[3], (D, QK), D ** -0.5, 0.125, ((0, 4), (1, 2)), jnp.float32),
        "value_weight": normal_values(keys[4], (D, VW), D ** -0.5, 0.125, ((0, 4), (1, 2)), jnp.float32),
        "query_factor": draw_query_factor(jax.random.fold_in(keys[11], 71), 0),
        "value_factor": draw_value_factor(jax.random.fold_in(keys[11], 71), 0),
        "query_first": normal_values(keys[7], (RANK, QK), 1.0, 6.0, ((0, 4), (1, 2)), jnp.float32),
        "query_second": jnp.clip(jnp.exp(math.log(3.0) - 2.3025851 * jax.random.uniform(keys[8], (RANK, QK), jnp.float32) ** block_levels(keys[8], (RANK, QK), ((0, 4), (1, 2)), -0.2, 0.2)), 0.3, 3.0),
        "value_first": normal_values(keys[9], (RANK, VW), 1.0, 6.0, ((0, 4), (1, 2)), jnp.float32),
        "value_second": jnp.clip(jnp.exp(math.log(3.0) - 2.3025851 * jax.random.uniform(keys[10], (RANK, VW), jnp.float32) ** block_levels(keys[10], (RANK, VW), ((0, 4), (1, 2)), -0.2, 0.2)), 0.3, 3.0),
    }


BETA_ONE = 0.8
BETA_TWO = 0.9
EPS_RATIO = 1e-08
EPS_NORM = 1e-06
RATE = 0.02

def update_one(grad, factor, weight, first, second):
    wide = factor.astype(jnp.float32)
    projected = jnp.dot(wide.T, grad, precision=lax.Precision.HIGHEST)
    first_new = BETA_ONE * first + (1.0 - BETA_ONE) * projected
    second_new = BETA_TWO * second + (1.0 - BETA_TWO) * projected * projected
    ratio = first_new / (jnp.sqrt(second_new) + EPS_RATIO)
    raw_step = jnp.dot(wide, ratio, precision=lax.Precision.HIGHEST)
    direction = raw_step * lax.rsqrt(jnp.mean(raw_step * raw_step) + EPS_NORM)
    master = weight - RATE * direction
    return (direction, master, first_new, second_new, master.astype(jnp.bfloat16))

def reference(saved_inputs, query_cotangent, value_cotangent, query_weight, value_weight, query_factor, value_factor, query_first, query_second, value_first, value_second):
    dims = (((0,), (0,)), ((), ()))
    query_grad = lax.dot_general(saved_inputs, query_cotangent, dims, preferred_element_type=jnp.float32)
    value_grad = lax.dot_general(saved_inputs, value_cotangent, dims, preferred_element_type=jnp.float32)
    q_dir, q_master, q_first, q_second, q_copy = update_one(query_grad, query_factor, query_weight, query_first, query_second)
    v_dir, v_master, v_first, v_second, v_copy = update_one(value_grad, value_factor, value_weight, value_first, value_second)
    return (q_dir, v_dir, q_master, v_master, q_first, q_second, v_first, v_second, q_copy, v_copy)
```

```python
import functools

import jax
import jax.numpy as jnp
from jax import lax
from jax.experimental import pallas as pl
from jax.experimental.pallas import tpu as pltpu
from jax.sharding import PartitionSpec as P

BETA_ONE = 0.8
BETA_TWO = 0.9
EPS_RATIO = 1e-08
EPS_NORM = 1e-06
RATE = 0.02
BF = jnp.bfloat16
F32 = jnp.float32


def moments(projected, first, second):
    first_new = BETA_ONE * first + (1.0 - BETA_ONE) * projected
    second_new = BETA_TWO * second + (1.0 - BETA_TWO) * projected * projected
    ratio = first_new / (jnp.sqrt(second_new) + EPS_RATIO)
    return (first_new, second_new, ratio)


def exchange(
    nz,
    nr,
    x_hbm,
    cq_hbm,
    cv_hbm,
    wq_hbm,
    wv_hbm,
    qf_hbm,
    vf_hbm,
    q1_hbm,
    q2_hbm,
    v1_hbm,
    v2_hbm,
    w_out,
    f_ref,
    ratio_ref,
    proj_out,
    scale_out,
    x_ref,
    cq_ref,
    cv_ref,
    wf_ref,
    wb_ref,
    low_ref,
    part_ref,
    rs_ref,
    z_ref,
    zg_ref,
    zh_ref,
    m1_ref,
    m2_ref,
    sq_ref,
    local_sem,
    f1_s,
    f1_r,
    w1_s,
    w1_r,
    f2_s,
    f2_r,
    w2_s,
    w2_r,
    rs_s,
    rs_r,
    zs_s,
    zs_r,
    zg_s,
    zg_r,
    ag_s,
    ag_r,
    tp_s,
    tp_r,
):
    z = lax.axis_index("fs")
    r = lax.axis_index("rep")
    t = lax.axis_index("tp")
    rows = qf_hbm.shape[0]
    part = rows // nr
    qc = cq_ref.shape[1]
    cols = w_out.shape[1]
    half = cols // 2
    width = w_out.shape[0]
    rank = low_ref.shape[2]
    own = rank // nr
    tokens = x_ref.shape[0]
    z_of = [lax.rem(z + k, nz) for k in range(nz)]
    z_from = [lax.rem(z + nz - k, nz) for k in range(nz)]
    r_of = [lax.rem(r + j, nr) for j in range(nr)]
    side = r + 1 - 2 * lax.rem(r, 2)
    over = lax.rem(r + 2, nr)
    corner = nr - 1 - r
    other = 1 - t

    def remote(src, dst, ss, rs, dev):
        return pltpu.make_async_remote_copy(
            src_ref=src,
            dst_ref=dst,
            send_sem=ss,
            recv_sem=rs,
            device_id=dev,
            device_id_type=pl.DeviceIdType.MESH,
        )

    def slab(zz, rr):
        return pl.ds(pl.multiple_of(zz * rows + rr * part, part), part)

    def fac_copy(src):
        return pltpu.make_async_copy(
            src,
            f_ref.at[t, pl.ds(pl.multiple_of(z * rows, rows), rows)],
            local_sem.at[0],
        )

    @pl.when(t == 0)
    def _():
        fac_copy(qf_hbm).start()

    @pl.when(t == 1)
    def _():
        fac_copy(vf_hbm).start()

    wq_in = pltpu.make_async_copy(wq_hbm, wf_ref.at[:, pl.ds(0, qc)], local_sem.at[1])
    wv_in = pltpu.make_async_copy(wv_hbm, wf_ref.at[:, pl.ds(qc, cols - qc)], local_sem.at[2])
    x_in = pltpu.make_async_copy(x_hbm, x_ref, local_sem.at[3])
    cq_in = pltpu.make_async_copy(cq_hbm, cq_ref, local_sem.at[4])
    cv_in = pltpu.make_async_copy(cv_hbm, cv_ref, local_sem.at[5])
    left, right = pl.ds(0, qc), pl.ds(qc, cols - qc)
    mom = [
        pltpu.make_async_copy(src, dst.at[:, at], local_sem.at[7 + n])
        for n, (src, dst, at) in enumerate(
            (
                (q1_hbm, m1_ref, left),
                (v1_hbm, m1_ref, right),
                (q2_hbm, m2_ref, left),
                (v2_hbm, m2_ref, right),
            )
        )
    ]
    for c in [wq_in, wv_in, x_in, cq_in, cv_in] + mom:
        c.start()

    barrier = pltpu.get_barrier_semaphore()
    peers = [(z_of[k], r, t) for k in range(1, nz)]
    peers += [(z, r_of[j], t) for j in range(1, nr)]
    peers += [(z, r, other)]
    for dev in peers:
        pl.semaphore_signal(
            barrier, inc=1, device_id=dev, device_id_type=pl.DeviceIdType.MESH
        )
    pl.semaphore_wait(barrier, len(peers))

    fac_copy(qf_hbm).wait()
    sends = []
    f1 = []
    for k in range(1, nz):
        here = f_ref.at[t, slab(z, r)]
        c = remote(here, here, f1_s.at[k - 1], f1_r.at[k - 1], (z_of[k], r, t))
        c.start()
        f1.append(c)
    wq_in.wait()
    wv_in.wait()
    wb_ref[...] = wf_ref[...].astype(BF)
    order = sorted(range(1, nz), key=lambda k: min(k, nz - k))
    w1 = {}
    for k in order:
        c = remote(
            wb_ref.at[pl.ds(pl.multiple_of(r * part, part), part)],
            w_out.at[slab(z, r)],
            w1_s.at[k - 1],
            w1_r.at[k - 1],
            (z_of[k], r, t),
        )
        c.start()
        w1[k] = c
    w_own = pltpu.make_async_copy(
        wb_ref, w_out.at[pl.ds(pl.multiple_of(z * rows, rows), rows)], local_sem.at[6]
    )
    w_own.start()

    f2 = []
    for k in range(1, nz):
        f1[k - 1].wait_recv()
        there = f_ref.at[t, slab(z_from[k], r)]
        for j in range(1, nr):
            n = (k - 1) * (nr - 1) + j - 1
            c = remote(there, there, f2_s.at[n], f2_r.at[n], (z, r_of[j], t))
            c.start()
            f2.append(c)
    for c in f2:
        c.wait_recv()
    w2 = {}

    def spread(k):
        w1[k].wait_recv()
        there = w_out.at[slab(z_from[k], r)]
        for n, dev in ((0, side), (1, over)):
            c = remote(there, there, w2_s.at[k - 1, n], w2_r.at[k - 1, n], (z, dev, t))
            c.start()
            w2[k, n] = c

    def relay(k):
        for n, src, dev, at in ((0, side, over, 0), (1, over, side, half)):
            w2[k, n].wait_recv()
            there = w_out.at[slab(z_from[k], src), pl.ds(at, half)]
            c = remote(
                there, there, w2_s.at[k - 1, 2 + n], w2_r.at[k - 1, 2 + n], (z, dev, t)
            )
            c.start()
            w2[k, 2 + n] = c

    stages = [[], [], []]
    for n, k in enumerate(order):
        stages[min(n, 2)].append(k)
    x_in.wait()
    tile = tokens // 3

    @pl.loop(0, 3)
    def _(i):
        span = pl.ds(pl.multiple_of(i * tile, tile), tile)
        low_ref[t, span] = jnp.dot(
            x_ref[span, :], f_ref[t], preferred_element_type=F32
        ).astype(BF)

    lx = remote(low_ref.at[t], low_ref.at[t], tp_s.at[1], tp_r.at[1], (z, r, other))
    lx.start()
    fx = remote(f_ref.at[t], f_ref.at[t], tp_s.at[0], tp_r.at[0], (z, r, other))
    fx.start()
    for k in stages[0]:
        spread(k)
    cq_in.wait()
    cv_in.wait()
    lx.wait_recv()
    dims = (((0,), (0,)), ((), ()))
    part_ref[:, :qc] = lax.dot_general(
        low_ref[0], cq_ref[...], dims, preferred_element_type=F32
    ).astype(BF)
    part_ref[:, qc:] = lax.dot_general(
        low_ref[1], cv_ref[...], dims, preferred_element_type=F32
    ).astype(BF)

    def low_rows(rr):
        return pl.ds(pl.multiple_of(rr * own, own), own)

    rsc = []
    for j in range(1, nr):
        c = remote(
            part_ref.at[low_rows(r_of[j])],
            rs_ref.at[j - 1],
            rs_s.at[j - 1],
            rs_r.at[j - 1],
            (z, r_of[j], t),
        )
        c.start()
        rsc.append(c)

    for k in stages[0]:
        relay(k)
    for c in rsc:
        c.wait_recv()
    total = part_ref[low_rows(r), :].astype(F32)
    for j in range(1, nr):
        total = total + rs_ref[j - 1].astype(F32)
    share = own // nz
    scatter = share % 16 == 0
    zc = []
    if scatter:
        zg_ref[...] = total.astype(BF)
    else:
        z_ref[z] = total.astype(BF)

    def z_rows(zz):
        return pl.ds(pl.multiple_of(zz * share, share), share)

    for k in range(1, nz):
        src = zg_ref.at[z_rows(z_of[k])] if scatter else z_ref.at[z]
        c = remote(src, z_ref.at[z], zs_s.at[k - 1], zs_r.at[k - 1], (z_of[k], r, t))
        c.start()
        zc.append(c)
    if scatter:
        z_ref[z] = zg_ref[z_rows(z), :]
    for k in stages[1]:
        spread(k)
    for c in zc:
        c.wait_recv()
    proj = z_ref[0].astype(F32)
    for k in range(1, nz):
        proj = proj + z_ref[k].astype(F32)
    gc = []
    if scatter:
        for c in zc:
            c.wait_send()
        zh = zh_ref
        zh[z_rows(z), :] = proj.astype(BF)
        for k in range(1, nz):
            here = zh.at[z_rows(z)]
            c = remote(here, here, zg_s.at[k - 1], zg_r.at[k - 1], (z_of[k], r, t))
            c.start()
            gc.append(c)
    for k in stages[1]:
        relay(k)
    for k in stages[2]:
        spread(k)
    for c in mom:
        c.wait()
    if scatter:
        for c in gc:
            c.wait_recv()
        proj = zh[...].astype(F32)
    proj_out[...] = proj
    _, _, ratio = moments(proj, m1_ref[...], m2_ref[...])
    ratio_ref[low_rows(r), :] = ratio.astype(BF)
    agc = []
    for j in range(1, nr):
        here = ratio_ref.at[low_rows(r)]
        c = remote(here, here, ag_s.at[j - 1], ag_r.at[j - 1], (z, r_of[j], t))
        c.start()
        agc.append(c)
    for k in stages[2]:
        relay(k)
    fx.wait_recv()
    for c in agc:
        c.wait_recv()
    step = min(256, width)

    def squares(i, acc):
        span = pl.ds(pl.multiple_of(i * step, step), step)
        a = jnp.dot(f_ref[0, span], ratio_ref[:, :qc], preferred_element_type=F32)
        b = jnp.dot(f_ref[1, span], ratio_ref[:, qc:], preferred_element_type=F32)
        a = jnp.sum(a * a, axis=0, keepdims=True)
        b = jnp.sum(b * b, axis=0, keepdims=True)
        return (acc[0] + a, acc[1] + b)

    qs, vs = lax.fori_loop(
        0,
        width // step,
        squares,
        (jnp.zeros((1, qc), F32), jnp.zeros((1, cols - qc), F32)),
    )
    qs = jnp.sum(qs, axis=1, keepdims=True)
    vs = jnp.sum(vs, axis=1, keepdims=True)
    row = lax.broadcasted_iota(jnp.int32, sq_ref.shape[1:], 0)
    sq_ref[t] = jnp.where(row == 0, qs / (width * qc * 2), vs / (width * (cols - qc) * 2))
    sx = remote(sq_ref.at[t], sq_ref.at[t], tp_s.at[2], tp_r.at[2], (z, r, other))
    sx.start()
    sx.wait_recv()
    scale_out[...] = lax.rsqrt(sq_ref[0] + sq_ref[1] + EPS_NORM)
    for k in range(1, nz):
        w2[k, 2].wait_recv()
        w2[k, 3].wait_recv()
    for c in f1 + list(w1.values()) + f2 + rsc + ([] if scatter else zc) + gc + agc + [fx, lx, sx] + list(w2.values()):
        c.wait_send()
    w_own.wait()


def run_exchange(nz, nr, x, cq, cv, wq, wv, qf, vf, q1, q2, v1, v2):
    tokens, width = x.shape
    qc = cq.shape[1]
    cols = qc + cv.shape[1]
    rows, rank = qf.shape
    own = rank // nr
    share = own // nz if (own // nz) % 16 == 0 else own
    any_spec = pl.BlockSpec(memory_space=pltpu.HBM)
    vmem = pl.BlockSpec(memory_space=pltpu.VMEM)
    dma = pltpu.SemaphoreType.DMA
    shape = jax.ShapeDtypeStruct
    return pl.pallas_call(
        functools.partial(exchange, nz, nr),
        out_shape=(
            shape((width, cols), BF),
            shape((2, width, rank), BF),
            shape((rank, cols), BF),
            shape((own, cols), F32),
            shape((8, 128), F32),
        ),
        in_specs=[any_spec] * 11,
        out_specs=(any_spec, vmem, vmem, vmem, vmem),
        scratch_shapes=[
            pltpu.VMEM((tokens, width), BF),
            pltpu.VMEM(cq.shape, BF),
            pltpu.VMEM(cv.shape, BF),
            pltpu.VMEM((rows, cols), F32),
            pltpu.VMEM((rows, cols), BF),
            pltpu.VMEM((2, tokens, rank), BF),
            pltpu.VMEM((rank, cols), BF),
            pltpu.VMEM((nr - 1, own, cols), BF),
            pltpu.VMEM((nz, share, cols), BF),
            pltpu.VMEM((own, cols), BF),
            pltpu.VMEM((own, cols), BF),
            pltpu.VMEM((own, cols), F32),
            pltpu.VMEM((own, cols), F32),
            pltpu.VMEM((2, 8, 128), F32),
            dma((11,)),
            dma((nz - 1,)),
            dma((nz - 1,)),
            dma((nz - 1,)),
            dma((nz - 1,)),
            dma(((nz - 1) * (nr - 1),)),
            dma(((nz - 1) * (nr - 1),)),
            dma((nz - 1, 4)),
            dma((nz - 1, 4)),
            dma((nr - 1,)),
            dma((nr - 1,)),
            dma((nz - 1,)),
            dma((nz - 1,)),
            dma((nz - 1,)),
            dma((nz - 1,)),
            dma((nr - 1,)),
            dma((nr - 1,)),
            dma((3,)),
            dma((3,)),
        ],
        compiler_params=pltpu.CompilerParams(
            collective_id=0, has_side_effects=True, vmem_limit_bytes=60 * 1024 * 1024
        ),
    )(x, cq, cv, wq, wv, qf, vf, q1, q2, v1, v2)


def finish(
    f_ref,
    ratio_ref,
    scale_ref,
    w_ref,
    wq_ref,
    wv_ref,
    qf_ref,
    vf_ref,
    proj_ref,
    q1_ref,
    q2_ref,
    v1_ref,
    v2_ref,
    qd_out,
    vd_out,
    qm_out,
    vm_out,
    q1_out,
    q2_out,
    v1_out,
    v2_out,
    qcopy_out,
    vcopy_out,
):
    qc = wq_ref.shape[1]
    sets = (
        (0, pl.ds(0, qc), wq_ref, qf_ref, q1_ref, q2_ref, qd_out, qm_out, q1_out, q2_out, qcopy_out),
        (
            1,
            pl.ds(qc, wv_ref.shape[1]),
            wv_ref,
            vf_ref,
            v1_ref,
            v2_ref,
            vd_out,
            vm_out,
            v1_out,
            v2_out,
            vcopy_out,
        ),
    )
    for n, at, w, f, m1, m2, d_out, m_out, m1_out, m2_out, c_out in sets:
        scale = scale_ref[n : n + 1, 0:1]
        ratio = ratio_ref[:, at]
        raw = jnp.dot(f_ref[n], ratio, preferred_element_type=F32)
        c_out[...] = (w_ref[:, at].astype(F32) - RATE * (raw * scale)).astype(BF)
        d = jnp.dot(f[...], ratio, preferred_element_type=F32) * scale
        d_out[...] = d
        m_out[...] = w[...] - RATE * d
        m1_out[...], m2_out[...], _ = moments(proj_ref[:, at], m1[...], m2[...])


def run_finish(factors, ratio, scale, weights, wq, wv, qf, vf, proj, q1, q2, v1, v2):
    rows, qc = wq.shape
    vc = wv.shape[1]
    width, cols = weights.shape
    rank, own = qf.shape[1], q1.shape[0]
    steps = 8 if rows % 128 == 0 else 4

    def tall(n, c):
        return pl.BlockSpec((n // steps, c), lambda i: (i, 0))

    def whole(a):
        return pl.BlockSpec(a.shape, lambda i: (0,) * a.ndim)

    shape = jax.ShapeDtypeStruct
    return pl.pallas_call(
        finish,
        grid=(steps,),
        in_specs=[
            pl.BlockSpec((2, width // steps, rank), lambda i: (0, i, 0)),
            whole(ratio),
            whole(scale),
            tall(width, cols),
            tall(rows, qc),
            tall(rows, vc),
            tall(rows, rank),
            tall(rows, rank),
            tall(own, cols),
            tall(own, qc),
            tall(own, qc),
            tall(own, vc),
            tall(own, vc),
        ],
        out_specs=[
            tall(rows, qc),
            tall(rows, vc),
            tall(rows, qc),
            tall(rows, vc),
            tall(own, qc),
            tall(own, qc),
            tall(own, vc),
            tall(own, vc),
            tall(width, qc),
            tall(width, vc),
        ],
        out_shape=[
            shape((rows, qc), F32),
            shape((rows, vc), F32),
            shape((rows, qc), F32),
            shape((rows, vc), F32),
            shape((own, qc), F32),
            shape((own, qc), F32),
            shape((own, vc), F32),
            shape((own, vc), F32),
            shape((width, qc), BF),
            shape((width, vc), BF),
        ],
        compiler_params=pltpu.CompilerParams(vmem_limit_bytes=60 * 1024 * 1024),
    )(factors, ratio, scale, weights, wq, wv, qf, vf, proj, q1, q2, v1, v2)


def line_exchange(
    quarter,
    chunks,
    x_hbm,
    cq_hbm,
    cv_hbm,
    wq_hbm,
    wv_hbm,
    qf_hbm,
    vf_hbm,
    q1_hbm,
    q2_hbm,
    v1_hbm,
    v2_hbm,
    w_ref,
    f_ref,
    ratio_ref,
    wf_ref,
    m1_out,
    m2_out,
    scale_out,
    x_ref,
    cq_ref,
    cv_ref,
    acc_ref,
    low_ref,
    part_ref,
    rs_ref,
    zs_ref,
    z_ref,
    zh_ref,
    m1_ref,
    m2_ref,
    g_ref,
    sq_ref,
    local_sem,
    fz_s,
    fz_r,
    fp_s,
    fp_r,
    wz_s,
    wz_r,
    wp_s,
    wp_r,
    rs_s,
    rs_r,
    zs_s,
    zs_r,
    zg_s,
    zg_r,
    ag_s,
    ag_r,
    tp_s,
    tp_r,
):
    z = lax.axis_index("fs")
    r = lax.axis_index("rep")
    t = lax.axis_index("tp")
    nz, nr = 4, 4
    rows = qf_hbm.shape[0]
    part = rows // nr
    qc = cq_ref.shape[1]
    width, cols = w_ref.shape
    half = cols // 2
    rank = low_ref.shape[2]
    own = rank // nr
    share = own // nz
    tokens = x_ref.shape[0]
    side = r + 1 - 2 * lax.rem(r, 2)
    over = lax.rem(r + 2, nr)
    corner = nr - 1 - r
    other = 1 - t
    peer = {1: side, 2: over, 3: corner}
    upper = lax.div(z, 2)
    near = z + 1 - 2 * lax.rem(z, 2)
    mid = 2 - upper
    far = 3 - 3 * upper
    planes = [near, mid, far]
    sent = []

    def remote(src, dst, ss, rs, dev):
        return pltpu.make_async_remote_copy(
            src_ref=src,
            dst_ref=dst,
            send_sem=ss,
            recv_sem=rs,
            device_id=dev,
            device_id_type=pl.DeviceIdType.MESH,
        )

    def send(src, dst, ss, rs, dev):
        c = remote(src, dst, ss, rs, dev)
        c.start()
        sent.append(c)
        return c

    def arrive(dst, rs):
        remote(dst, dst, tp_s.at[0], rs, (z, r, other)).wait_recv()

    def at(start, size, step):
        return pl.ds(pl.multiple_of(start, step), size)

    def fac_copy(src):
        return pltpu.make_async_copy(src, f_ref.at[t, at(z * rows, rows, rows)], local_sem.at[0])

    @pl.when(t == 0)
    def _():
        fac_copy(qf_hbm).start()

    @pl.when(t == 1)
    def _():
        fac_copy(vf_hbm).start()

    left, right = pl.ds(0, qc), pl.ds(qc, cols - qc)
    wq_in = pltpu.make_async_copy(wq_hbm, wf_ref.at[:, left], local_sem.at[1])
    wv_in = pltpu.make_async_copy(wv_hbm, wf_ref.at[:, right], local_sem.at[2])
    x_in = pltpu.make_async_copy(x_hbm, x_ref, local_sem.at[3])
    cq_in = pltpu.make_async_copy(cq_hbm, cq_ref, local_sem.at[4])
    cv_in = pltpu.make_async_copy(cv_hbm, cv_ref, local_sem.at[5])
    mom = [
        pltpu.make_async_copy(src, dst.at[:, span], local_sem.at[6 + n])
        for n, (src, dst, span) in enumerate(
            (
                (q1_hbm, m1_ref, left),
                (v1_hbm, m1_ref, right),
                (q2_hbm, m2_ref, left),
                (v2_hbm, m2_ref, right),
            )
        )
    ]
    for c in [wq_in, wv_in, x_in, cq_in, cv_in] + mom:
        c.start()

    barrier = pltpu.get_barrier_semaphore()
    peers = [(p, r, t) for p in planes]
    peers += [(z, peer[j], t) for j in peer]
    peers += [(z, r, other)]
    for dev in peers:
        pl.semaphore_signal(
            barrier, inc=1, device_id=dev, device_id_type=pl.DeviceIdType.MESH
        )
    pl.semaphore_wait(barrier, len(peers))

    def fac_rows(plane, rr):
        return f_ref.at[t, at(plane * rows + rr * part, part, part)]

    fac_copy(qf_hbm).wait()
    for i, p in enumerate(planes):
        here = fac_rows(z, r)
        send(here, here, fz_s.at[i], fz_r.at[z], (p, r, t))

    offsets = [sum(chunks[:c]) for c in range(len(chunks))]

    def w_rows(plane, rr, c):
        return w_ref.at[at(plane * rows + rr * quarter + offsets[c], chunks[c], 16)]

    def w_rest(plane):
        return w_ref.at[at(plane * rows + nr * quarter, rows - nr * quarter, 16)]

    wq_in.wait()
    wv_in.wait()
    w_ref[at(z * rows, rows, rows), :] = wf_ref[...].astype(BF)

    def w_line(i, c):
        here = w_rows(z, r, c)
        send(here, here, wz_s.at[i, c], wz_r.at[z, c], (planes[i], r, t))

    def w_line_rest(i):
        here = w_rest(z)
        n = len(chunks)
        send(here, here, wz_s.at[i, n], wz_r.at[z, n], (planes[i], r, t))

    for i in range(3):
        for c in range(len(chunks)):
            w_line(i, c)

    def spread(i, c):
        there = w_rows(planes[i], r, c)
        arrive(there, wz_r.at[planes[i], c])
        for n, dev in ((0, side), (1, over)):
            send(there, there, wp_s.at[i, c, n], wp_r.at[i, c, n], (z, dev, t))

    def relay(i, c):
        for n, src, dev, begin in ((0, side, over, 0), (1, over, side, half)):
            whole = w_rows(planes[i], src, c)
            arrive(whole, wp_r.at[i, c, n])
            there = whole.at[:, pl.ds(begin, half)]
            send(there, there, wp_s.at[i, c, 2 + n], wp_r.at[i, c, 2 + n], (z, dev, t))

    def low_add(plane, first):
        tile = tokens // 3

        @pl.loop(0, 3)
        def _(n):
            span = at(n * tile, tile, 16)
            a = jnp.dot(
                x_ref[span, at(plane * rows, rows, rows)],
                f_ref[t, at(plane * rows, rows, rows)],
                preferred_element_type=F32,
            )
            acc_ref[span, :] = a if first else acc_ref[span, :] + a

    def fac_spread(i):
        there = fac_rows(planes[i], r)
        arrive(there, fz_r.at[planes[i]])
        for j in (3, 1, 2):
            send(there, there, fp_s.at[i, j - 1], fp_r.at[i, j - 1], (z, peer[j], t))

    def fac_gather(i):
        for j in (1, 2, 3):
            arrive(fac_rows(planes[i], peer[j]), fp_r.at[i, j - 1])
        low_add(planes[i], False)

    x_in.wait()
    low_add(z, True)
    fac_spread(0)
    fac_spread(1)
    fac_spread(2)
    spread(0, 0)
    fac_gather(0)
    spread(0, 1)
    fac_gather(1)
    fac_gather(2)
    low_ref[t] = acc_ref[...].astype(BF)
    send(low_ref.at[t], low_ref.at[t], tp_s.at[1], tp_r.at[1], (z, r, other))
    fx = send(f_ref.at[t], f_ref.at[t], tp_s.at[0], tp_r.at[0], (z, r, other))
    cq_in.wait()
    cv_in.wait()
    arrive(low_ref.at[other], tp_r.at[1])
    dims = (((0,), (0,)), ((), ()))
    part_ref[:, :qc] = lax.dot_general(
        low_ref[0], cq_ref[...], dims, preferred_element_type=F32
    ).astype(BF)
    part_ref[:, qc:] = lax.dot_general(
        low_ref[1], cv_ref[...], dims, preferred_element_type=F32
    ).astype(BF)

    def low_rows(rr, plane):
        return at(rr * own + plane * share, share, share)

    def share_rows(plane):
        return at(plane * share, share, share)

    order = [far, mid, near, z]
    for i, p in enumerate(order):
        for j in (3, 1, 2):
            send(
                part_ref.at[low_rows(peer[j], p)],
                rs_ref.at[j - 1, share_rows(p)],
                rs_s.at[i, j - 1],
                rs_r.at[i, j - 1],
                (z, peer[j], t),
            )
    relay(0, 0)
    relay(0, 1)

    def collect(i, p):
        for j in (1, 2, 3):
            arrive(rs_ref.at[j - 1, share_rows(p)], rs_r.at[i, j - 1])
        total = part_ref[low_rows(r, p), :].astype(F32)
        for j in (1, 2, 3):
            total = total + rs_ref[j - 1, share_rows(p), :].astype(F32)
        return total

    for i, p in enumerate(order[:3]):
        zs_ref[share_rows(p), :] = collect(i, p).astype(BF)
        send(zs_ref.at[share_rows(p)], z_ref.at[z], zs_s.at[i], zs_r.at[z], (p, r, t))
    spread(1, 0)
    proj = collect(3, z)
    w_line_rest(0)
    for c in mom:
        c.wait()
    for p in planes:
        arrive(z_ref.at[p], zs_r.at[p])
        proj = proj + z_ref[p].astype(F32)
    zh_ref[share_rows(z), :] = proj.astype(BF)
    for i, p in ((2, far), (1, mid), (0, near)):
        here = zh_ref.at[share_rows(z)]
        send(here, here, zg_s.at[i], zg_r.at[z], (p, r, t))

    def ratios(i, p):
        span = share_rows(p)
        first, second, ratio = moments(
            zh_ref[span, :].astype(F32), m1_ref[span, :], m2_ref[span, :]
        )
        m1_out[span, :] = first
        m2_out[span, :] = second
        ratio_ref[low_rows(r, p), :] = ratio.astype(BF)
        here = ratio_ref.at[low_rows(r, p)]
        for j in (3, 1, 2):
            send(here, here, ag_s.at[i, j - 1], ag_r.at[i, j - 1], (z, peer[j], t))

    ratios(0, z)
    w_line_rest(1)
    w_line_rest(2)
    for i, p in enumerate(planes):
        arrive(zh_ref.at[share_rows(p)], zg_r.at[p])
        ratios(1 + i, p)
    spread(1, 1)
    relay(1, 0)
    spread(2, 0)
    spread(2, 1)
    arrive(f_ref.at[other], tp_r.at[0])
    for n in range(2):
        g = lax.dot_general(f_ref[n], f_ref[n], dims, preferred_element_type=F32)
        top = g.astype(BF)
        g_ref[n, 0] = top
        g_ref[n, 1] = (g - top.astype(F32)).astype(BF)
    relay(1, 1)
    for i, p in enumerate([z] + planes):
        for j in (1, 2, 3):
            arrive(ratio_ref.at[low_rows(peer[j], p)], ag_r.at[i, j - 1])
    relay(2, 0)
    relay(2, 1)

    def squares(n, span):
        ratio = ratio_ref[:, span]
        a = jnp.dot(g_ref[n, 0], ratio, preferred_element_type=F32)
        a = a + jnp.dot(g_ref[n, 1], ratio, preferred_element_type=F32)
        a = jnp.sum(a * ratio.astype(F32), axis=0, keepdims=True)
        return jnp.sum(a, axis=1, keepdims=True)

    qs = squares(0, slice(0, qc)) / (width * qc * 2)
    vs = squares(1, slice(qc, cols)) / (width * (cols - qc) * 2)
    line = lax.broadcasted_iota(jnp.int32, sq_ref.shape[1:], 0)
    sq_ref[t] = jnp.where(line == 0, qs, vs)
    send(sq_ref.at[t], sq_ref.at[t], tp_s.at[2], tp_r.at[2], (z, r, other))
    arrive(sq_ref.at[other], tp_r.at[2])
    scale_out[...] = lax.rsqrt(jnp.maximum(sq_ref[0] + sq_ref[1], 0.0) + EPS_NORM)
    for i, p in enumerate(planes):
        arrive(w_rest(p), wz_r.at[p, len(chunks)])
        for c in range(len(chunks)):
            for n, begin in ((2, 0), (3, half)):
                arrive(w_rows(p, corner, c).at[:, pl.ds(begin, half)], wp_r.at[i, c, n])
    for c in sent:
        c.wait_send()


def run_line_exchange(x, cq, cv, wq, wv, qf, vf, q1, q2, v1, v2):
    tokens, width = x.shape
    qc = cq.shape[1]
    cols = qc + cv.shape[1]
    rows, rank = qf.shape
    own = rank // 4
    share = own // 4
    quarter = rows // 4 // 128 * 112
    chunks = (quarter // 32 * 16, quarter - quarter // 32 * 16)
    any_spec = pl.BlockSpec(memory_space=pltpu.HBM)
    vmem = pl.BlockSpec(memory_space=pltpu.VMEM)
    dma = pltpu.SemaphoreType.DMA
    n = len(chunks)
    return pl.pallas_call(
        functools.partial(line_exchange, quarter, chunks),
        out_shape=(
            pltpu.VMEM((width, cols), BF),
            pltpu.VMEM((2, width, rank), BF),
            pltpu.VMEM((rank, cols), BF),
            pltpu.VMEM((rows, cols), F32),
            pltpu.VMEM((own, cols), F32),
            pltpu.VMEM((own, cols), F32),
            pltpu.VMEM((8, 128), F32),
        ),
        in_specs=[any_spec] * 11,
        out_specs=(vmem,) * 7,
        scratch_shapes=[
            pltpu.VMEM((tokens, width), BF),
            pltpu.VMEM(cq.shape, BF),
            pltpu.VMEM(cv.shape, BF),
            pltpu.VMEM((tokens, rank), F32),
            pltpu.VMEM((2, tokens, rank), BF),
            pltpu.VMEM((rank, cols), BF),
            pltpu.VMEM((3, own, cols), BF),
            pltpu.VMEM((own, cols), BF),
            pltpu.VMEM((4, share, cols), BF),
            pltpu.VMEM((own, cols), BF),
            pltpu.VMEM((own, cols), F32),
            pltpu.VMEM((own, cols), F32),
            pltpu.VMEM((2, 2, rank, rank), BF),
            pltpu.VMEM((2, 8, 128), F32),
            dma((10,)),
            dma((3,)),
            dma((4,)),
            dma((3, 3)),
            dma((3, 3)),
            dma((3, n + 1)),
            dma((4, n + 1)),
            dma((3, n, 4)),
            dma((3, n, 4)),
            dma((4, 3)),
            dma((4, 3)),
            dma((3,)),
            dma((4,)),
            dma((3,)),
            dma((4,)),
            dma((4, 3)),
            dma((4, 3)),
            dma((3,)),
            dma((3,)),
        ],
        compiler_params=pltpu.CompilerParams(
            collective_id=0, has_side_effects=True, vmem_limit_bytes=48 * 1024 * 1024
        ),
    )(x, cq, cv, wq, wv, qf, vf, q1, q2, v1, v2)


def line_finish(
    steps,
    w_ref,
    f_ref,
    ratio_ref,
    wf_ref,
    m1_ref,
    m2_ref,
    scale_ref,
    qd_out,
    vd_out,
    qm_out,
    vm_out,
    q1_out,
    q2_out,
    v1_out,
    v2_out,
    qcopy_out,
    vcopy_out,
):
    i = pl.program_id(0)
    z = lax.axis_index("fs")
    rows, cols = wf_ref.shape
    qc = qd_out.shape[1]
    tall, small, low = w_ref.shape[0] // steps, rows // steps, m1_ref.shape[0] // steps
    every = pl.ds(pl.multiple_of(i * tall, tall), tall)
    mine = pl.ds(pl.multiple_of(z * rows + i * small, small), small)
    here = pl.ds(pl.multiple_of(i * small, small), small)
    moment = pl.ds(pl.multiple_of(i * low, low), low)
    sets = (
        (0, slice(0, qc), qd_out, qm_out, q1_out, q2_out, qcopy_out),
        (1, slice(qc, cols), vd_out, vm_out, v1_out, v2_out, vcopy_out),
    )
    for n, at, d_out, m_out, m1_out, m2_out, c_out in sets:
        scale = scale_ref[n : n + 1, 0:1]
        ratio = ratio_ref[:, at]
        d = jnp.dot(f_ref[n, mine], ratio, preferred_element_type=F32) * scale
        d_out[...] = d
        m_out[...] = wf_ref[here, at] - RATE * d
        m1_out[...] = m1_ref[moment, at]
        m2_out[...] = m2_ref[moment, at]
        raw = jnp.dot(f_ref[n, every], ratio, preferred_element_type=F32)
        c_out[...] = (w_ref[every, at].astype(F32) - RATE * (raw * scale)).astype(BF)


def run_line_finish(weights, factors, ratio, wf, m1, m2, scale, qc):
    rows, cols = wf.shape
    vc = cols - qc
    width, own = weights.shape[0], m1.shape[0]
    steps = 8

    def tall(n, c):
        return pl.BlockSpec((n // steps, c), lambda i: (i, 0))

    shape = jax.ShapeDtypeStruct
    return pl.pallas_call(
        functools.partial(line_finish, steps),
        grid=(steps,),
        in_specs=[pl.BlockSpec(memory_space=pltpu.VMEM)] * 7,
        out_specs=[
            tall(rows, qc),
            tall(rows, vc),
            tall(rows, qc),
            tall(rows, vc),
            tall(own, qc),
            tall(own, qc),
            tall(own, vc),
            tall(own, vc),
            tall(width, qc),
            tall(width, vc),
        ],
        out_shape=[
            shape((rows, qc), F32),
            shape((rows, vc), F32),
            shape((rows, qc), F32),
            shape((rows, vc), F32),
            shape((own, qc), F32),
            shape((own, qc), F32),
            shape((own, vc), F32),
            shape((own, vc), F32),
            shape((width, qc), BF),
            shape((width, vc), BF),
        ],
        compiler_params=pltpu.CompilerParams(vmem_limit_bytes=24 * 1024 * 1024),
    )(weights, factors, ratio, wf, m1, m2, scale)


def suits_line(nz, nr, qf, cq, cv):
    rows, rank = qf.shape
    cols = cq.shape[1] + cv.shape[1]
    return nz == 4 and nr == 4 and rows % 512 == 0 and rank % 256 == 0 and cols % 256 == 0


def local(nz, nr, *args):
    _, cq, cv, wq, wv, qf, vf, q1, q2, v1, v2 = args
    if suits_line(nz, nr, qf, cq, cv):
        return tuple(run_line_finish(*run_line_exchange(*args), cq.shape[1]))
    weights, factors, ratio, proj, scale = run_exchange(nz, nr, *args)
    return tuple(
        run_finish(factors, ratio, scale, weights, wq, wv, qf, vf, proj, q1, q2, v1, v2)
    )


def solution(mesh):
    return jax.shard_map(
        functools.partial(local, mesh.shape["fs"], mesh.shape["rep"]),
        mesh=mesh,
        in_specs=(
            P(("fs", "rep"), None),
            P(("fs", "rep"), "tp"),
            P(("fs", "rep"), "tp"),
            P("fs", "tp"),
            P("fs", "tp"),
            P("fs", None),
            P("fs", None),
            P("rep", "tp"),
            P("rep", "tp"),
            P("rep", "tp"),
            P("rep", "tp"),
        ),
        out_specs=(
            P("fs", "tp"),
            P("fs", "tp"),
            P("fs", "tp"),
            P("fs", "tp"),
            P("rep", "tp"),
            P("rep", "tp"),
            P("rep", "tp"),
            P("rep", "tp"),
            P(None, "tp"),
            P(None, "tp"),
        ),
        check_vma=False,
    )
```

```python
import functools

import jax
import jax.numpy as jnp
from jax import lax
from jax.experimental import pallas as pl
from jax.experimental.pallas import tpu as pltpu
from jax.sharding import PartitionSpec as P

BETA_ONE = 0.8
BETA_TWO = 0.9
EPS_RATIO = 1e-08
EPS_NORM = 1e-06
RATE = 0.02
BF = jnp.bfloat16
F32 = jnp.float32


def moments(projected, first, second):
    first_new = BETA_ONE * first + (1.0 - BETA_ONE) * projected
    second_new = BETA_TWO * second + (1.0 - BETA_TWO) * projected * projected
    ratio = first_new / (jnp.sqrt(second_new) + EPS_RATIO)
    return (first_new, second_new, ratio)


def exchange(
    nz,
    nr,
    x_hbm,
    cq_hbm,
    cv_hbm,
    wq_hbm,
    wv_hbm,
    qf_hbm,
    vf_hbm,
    q1_hbm,
    q2_hbm,
    v1_hbm,
    v2_hbm,
    w_out,
    f_ref,
    ratio_ref,
    proj_out,
    scale_out,
    x_ref,
    cq_ref,
    cv_ref,
    wf_ref,
    wb_ref,
    low_ref,
    part_ref,
    rs_ref,
    z_ref,
    zg_ref,
    zh_ref,
    m1_ref,
    m2_ref,
    sq_ref,
    local_sem,
    f1_s,
    f1_r,
    w1_s,
    w1_r,
    f2_s,
    f2_r,
    w2_s,
    w2_r,
    rs_s,
    rs_r,
    zs_s,
    zs_r,
    zg_s,
    zg_r,
    ag_s,
    ag_r,
    tp_s,
    tp_r,
):
    z = lax.axis_index("fs")
    r = lax.axis_index("rep")
    t = lax.axis_index("tp")
    rows = qf_hbm.shape[0]
    part = rows // nr
    qc = cq_ref.shape[1]
    cols = w_out.shape[1]
    half = cols // 2
    width = w_out.shape[0]
    rank = low_ref.shape[2]
    own = rank // nr
    tokens = x_ref.shape[0]
    z_of = [lax.rem(z + k, nz) for k in range(nz)]
    z_from = [lax.rem(z + nz - k, nz) for k in range(nz)]
    r_of = [lax.rem(r + j, nr) for j in range(nr)]
    side = r + 1 - 2 * lax.rem(r, 2)
    over = lax.rem(r + 2, nr)
    corner = nr - 1 - r
    other = 1 - t

    def remote(src, dst, ss, rs, dev):
        return pltpu.make_async_remote_copy(
            src_ref=src,
            dst_ref=dst,
            send_sem=ss,
            recv_sem=rs,
            device_id=dev,
            device_id_type=pl.DeviceIdType.MESH,
        )

    def slab(zz, rr):
        return pl.ds(pl.multiple_of(zz * rows + rr * part, part), part)

    def fac_copy(src):
        return pltpu.make_async_copy(
            src,
            f_ref.at[t, pl.ds(pl.multiple_of(z * rows, rows), rows)],
            local_sem.at[0],
        )

    @pl.when(t == 0)
    def _():
        fac_copy(qf_hbm).start()

    @pl.when(t == 1)
    def _():
        fac_copy(vf_hbm).start()

    wq_in = pltpu.make_async_copy(wq_hbm, wf_ref.at[:, pl.ds(0, qc)], local_sem.at[1])
    wv_in = pltpu.make_async_copy(wv_hbm, wf_ref.at[:, pl.ds(qc, cols - qc)], local_sem.at[2])
    x_in = pltpu.make_async_copy(x_hbm, x_ref, local_sem.at[3])
    cq_in = pltpu.make_async_copy(cq_hbm, cq_ref, local_sem.at[4])
    cv_in = pltpu.make_async_copy(cv_hbm, cv_ref, local_sem.at[5])
    left, right = pl.ds(0, qc), pl.ds(qc, cols - qc)
    mom = [
        pltpu.make_async_copy(src, dst.at[:, at], local_sem.at[7 + n])
        for n, (src, dst, at) in enumerate(
            (
                (q1_hbm, m1_ref, left),
                (v1_hbm, m1_ref, right),
                (q2_hbm, m2_ref, left),
                (v2_hbm, m2_ref, right),
            )
        )
    ]
    for c in [wq_in, wv_in, x_in, cq_in, cv_in] + mom:
        c.start()

    barrier = pltpu.get_barrier_semaphore()
    peers = [(z_of[k], r, t) for k in range(1, nz)]
    peers += [(z, r_of[j], t) for j in range(1, nr)]
    peers += [(z, r, other)]
    for dev in peers:
        pl.semaphore_signal(
            barrier, inc=1, device_id=dev, device_id_type=pl.DeviceIdType.MESH
        )
    pl.semaphore_wait(barrier, len(peers))

    fac_copy(qf_hbm).wait()
    sends = []
    f1 = []
    for k in range(1, nz):
        here = f_ref.at[t, slab(z, r)]
        c = remote(here, here, f1_s.at[k - 1], f1_r.at[k - 1], (z_of[k], r, t))
        c.start()
        f1.append(c)
    wq_in.wait()
    wv_in.wait()
    wb_ref[...] = wf_ref[...].astype(BF)
    order = sorted(range(1, nz), key=lambda k: min(k, nz - k))
    w1 = {}
    for k in order:
        c = remote(
            wb_ref.at[pl.ds(pl.multiple_of(r * part, part), part)],
            w_out.at[slab(z, r)],
            w1_s.at[k - 1],
            w1_r.at[k - 1],
            (z_of[k], r, t),
        )
        c.start()
        w1[k] = c
    w_own = pltpu.make_async_copy(
        wb_ref, w_out.at[pl.ds(pl.multiple_of(z * rows, rows), rows)], local_sem.at[6]
    )
    w_own.start()

    f2 = []
    for k in range(1, nz):
        f1[k - 1].wait_recv()
        there = f_ref.at[t, slab(z_from[k], r)]
        for j in range(1, nr):
            n = (k - 1) * (nr - 1) + j - 1
            c = remote(there, there, f2_s.at[n], f2_r.at[n], (z, r_of[j], t))
            c.start()
            f2.append(c)
    for c in f2:
        c.wait_recv()
    w2 = {}

    def spread(k):
        w1[k].wait_recv()
        there = w_out.at[slab(z_from[k], r)]
        for n, dev in ((0, side), (1, over)):
            c = remote(there, there, w2_s.at[k - 1, n], w2_r.at[k - 1, n], (z, dev, t))
            c.start()
            w2[k, n] = c

    def relay(k):
        for n, src, dev, at in ((0, side, over, 0), (1, over, side, half)):
            w2[k, n].wait_recv()
            there = w_out.at[slab(z_from[k], src), pl.ds(at, half)]
            c = remote(
                there, there, w2_s.at[k - 1, 2 + n], w2_r.at[k - 1, 2 + n], (z, dev, t)
            )
            c.start()
            w2[k, 2 + n] = c

    stages = [[], [], []]
    for n, k in enumerate(order):
        stages[min(n, 2)].append(k)
    x_in.wait()
    tile = tokens // 3

    @pl.loop(0, 3)
    def _(i):
        span = pl.ds(pl.multiple_of(i * tile, tile), tile)
        low_ref[t, span] = jnp.dot(
            x_ref[span, :], f_ref[t], preferred_element_type=F32
        ).astype(BF)

    lx = remote(low_ref.at[t], low_ref.at[t], tp_s.at[1], tp_r.at[1], (z, r, other))
    lx.start()
    fx = remote(f_ref.at[t], f_ref.at[t], tp_s.at[0], tp_r.at[0], (z, r, other))
    fx.start()
    for k in stages[0]:
        spread(k)
    cq_in.wait()
    cv_in.wait()
    lx.wait_recv()
    dims = (((0,), (0,)), ((), ()))
    part_ref[:, :qc] = lax.dot_general(
        low_ref[0], cq_ref[...], dims, preferred_element_type=F32
    ).astype(BF)
    part_ref[:, qc:] = lax.dot_general(
        low_ref[1], cv_ref[...], dims, preferred_element_type=F32
    ).astype(BF)

    def low_rows(rr):
        return pl.ds(pl.multiple_of(rr * own, own), own)

    rsc = []
    for j in range(1, nr):
        c = remote(
            part_ref.at[low_rows(r_of[j])],
            rs_ref.at[j - 1],
            rs_s.at[j - 1],
            rs_r.at[j - 1],
            (z, r_of[j], t),
        )
        c.start()
        rsc.append(c)

    for k in stages[0]:
        relay(k)
    for c in rsc:
        c.wait_recv()
    total = part_ref[low_rows(r), :].astype(F32)
    for j in range(1, nr):
        total = total + rs_ref[j - 1].astype(F32)
    share = own // nz
    scatter = share % 16 == 0
    zc = []
    if scatter:
        zg_ref[...] = total.astype(BF)
    else:
        z_ref[z] = total.astype(BF)

    def z_rows(zz):
        return pl.ds(pl.multiple_of(zz * share, share), share)

    for k in range(1, nz):
        src = zg_ref.at[z_rows(z_of[k])] if scatter else z_ref.at[z]
        c = remote(src, z_ref.at[z], zs_s.at[k - 1], zs_r.at[k - 1], (z_of[k], r, t))
        c.start()
        zc.append(c)
    if scatter:
        z_ref[z] = zg_ref[z_rows(z), :]
    for k in stages[1]:
        spread(k)
    for c in zc:
        c.wait_recv()
    proj = z_ref[0].astype(F32)
    for k in range(1, nz):
        proj = proj + z_ref[k].astype(F32)
    gc = []
    if scatter:
        for c in zc:
            c.wait_send()
        zh = zh_ref
        zh[z_rows(z), :] = proj.astype(BF)
        for k in range(1, nz):
            here = zh.at[z_rows(z)]
            c = remote(here, here, zg_s.at[k - 1], zg_r.at[k - 1], (z_of[k], r, t))
            c.start()
            gc.append(c)
    for k in stages[1]:
        relay(k)
    for k in stages[2]:
        spread(k)
    for c in mom:
        c.wait()
    if scatter:
        for c in gc:
            c.wait_recv()
        proj = zh[...].astype(F32)
    proj_out[...] = proj
    _, _, ratio = moments(proj, m1_ref[...], m2_ref[...])
    ratio_ref[low_rows(r), :] = ratio.astype(BF)
    agc = []
    for j in range(1, nr):
        here = ratio_ref.at[low_rows(r)]
        c = remote(here, here, ag_s.at[j - 1], ag_r.at[j - 1], (z, r_of[j], t))
        c.start()
        agc.append(c)
    for k in stages[2]:
        relay(k)
    fx.wait_recv()
    for c in agc:
        c.wait_recv()
    step = min(256, width)

    def squares(i, acc):
        span = pl.ds(pl.multiple_of(i * step, step), step)
        a = jnp.dot(f_ref[0, span], ratio_ref[:, :qc], preferred_element_type=F32)
        b = jnp.dot(f_ref[1, span], ratio_ref[:, qc:], preferred_element_type=F32)
        a = jnp.sum(a * a, axis=0, keepdims=True)
        b = jnp.sum(b * b, axis=0, keepdims=True)
        return (acc[0] + a, acc[1] + b)

    qs, vs = lax.fori_loop(
        0,
        width // step,
        squares,
        (jnp.zeros((1, qc), F32), jnp.zeros((1, cols - qc), F32)),
    )
    qs = jnp.sum(qs, axis=1, keepdims=True)
    vs = jnp.sum(vs, axis=1, keepdims=True)
    row = lax.broadcasted_iota(jnp.int32, sq_ref.shape[1:], 0)
    sq_ref[t] = jnp.where(row == 0, qs / (width * qc * 2), vs / (width * (cols - qc) * 2))
    sx = remote(sq_ref.at[t], sq_ref.at[t], tp_s.at[2], tp_r.at[2], (z, r, other))
    sx.start()
    sx.wait_recv()
    scale_out[...] = lax.rsqrt(sq_ref[0] + sq_ref[1] + EPS_NORM)
    for k in range(1, nz):
        w2[k, 2].wait_recv()
        w2[k, 3].wait_recv()
    for c in f1 + list(w1.values()) + f2 + rsc + ([] if scatter else zc) + gc + agc + [fx, lx, sx] + list(w2.values()):
        c.wait_send()
    w_own.wait()


def run_exchange(nz, nr, x, cq, cv, wq, wv, qf, vf, q1, q2, v1, v2):
    tokens, width = x.shape
    qc = cq.shape[1]
    cols = qc + cv.shape[1]
    rows, rank = qf.shape
    own = rank // nr
    share = own // nz if (own // nz) % 16 == 0 else own
    any_spec = pl.BlockSpec(memory_space=pltpu.HBM)
    vmem = pl.BlockSpec(memory_space=pltpu.VMEM)
    dma = pltpu.SemaphoreType.DMA
    shape = jax.ShapeDtypeStruct
    return pl.pallas_call(
        functools.partial(exchange, nz, nr),
        out_shape=(
            shape((width, cols), BF),
            shape((2, width, rank), BF),
            shape((rank, cols), BF),
            shape((own, cols), F32),
            shape((8, 128), F32),
        ),
        in_specs=[any_spec] * 11,
        out_specs=(any_spec, vmem, vmem, vmem, vmem),
        scratch_shapes=[
            pltpu.VMEM((tokens, width), BF),
            pltpu.VMEM(cq.shape, BF),
            pltpu.VMEM(cv.shape, BF),
            pltpu.VMEM((rows, cols), F32),
            pltpu.VMEM((rows, cols), BF),
            pltpu.VMEM((2, tokens, rank), BF),
            pltpu.VMEM((rank, cols), BF),
            pltpu.VMEM((nr - 1, own, cols), BF),
            pltpu.VMEM((nz, share, cols), BF),
            pltpu.VMEM((own, cols), BF),
            pltpu.VMEM((own, cols), BF),
            pltpu.VMEM((own, cols), F32),
            pltpu.VMEM((own, cols), F32),
            pltpu.VMEM((2, 8, 128), F32),
            dma((11,)),
            dma((nz - 1,)),
            dma((nz - 1,)),
            dma((nz - 1,)),
            dma((nz - 1,)),
            dma(((nz - 1) * (nr - 1),)),
            dma(((nz - 1) * (nr - 1),)),
            dma((nz - 1, 4)),
            dma((nz - 1, 4)),
            dma((nr - 1,)),
            dma((nr - 1,)),
            dma((nz - 1,)),
            dma((nz - 1,)),
            dma((nz - 1,)),
            dma((nz - 1,)),
            dma((nr - 1,)),
            dma((nr - 1,)),
            dma((3,)),
            dma((3,)),
        ],
        compiler_params=pltpu.CompilerParams(
            collective_id=0, has_side_effects=True, vmem_limit_bytes=60 * 1024 * 1024
        ),
    )(x, cq, cv, wq, wv, qf, vf, q1, q2, v1, v2)


def finish(
    f_ref,
    ratio_ref,
    scale_ref,
    w_ref,
    wq_ref,
    wv_ref,
    qf_ref,
    vf_ref,
    proj_ref,
    q1_ref,
    q2_ref,
    v1_ref,
    v2_ref,
    qd_out,
    vd_out,
    qm_out,
    vm_out,
    q1_out,
    q2_out,
    v1_out,
    v2_out,
    qcopy_out,
    vcopy_out,
):
    qc = wq_ref.shape[1]
    sets = (
        (0, pl.ds(0, qc), wq_ref, qf_ref, q1_ref, q2_ref, qd_out, qm_out, q1_out, q2_out, qcopy_out),
        (
            1,
            pl.ds(qc, wv_ref.shape[1]),
            wv_ref,
            vf_ref,
            v1_ref,
            v2_ref,
            vd_out,
            vm_out,
            v1_out,
            v2_out,
            vcopy_out,
        ),
    )
    for n, at, w, f, m1, m2, d_out, m_out, m1_out, m2_out, c_out in sets:
        scale = scale_ref[n : n + 1, 0:1]
        ratio = ratio_ref[:, at]
        raw = jnp.dot(f_ref[n], ratio, preferred_element_type=F32)
        c_out[...] = (w_ref[:, at].astype(F32) - RATE * (raw * scale)).astype(BF)
        d = jnp.dot(f[...], ratio, preferred_element_type=F32) * scale
        d_out[...] = d
        m_out[...] = w[...] - RATE * d
        m1_out[...], m2_out[...], _ = moments(proj_ref[:, at], m1[...], m2[...])


def run_finish(factors, ratio, scale, weights, wq, wv, qf, vf, proj, q1, q2, v1, v2):
    rows, qc = wq.shape
    vc = wv.shape[1]
    width, cols = weights.shape
    rank, own = qf.shape[1], q1.shape[0]
    steps = 8 if rows % 128 == 0 else 4

    def tall(n, c):
        return pl.BlockSpec((n // steps, c), lambda i: (i, 0))

    def whole(a):
        return pl.BlockSpec(a.shape, lambda i: (0,) * a.ndim)

    shape = jax.ShapeDtypeStruct
    return pl.pallas_call(
        finish,
        grid=(steps,),
        in_specs=[
            pl.BlockSpec((2, width // steps, rank), lambda i: (0, i, 0)),
            whole(ratio),
            whole(scale),
            tall(width, cols),
            tall(rows, qc),
            tall(rows, vc),
            tall(rows, rank),
            tall(rows, rank),
            tall(own, cols),
            tall(own, qc),
            tall(own, qc),
            tall(own, vc),
            tall(own, vc),
        ],
        out_specs=[
            tall(rows, qc),
            tall(rows, vc),
            tall(rows, qc),
            tall(rows, vc),
            tall(own, qc),
            tall(own, qc),
            tall(own, vc),
            tall(own, vc),
            tall(width, qc),
            tall(width, vc),
        ],
        out_shape=[
            shape((rows, qc), F32),
            shape((rows, vc), F32),
            shape((rows, qc), F32),
            shape((rows, vc), F32),
            shape((own, qc), F32),
            shape((own, qc), F32),
            shape((own, vc), F32),
            shape((own, vc), F32),
            shape((width, qc), BF),
            shape((width, vc), BF),
        ],
        compiler_params=pltpu.CompilerParams(vmem_limit_bytes=60 * 1024 * 1024),
    )(factors, ratio, scale, weights, wq, wv, qf, vf, proj, q1, q2, v1, v2)


def line_exchange(
    quarter,
    chunks,
    rests,
    x_hbm,
    cq_hbm,
    cv_hbm,
    wq_hbm,
    wv_hbm,
    qf_hbm,
    vf_hbm,
    q1_hbm,
    q2_hbm,
    v1_hbm,
    v2_hbm,
    w_ref,
    f_ref,
    ratio_ref,
    wf_ref,
    m1_out,
    m2_out,
    scale_out,
    x_ref,
    cq_ref,
    cv_ref,
    acc_ref,
    low_ref,
    part_ref,
    ra_ref,
    tb_ref,
    rb_ref,
    zs_ref,
    zo_ref,
    z_ref,
    zh_ref,
    m1_ref,
    m2_ref,
    g_ref,
    sq_ref,
    local_sem,
    fz_s,
    fz_r,
    fp_s,
    fp_r,
    wz_s,
    wz_r,
    wp_s,
    wp_r,
    ra_s,
    ra_r,
    rb_s,
    rb_r,
    zs_s,
    zs_r,
    zg_s,
    zg_r,
    ag_s,
    ag_r,
    tp_s,
    tp_r,
):
    z = lax.axis_index("fs")
    r = lax.axis_index("rep")
    t = lax.axis_index("tp")
    nz, nr = 4, 4
    rows = qf_hbm.shape[0]
    part = rows // nr
    qc = cq_ref.shape[1]
    width, cols = w_ref.shape
    half = cols // 2
    rank = low_ref.shape[2]
    own = rank // nr
    share = own // nz
    tokens = x_ref.shape[0]
    px, py = lax.rem(r, 2), lax.div(r, 2)
    side = r + 1 - 2 * px
    over = lax.rem(r + 2, nr)
    corner = nr - 1 - r
    other = 1 - t
    upper = lax.div(z, 2)
    near = z + 1 - 2 * lax.rem(z, 2)
    mid = 2 - upper
    far = 3 - 3 * upper
    planes = [near, mid, far]
    inner = jnp.logical_and(z > 0, z < nz - 1)
    sent, passed = [], []

    def remote(src, dst, ss, rs, dev):
        return pltpu.make_async_remote_copy(
            src_ref=src,
            dst_ref=dst,
            send_sem=ss,
            recv_sem=rs,
            device_id=dev,
            device_id_type=pl.DeviceIdType.MESH,
        )

    def send(src, dst, ss, rs, dev):
        c = remote(src, dst, ss, rs, dev)
        c.start()
        sent.append(c)

    def send_inner(src, dst, ss, rs, dev):
        c = remote(src, dst, ss, rs, dev)
        passed.append(c)

        @pl.when(inner)
        def _():
            c.start()

    def arrive(dst, rs):
        remote(dst, dst, tp_s.at[0], rs, (z, r, other)).wait_recv()

    def at(start, size, step):
        return pl.ds(pl.multiple_of(start, step), size)

    def fac_copy(src):
        return pltpu.make_async_copy(src, f_ref.at[t, at(z * rows, rows, rows)], local_sem.at[0])

    @pl.when(t == 0)
    def _():
        fac_copy(qf_hbm).start()

    @pl.when(t == 1)
    def _():
        fac_copy(vf_hbm).start()

    left, right = pl.ds(0, qc), pl.ds(qc, cols - qc)
    wq_in = pltpu.make_async_copy(wq_hbm, wf_ref.at[:, left], local_sem.at[1])
    wv_in = pltpu.make_async_copy(wv_hbm, wf_ref.at[:, right], local_sem.at[2])
    x_in = pltpu.make_async_copy(x_hbm, x_ref, local_sem.at[3])
    cq_in = pltpu.make_async_copy(cq_hbm, cq_ref, local_sem.at[4])
    cv_in = pltpu.make_async_copy(cv_hbm, cv_ref, local_sem.at[5])
    mom = [
        pltpu.make_async_copy(src, dst.at[:, span], local_sem.at[6 + n])
        for n, (src, dst, span) in enumerate(
            (
                (q1_hbm, m1_ref, left),
                (v1_hbm, m1_ref, right),
                (q2_hbm, m2_ref, left),
                (v2_hbm, m2_ref, right),
            )
        )
    ]
    for c in [wq_in, wv_in, x_in, cq_in, cv_in] + mom:
        c.start()

    barrier = pltpu.get_barrier_semaphore()
    peers = [(p, r, t) for p in planes]
    peers += [(z, p, t) for p in (side, over, corner)]
    peers += [(z, r, other)]
    for dev in peers:
        pl.semaphore_signal(
            barrier, inc=1, device_id=dev, device_id_type=pl.DeviceIdType.MESH
        )
    pl.semaphore_wait(barrier, len(peers))

    class Spread:
        def __init__(self, view, split, ss, rs):
            self.view, self.split, self.ss, self.rs = view, split, ss, rs

        def start(self):
            here = self.view(r)
            for n, dev in ((0, side), (1, over)):
                send(here, here, self.ss.at[n], self.rs.at[n], (z, dev, t))

        def relay(self):
            for n, src, dev in ((0, side, over), (1, over, side)):
                whole = self.view(src)
                arrive(whole, self.rs.at[n])
                there = self.split(whole, n)
                send(there, there, self.ss.at[2 + n], self.rs.at[2 + n], (z, dev, t))

        def finish(self):
            for n in range(2):
                arrive(self.split(self.view(corner), n), self.rs.at[2 + n])

    def halves(ref, n):
        return ref.at[:, pl.ds(n * half, half)]

    def fac_rows(plane, rr):
        return f_ref.at[t, at(plane * rows + rr * part, part, part)]

    fac_copy(qf_hbm).wait()
    for i, p in enumerate(planes):
        here = fac_rows(z, r)
        send(here, here, fz_s.at[i], fz_r.at[z], (p, r, t))

    spans = [(n, s, True) for n, s in zip([sum(chunks[:c]) for c in range(len(chunks))], chunks)]
    spans += [(n, s, False) for n, s in zip([sum(rests[:c]) for c in range(len(rests))], rests)]

    def w_rows(plane, rr, c):
        begin, size, split = spans[c]
        begin = plane * rows + begin + (rr * quarter if split else nr * quarter)
        return w_ref.at[at(begin, size, 8)]

    def w_own(c):
        here = w_rows(z, r, c)
        send(here, here, wz_s.at[3, c], wz_r.at[z, c], (near, r, t))
        send_inner(here, here, wz_s.at[4, c], wz_r.at[z, c], (mid, r, t))

    def w_pass(i, c):
        here = w_rows(planes[i], r, c)
        to = near if i else mid
        copy = remote(here, here, wz_s.at[i, c], wz_r.at[planes[i], c], (to, r, t))
        passed.append(copy)

        @pl.when(inner)
        def _():
            arrive(here, wz_r.at[planes[i], c])
            copy.start()

    def w_land(i, c):
        @pl.when(jnp.logical_not(inner))
        def _():
            arrive(w_rows(planes[i], r, c), wz_r.at[planes[i], c])

    def w_start(i, c):
        w_land(i, c)
        w_in[i][c].start()

    w_in = [
        [
            Spread(functools.partial(lambda p, c, rr: w_rows(p, rr, c), p, c), halves, wp_s.at[i, c], wp_r.at[i, c])
            for c in range(len(chunks))
        ]
        for i, p in enumerate(planes)
    ]

    def low_add(plane, first):
        tile = tokens // 3

        @pl.loop(0, 3)
        def _(n):
            span = at(n * tile, tile, 16)
            a = jnp.dot(
                x_ref[span, at(plane * rows, rows, rows)],
                f_ref[t, at(plane * rows, rows, rows)],
                preferred_element_type=F32,
            )
            acc_ref[span, :] = a if first else acc_ref[span, :] + a

    fac = [
        Spread(
            functools.partial(fac_rows, p),
            lambda ref, n: ref.at[pl.ds(n * (part // 2), part // 2)],
            fp_s.at[i],
            fp_r.at[i],
        )
        for i, p in enumerate(planes)
    ]

    def fac_start(i):
        arrive(fac_rows(planes[i], r), fz_r.at[planes[i]])
        fac[i].start()

    def fac_finish(i):
        fac[i].finish()
        low_add(planes[i], False)

    def share_rows(plane):
        return at(plane * share, share, share)

    def low_rows(rr, plane):
        return at(rr * own + plane * share, share, share)

    lo, hi = pl.ds(0, half), pl.ds(half, half)
    order = [far, mid, near, z]

    def sum_start(i):
        span = share_rows(order[i])
        for n, src, dev in (
            (0, part_ref.at[:, 1 - px, span, lo], side),
            (1, part_ref.at[1 - py, :, span, hi], over),
        ):
            send(src, ra_ref.at[n, :, span], ra_s.at[i, n], ra_r.at[i, n], (z, dev, t))

    def sum_relay(i):
        span = share_rows(order[i])
        for n in range(2):
            arrive(ra_ref.at[n, :, span], ra_r.at[i, n])
        for n, mine, theirs, dev in (
            (0, part_ref[1 - py, px, span, lo], ra_ref[0, 1 - py, span, :], over),
            (1, part_ref[py, 1 - px, span, hi], ra_ref[1, 1 - px, span, :], side),
        ):
            tb_ref[n, span, :] = (mine.astype(F32) + theirs.astype(F32)).astype(BF)
            send(tb_ref.at[n, span], rb_ref.at[n, span], rb_s.at[i, n], rb_r.at[i, n], (z, dev, t))

    def sum_finish(i):
        span = share_rows(order[i])
        for n in range(2):
            arrive(rb_ref.at[n, span], rb_r.at[i, n])
        out = []
        for n, cut, theirs in ((0, lo, ra_ref[0, py, span, :]), (1, hi, ra_ref[1, px, span, :])):
            a = part_ref[py, px, span, cut].astype(F32) + theirs.astype(F32)
            out.append(a + rb_ref[n, span, :].astype(F32))
        if i == 3:
            zo_ref[:, lo], zo_ref[:, hi] = out
        else:
            zs_ref[span, lo] = out[0].astype(BF)
            zs_ref[span, hi] = out[1].astype(BF)
            send(zs_ref.at[span], z_ref.at[z], zs_s.at[i], zs_r.at[z], (order[i], r, t))

    def line_sum():
        proj = zo_ref[...]
        for p in planes:
            arrive(z_ref.at[p], zs_r.at[p])
            proj = proj + z_ref[p].astype(F32)
        here = zh_ref.at[share_rows(z)]
        zh_ref[share_rows(z), :] = proj.astype(BF)
        for i, p in ((2, far), (1, mid), (0, near)):
            send(here, here, zg_s.at[i], zg_r.at[z], (p, r, t))

    ratio_in = [
        Spread(
            functools.partial(lambda p, rr: ratio_ref.at[low_rows(rr, p)], p),
            halves,
            ag_s.at[i],
            ag_r.at[i],
        )
        for i, p in enumerate([z] + planes)
    ]

    def ratio_start(i):
        p = z
        if i:
            p = planes[i - 1]
            arrive(zh_ref.at[share_rows(p)], zg_r.at[p])
        span = share_rows(p)
        first, second, ratio = moments(
            zh_ref[span, :].astype(F32), m1_ref[span, :], m2_ref[span, :]
        )
        m1_out[span, :] = first
        m2_out[span, :] = second
        ratio_ref[low_rows(r, p), :] = ratio.astype(BF)
        ratio_in[i].start()

    dims = (((0,), (0,)), ((), ()))

    def low_parts():
        for n, c_ref, span in ((0, cq_ref, slice(0, qc)), (1, cv_ref, slice(qc, cols))):
            a = lax.dot_general(
                low_ref[n], c_ref[...], dims, preferred_element_type=F32
            ).astype(BF)
            for k in range(nr):
                part_ref[k // 2, k % 2, :, span] = a[k * own : (k + 1) * own]

    def gram():
        arrive(f_ref.at[other], tp_r.at[0])
        for n in range(2):
            g = lax.dot_general(f_ref[n], f_ref[n], dims, preferred_element_type=F32)
            top = g.astype(BF)
            g_ref[n, 0] = top
            g_ref[n, 1] = (g - top.astype(F32)).astype(BF)

    def squares(n, span):
        ratio = ratio_ref[:, span]
        a = jnp.dot(g_ref[n, 0], ratio, preferred_element_type=F32)
        a = a + jnp.dot(g_ref[n, 1], ratio, preferred_element_type=F32)
        a = jnp.sum(a * ratio.astype(F32), axis=0, keepdims=True)
        return jnp.sum(a, axis=1, keepdims=True)

    wq_in.wait()
    wv_in.wait()
    w_ref[at(z * rows, rows, rows), :] = wf_ref[...].astype(BF)
    x_in.wait()
    low_add(z, True)
    fac_start(0)
    w_own(0)
    w_own(1)
    fac_start(1)
    fac_start(2)
    fac[0].relay()
    fac[1].relay()
    w_pass(0, 0)
    w_pass(1, 0)
    fac[2].relay()
    w_start(0, 0)
    fac_finish(0)
    w_pass(0, 1)
    w_pass(1, 1)
    w_start(0, 1)
    fac_finish(1)
    fac_finish(2)
    low_ref[t] = acc_ref[...].astype(BF)
    send(low_ref.at[t], low_ref.at[t], tp_s.at[1], tp_r.at[1], (z, r, other))
    send(f_ref.at[t], f_ref.at[t], tp_s.at[0], tp_r.at[0], (z, r, other))
    w_pass(2, 0)
    cq_in.wait()
    cv_in.wait()
    arrive(low_ref.at[other], tp_r.at[1])
    low_parts()
    for i in range(4):
        sum_start(i)
    w_in[0][0].relay()
    w_in[0][1].relay()
    w_pass(2, 1)
    w_own(2)
    sum_relay(0)
    sum_relay(1)
    sum_relay(2)
    sum_relay(3)
    w_start(1, 0)
    w_pass(0, 2)
    w_pass(1, 2)
    sum_finish(0)
    sum_finish(1)
    sum_finish(2)
    sum_finish(3)
    w_start(1, 1)
    w_pass(2, 2)
    for c in mom:
        c.wait()
    line_sum()
    w_in[1][0].relay()
    ratio_start(0)
    w_start(2, 0)
    ratio_start(1)
    ratio_start(2)
    ratio_start(3)
    w_own(3)
    w_in[1][1].relay()
    w_start(2, 1)
    ratio_in[0].relay()
    ratio_in[1].relay()
    ratio_in[2].relay()
    ratio_in[3].relay()
    w_pass(0, 3)
    w_pass(1, 3)
    gram()
    w_in[2][0].relay()
    w_pass(2, 3)
    for i in range(4):
        ratio_in[i].finish()
    qs = squares(0, slice(0, qc)) / (width * qc * 2)
    vs = squares(1, slice(qc, cols)) / (width * (cols - qc) * 2)
    line = lax.broadcasted_iota(jnp.int32, sq_ref.shape[1:], 0)
    sq_ref[t] = jnp.where(line == 0, qs, vs)
    send(sq_ref.at[t], sq_ref.at[t], tp_s.at[2], tp_r.at[2], (z, r, other))
    w_in[2][1].relay()
    for c in range(len(chunks), len(spans)):
        for i in range(3):
            w_land(i, c)
    arrive(sq_ref.at[other], tp_r.at[2])
    scale_out[...] = lax.rsqrt(jnp.maximum(sq_ref[0] + sq_ref[1], 0.0) + EPS_NORM)
    for i in range(3):
        for c in range(len(chunks)):
            w_in[i][c].finish()
    for c in sent:
        c.wait_send()

    @pl.when(inner)
    def _():
        for c in passed:
            c.wait_send()


def run_line_exchange(x, cq, cv, wq, wv, qf, vf, q1, q2, v1, v2):
    tokens, width = x.shape
    qc = cq.shape[1]
    cols = qc + cv.shape[1]
    rows, rank = qf.shape
    own = rank // 4
    share = own // 4
    unit = rows // 64
    quarter = 13 * unit
    chunks = (7 * unit, 6 * unit)
    rests = (6 * unit, 6 * unit)
    any_spec = pl.BlockSpec(memory_space=pltpu.HBM)
    vmem = pl.BlockSpec(memory_space=pltpu.VMEM)
    dma = pltpu.SemaphoreType.DMA
    n = len(chunks)
    m = n + len(rests)
    return pl.pallas_call(
        functools.partial(line_exchange, quarter, chunks, rests),
        out_shape=(
            pltpu.VMEM((width, cols), BF),
            pltpu.VMEM((2, width, rank), BF),
            pltpu.VMEM((rank, cols), BF),
            pltpu.VMEM((rows, cols), F32),
            pltpu.VMEM((own, cols), F32),
            pltpu.VMEM((own, cols), F32),
            pltpu.VMEM((8, 128), F32),
        ),
        in_specs=[any_spec] * 11,
        out_specs=(vmem,) * 7,
        scratch_shapes=[
            pltpu.VMEM((tokens, width), BF),
            pltpu.VMEM(cq.shape, BF),
            pltpu.VMEM(cv.shape, BF),
            pltpu.VMEM((tokens, rank), F32),
            pltpu.VMEM((2, tokens, rank), BF),
            pltpu.VMEM((2, 2, own, cols), BF),
            pltpu.VMEM((2, 2, own, cols // 2), BF),
            pltpu.VMEM((2, own, cols // 2), BF),
            pltpu.VMEM((2, own, cols // 2), BF),
            pltpu.VMEM((own, cols), BF),
            pltpu.VMEM((share, cols), F32),
            pltpu.VMEM((4, share, cols), BF),
            pltpu.VMEM((own, cols), BF),
            pltpu.VMEM((own, cols), F32),
            pltpu.VMEM((own, cols), F32),
            pltpu.VMEM((2, 2, rank, rank), BF),
            pltpu.VMEM((2, 8, 128), F32),
            dma((10,)),
            dma((3,)),
            dma((4,)),
            dma((3, 4)),
            dma((3, 4)),
            dma((5, m)),
            dma((4, m)),
            dma((3, n, 4)),
            dma((3, n, 4)),
            dma((4, 2)),
            dma((4, 2)),
            dma((4, 2)),
            dma((4, 2)),
            dma((3,)),
            dma((4,)),
            dma((3,)),
            dma((4,)),
            dma((4, 4)),
            dma((4, 4)),
            dma((3,)),
            dma((3,)),
        ],
        compiler_params=pltpu.CompilerParams(
            collective_id=0, has_side_effects=True, vmem_limit_bytes=48 * 1024 * 1024
        ),
    )(x, cq, cv, wq, wv, qf, vf, q1, q2, v1, v2)


def line_finish(
    steps,
    w_ref,
    f_ref,
    ratio_ref,
    wf_ref,
    m1_ref,
    m2_ref,
    scale_ref,
    qd_out,
    vd_out,
    qm_out,
    vm_out,
    q1_out,
    q2_out,
    v1_out,
    v2_out,
    qcopy_out,
    vcopy_out,
):
    i = pl.program_id(0)
    z = lax.axis_index("fs")
    rows, cols = wf_ref.shape
    qc = qd_out.shape[1]
    tall, small, low = w_ref.shape[0] // steps, rows // steps, m1_ref.shape[0] // steps
    every = pl.ds(pl.multiple_of(i * tall, tall), tall)
    mine = pl.ds(pl.multiple_of(z * rows + i * small, small), small)
    here = pl.ds(pl.multiple_of(i * small, small), small)
    moment = pl.ds(pl.multiple_of(i * low, low), low)
    sets = (
        (0, slice(0, qc), qd_out, qm_out, q1_out, q2_out, qcopy_out),
        (1, slice(qc, cols), vd_out, vm_out, v1_out, v2_out, vcopy_out),
    )
    for n, at, d_out, m_out, m1_out, m2_out, c_out in sets:
        scale = scale_ref[n : n + 1, 0:1]
        ratio = ratio_ref[:, at]
        d = jnp.dot(f_ref[n, mine], ratio, preferred_element_type=F32) * scale
        d_out[...] = d
        m_out[...] = wf_ref[here, at] - RATE * d
        m1_out[...] = m1_ref[moment, at]
        m2_out[...] = m2_ref[moment, at]
        raw = jnp.dot(f_ref[n, every], ratio, preferred_element_type=F32)
        c_out[...] = (w_ref[every, at].astype(F32) - RATE * (raw * scale)).astype(BF)


def run_line_finish(weights, factors, ratio, wf, m1, m2, scale, qc):
    rows, cols = wf.shape
    vc = cols - qc
    width, own = weights.shape[0], m1.shape[0]
    steps = 8

    def tall(n, c):
        return pl.BlockSpec((n // steps, c), lambda i: (i, 0))

    shape = jax.ShapeDtypeStruct
    return pl.pallas_call(
        functools.partial(line_finish, steps),
        grid=(steps,),
        in_specs=[pl.BlockSpec(memory_space=pltpu.VMEM)] * 7,
        out_specs=[
            tall(rows, qc),
            tall(rows, vc),
            tall(rows, qc),
            tall(rows, vc),
            tall(own, qc),
            tall(own, qc),
            tall(own, vc),
            tall(own, vc),
            tall(width, qc),
            tall(width, vc),
        ],
        out_shape=[
            shape((rows, qc), F32),
            shape((rows, vc), F32),
            shape((rows, qc), F32),
            shape((rows, vc), F32),
            shape((own, qc), F32),
            shape((own, qc), F32),
            shape((own, vc), F32),
            shape((own, vc), F32),
            shape((width, qc), BF),
            shape((width, vc), BF),
        ],
        compiler_params=pltpu.CompilerParams(vmem_limit_bytes=24 * 1024 * 1024),
    )(weights, factors, ratio, wf, m1, m2, scale)


def suits_line(nz, nr, qf, cq, cv):
    rows, rank = qf.shape
    cols = cq.shape[1] + cv.shape[1]
    return nz == 4 and nr == 4 and rows % 512 == 0 and rank % 256 == 0 and cols % 256 == 0


def local(nz, nr, *args):
    _, cq, cv, wq, wv, qf, vf, q1, q2, v1, v2 = args
    if suits_line(nz, nr, qf, cq, cv):
        return tuple(run_line_finish(*run_line_exchange(*args), cq.shape[1]))
    weights, factors, ratio, proj, scale = run_exchange(nz, nr, *args)
    return tuple(
        run_finish(factors, ratio, scale, weights, wq, wv, qf, vf, proj, q1, q2, v1, v2)
    )


def solution(mesh):
    return jax.shard_map(
        functools.partial(local, mesh.shape["fs"], mesh.shape["rep"]),
        mesh=mesh,
        in_specs=(
            P(("fs", "rep"), None),
            P(("fs", "rep"), "tp"),
            P(("fs", "rep"), "tp"),
            P("fs", "tp"),
            P("fs", "tp"),
            P("fs", None),
            P("fs", None),
            P("rep", "tp"),
            P("rep", "tp"),
            P("rep", "tp"),
            P("rep", "tp"),
        ),
        out_specs=(
            P("fs", "tp"),
            P("fs", "tp"),
            P("fs", "tp"),
            P("fs", "tp"),
            P("rep", "tp"),
            P("rep", "tp"),
            P("rep", "tp"),
            P("rep", "tp"),
            P(None, "tp"),
            P(None, "tp"),
        ),
        check_vma=False,
    )
```

```python
import functools

import jax
import jax.numpy as jnp
from jax import lax
from jax.experimental import pallas as pl
from jax.experimental.pallas import tpu as pltpu
from jax.sharding import PartitionSpec as P

BETA_ONE = 0.8
BETA_TWO = 0.9
EPS_RATIO = 1e-08
EPS_NORM = 1e-06
RATE = 0.02
BF = jnp.bfloat16
F32 = jnp.float32


def moments(projected, first, second):
    first_new = BETA_ONE * first + (1.0 - BETA_ONE) * projected
    second_new = BETA_TWO * second + (1.0 - BETA_TWO) * projected * projected
    ratio = first_new / (jnp.sqrt(second_new) + EPS_RATIO)
    return (first_new, second_new, ratio)


def exchange(
    nz,
    nr,
    x_hbm,
    cq_hbm,
    cv_hbm,
    wq_hbm,
    wv_hbm,
    qf_hbm,
    vf_hbm,
    q1_hbm,
    q2_hbm,
    v1_hbm,
    v2_hbm,
    w_out,
    f_ref,
    ratio_ref,
    proj_out,
    scale_out,
    x_ref,
    cq_ref,
    cv_ref,
    wf_ref,
    wb_ref,
    low_ref,
    part_ref,
    rs_ref,
    z_ref,
    zg_ref,
    zh_ref,
    m1_ref,
    m2_ref,
    sq_ref,
    local_sem,
    f1_s,
    f1_r,
    w1_s,
    w1_r,
    f2_s,
    f2_r,
    w2_s,
    w2_r,
    rs_s,
    rs_r,
    zs_s,
    zs_r,
    zg_s,
    zg_r,
    ag_s,
    ag_r,
    tp_s,
    tp_r,
):
    z = lax.axis_index("fs")
    r = lax.axis_index("rep")
    t = lax.axis_index("tp")
    rows = qf_hbm.shape[0]
    part = rows // nr
    qc = cq_ref.shape[1]
    cols = w_out.shape[1]
    half = cols // 2
    width = w_out.shape[0]
    rank = low_ref.shape[2]
    own = rank // nr
    tokens = x_ref.shape[0]
    z_of = [lax.rem(z + k, nz) for k in range(nz)]
    z_from = [lax.rem(z + nz - k, nz) for k in range(nz)]
    r_of = [lax.rem(r + j, nr) for j in range(nr)]
    side = r + 1 - 2 * lax.rem(r, 2)
    over = lax.rem(r + 2, nr)
    corner = nr - 1 - r
    other = 1 - t

    def remote(src, dst, ss, rs, dev):
        return pltpu.make_async_remote_copy(
            src_ref=src,
            dst_ref=dst,
            send_sem=ss,
            recv_sem=rs,
            device_id=dev,
            device_id_type=pl.DeviceIdType.MESH,
        )

    def slab(zz, rr):
        return pl.ds(pl.multiple_of(zz * rows + rr * part, part), part)

    def fac_copy(src):
        return pltpu.make_async_copy(
            src,
            f_ref.at[t, pl.ds(pl.multiple_of(z * rows, rows), rows)],
            local_sem.at[0],
        )

    @pl.when(t == 0)
    def _():
        fac_copy(qf_hbm).start()

    @pl.when(t == 1)
    def _():
        fac_copy(vf_hbm).start()

    wq_in = pltpu.make_async_copy(wq_hbm, wf_ref.at[:, pl.ds(0, qc)], local_sem.at[1])
    wv_in = pltpu.make_async_copy(wv_hbm, wf_ref.at[:, pl.ds(qc, cols - qc)], local_sem.at[2])
    x_in = pltpu.make_async_copy(x_hbm, x_ref, local_sem.at[3])
    cq_in = pltpu.make_async_copy(cq_hbm, cq_ref, local_sem.at[4])
    cv_in = pltpu.make_async_copy(cv_hbm, cv_ref, local_sem.at[5])
    left, right = pl.ds(0, qc), pl.ds(qc, cols - qc)
    mom = [
        pltpu.make_async_copy(src, dst.at[:, at], local_sem.at[7 + n])
        for n, (src, dst, at) in enumerate(
            (
                (q1_hbm, m1_ref, left),
                (v1_hbm, m1_ref, right),
                (q2_hbm, m2_ref, left),
                (v2_hbm, m2_ref, right),
            )
        )
    ]
    for c in [wq_in, wv_in, x_in, cq_in, cv_in] + mom:
        c.start()

    barrier = pltpu.get_barrier_semaphore()
    peers = [(z_of[k], r, t) for k in range(1, nz)]
    peers += [(z, r_of[j], t) for j in range(1, nr)]
    peers += [(z, r, other)]
    for dev in peers:
        pl.semaphore_signal(
            barrier, inc=1, device_id=dev, device_id_type=pl.DeviceIdType.MESH
        )
    pl.semaphore_wait(barrier, len(peers))

    fac_copy(qf_hbm).wait()
    sends = []
    f1 = []
    for k in range(1, nz):
        here = f_ref.at[t, slab(z, r)]
        c = remote(here, here, f1_s.at[k - 1], f1_r.at[k - 1], (z_of[k], r, t))
        c.start()
        f1.append(c)
    wq_in.wait()
    wv_in.wait()
    wb_ref[...] = wf_ref[...].astype(BF)
    order = sorted(range(1, nz), key=lambda k: min(k, nz - k))
    w1 = {}
    for k in order:
        c = remote(
            wb_ref.at[pl.ds(pl.multiple_of(r * part, part), part)],
            w_out.at[slab(z, r)],
            w1_s.at[k - 1],
            w1_r.at[k - 1],
            (z_of[k], r, t),
        )
        c.start()
        w1[k] = c
    w_own = pltpu.make_async_copy(
        wb_ref, w_out.at[pl.ds(pl.multiple_of(z * rows, rows), rows)], local_sem.at[6]
    )
    w_own.start()

    f2 = []
    for k in range(1, nz):
        f1[k - 1].wait_recv()
        there = f_ref.at[t, slab(z_from[k], r)]
        for j in range(1, nr):
            n = (k - 1) * (nr - 1) + j - 1
            c = remote(there, there, f2_s.at[n], f2_r.at[n], (z, r_of[j], t))
            c.start()
            f2.append(c)
    for c in f2:
        c.wait_recv()
    w2 = {}

    def spread(k):
        w1[k].wait_recv()
        there = w_out.at[slab(z_from[k], r)]
        for n, dev in ((0, side), (1, over)):
            c = remote(there, there, w2_s.at[k - 1, n], w2_r.at[k - 1, n], (z, dev, t))
            c.start()
            w2[k, n] = c

    def relay(k):
        for n, src, dev, at in ((0, side, over, 0), (1, over, side, half)):
            w2[k, n].wait_recv()
            there = w_out.at[slab(z_from[k], src), pl.ds(at, half)]
            c = remote(
                there, there, w2_s.at[k - 1, 2 + n], w2_r.at[k - 1, 2 + n], (z, dev, t)
            )
            c.start()
            w2[k, 2 + n] = c

    stages = [[], [], []]
    for n, k in enumerate(order):
        stages[min(n, 2)].append(k)
    x_in.wait()
    tile = tokens // 3

    @pl.loop(0, 3)
    def _(i):
        span = pl.ds(pl.multiple_of(i * tile, tile), tile)
        low_ref[t, span] = jnp.dot(
            x_ref[span, :], f_ref[t], preferred_element_type=F32
        ).astype(BF)

    lx = remote(low_ref.at[t], low_ref.at[t], tp_s.at[1], tp_r.at[1], (z, r, other))
    lx.start()
    fx = remote(f_ref.at[t], f_ref.at[t], tp_s.at[0], tp_r.at[0], (z, r, other))
    fx.start()
    for k in stages[0]:
        spread(k)
    cq_in.wait()
    cv_in.wait()
    lx.wait_recv()
    dims = (((0,), (0,)), ((), ()))
    part_ref[:, :qc] = lax.dot_general(
        low_ref[0], cq_ref[...], dims, preferred_element_type=F32
    ).astype(BF)
    part_ref[:, qc:] = lax.dot_general(
        low_ref[1], cv_ref[...], dims, preferred_element_type=F32
    ).astype(BF)

    def low_rows(rr):
        return pl.ds(pl.multiple_of(rr * own, own), own)

    rsc = []
    for j in range(1, nr):
        c = remote(
            part_ref.at[low_rows(r_of[j])],
            rs_ref.at[j - 1],
            rs_s.at[j - 1],
            rs_r.at[j - 1],
            (z, r_of[j], t),
        )
        c.start()
        rsc.append(c)

    for k in stages[0]:
        relay(k)
    for c in rsc:
        c.wait_recv()
    total = part_ref[low_rows(r), :].astype(F32)
    for j in range(1, nr):
        total = total + rs_ref[j - 1].astype(F32)
    share = own // nz
    scatter = share % 16 == 0
    zc = []
    if scatter:
        zg_ref[...] = total.astype(BF)
    else:
        z_ref[z] = total.astype(BF)

    def z_rows(zz):
        return pl.ds(pl.multiple_of(zz * share, share), share)

    for k in range(1, nz):
        src = zg_ref.at[z_rows(z_of[k])] if scatter else z_ref.at[z]
        c = remote(src, z_ref.at[z], zs_s.at[k - 1], zs_r.at[k - 1], (z_of[k], r, t))
        c.start()
        zc.append(c)
    if scatter:
        z_ref[z] = zg_ref[z_rows(z), :]
    for k in stages[1]:
        spread(k)
    for c in zc:
        c.wait_recv()
    proj = z_ref[0].astype(F32)
    for k in range(1, nz):
        proj = proj + z_ref[k].astype(F32)
    gc = []
    if scatter:
        for c in zc:
            c.wait_send()
        zh = zh_ref
        zh[z_rows(z), :] = proj.astype(BF)
        for k in range(1, nz):
            here = zh.at[z_rows(z)]
            c = remote(here, here, zg_s.at[k - 1], zg_r.at[k - 1], (z_of[k], r, t))
            c.start()
            gc.append(c)
    for k in stages[1]:
        relay(k)
    for k in stages[2]:
        spread(k)
    for c in mom:
        c.wait()
    if scatter:
        for c in gc:
            c.wait_recv()
        proj = zh[...].astype(F32)
    proj_out[...] = proj
    _, _, ratio = moments(proj, m1_ref[...], m2_ref[...])
    ratio_ref[low_rows(r), :] = ratio.astype(BF)
    agc = []
    for j in range(1, nr):
        here = ratio_ref.at[low_rows(r)]
        c = remote(here, here, ag_s.at[j - 1], ag_r.at[j - 1], (z, r_of[j], t))
        c.start()
        agc.append(c)
    for k in stages[2]:
        relay(k)
    fx.wait_recv()
    for c in agc:
        c.wait_recv()
    step = min(256, width)

    def squares(i, acc):
        span = pl.ds(pl.multiple_of(i * step, step), step)
        a = jnp.dot(f_ref[0, span], ratio_ref[:, :qc], preferred_element_type=F32)
        b = jnp.dot(f_ref[1, span], ratio_ref[:, qc:], preferred_element_type=F32)
        a = jnp.sum(a * a, axis=0, keepdims=True)
        b = jnp.sum(b * b, axis=0, keepdims=True)
        return (acc[0] + a, acc[1] + b)

    qs, vs = lax.fori_loop(
        0,
        width // step,
        squares,
        (jnp.zeros((1, qc), F32), jnp.zeros((1, cols - qc), F32)),
    )
    qs = jnp.sum(qs, axis=1, keepdims=True)
    vs = jnp.sum(vs, axis=1, keepdims=True)
    row = lax.broadcasted_iota(jnp.int32, sq_ref.shape[1:], 0)
    sq_ref[t] = jnp.where(row == 0, qs / (width * qc * 2), vs / (width * (cols - qc) * 2))
    sx = remote(sq_ref.at[t], sq_ref.at[t], tp_s.at[2], tp_r.at[2], (z, r, other))
    sx.start()
    sx.wait_recv()
    scale_out[...] = lax.rsqrt(sq_ref[0] + sq_ref[1] + EPS_NORM)
    for k in range(1, nz):
        w2[k, 2].wait_recv()
        w2[k, 3].wait_recv()
    for c in f1 + list(w1.values()) + f2 + rsc + ([] if scatter else zc) + gc + agc + [fx, lx, sx] + list(w2.values()):
        c.wait_send()
    w_own.wait()


def run_exchange(nz, nr, x, cq, cv, wq, wv, qf, vf, q1, q2, v1, v2):
    tokens, width = x.shape
    qc = cq.shape[1]
    cols = qc + cv.shape[1]
    rows, rank = qf.shape
    own = rank // nr
    share = own // nz if (own // nz) % 16 == 0 else own
    any_spec = pl.BlockSpec(memory_space=pltpu.HBM)
    vmem = pl.BlockSpec(memory_space=pltpu.VMEM)
    dma = pltpu.SemaphoreType.DMA
    shape = jax.ShapeDtypeStruct
    return pl.pallas_call(
        functools.partial(exchange, nz, nr),
        out_shape=(
            shape((width, cols), BF),
            shape((2, width, rank), BF),
            shape((rank, cols), BF),
            shape((own, cols), F32),
            shape((8, 128), F32),
        ),
        in_specs=[any_spec] * 11,
        out_specs=(any_spec, vmem, vmem, vmem, vmem),
        scratch_shapes=[
            pltpu.VMEM((tokens, width), BF),
            pltpu.VMEM(cq.shape, BF),
            pltpu.VMEM(cv.shape, BF),
            pltpu.VMEM((rows, cols), F32),
            pltpu.VMEM((rows, cols), BF),
            pltpu.VMEM((2, tokens, rank), BF),
            pltpu.VMEM((rank, cols), BF),
            pltpu.VMEM((nr - 1, own, cols), BF),
            pltpu.VMEM((nz, share, cols), BF),
            pltpu.VMEM((own, cols), BF),
            pltpu.VMEM((own, cols), BF),
            pltpu.VMEM((own, cols), F32),
            pltpu.VMEM((own, cols), F32),
            pltpu.VMEM((2, 8, 128), F32),
            dma((11,)),
            dma((nz - 1,)),
            dma((nz - 1,)),
            dma((nz - 1,)),
            dma((nz - 1,)),
            dma(((nz - 1) * (nr - 1),)),
            dma(((nz - 1) * (nr - 1),)),
            dma((nz - 1, 4)),
            dma((nz - 1, 4)),
            dma((nr - 1,)),
            dma((nr - 1,)),
            dma((nz - 1,)),
            dma((nz - 1,)),
            dma((nz - 1,)),
            dma((nz - 1,)),
            dma((nr - 1,)),
            dma((nr - 1,)),
            dma((3,)),
            dma((3,)),
        ],
        compiler_params=pltpu.CompilerParams(
            collective_id=0, has_side_effects=True, vmem_limit_bytes=60 * 1024 * 1024
        ),
    )(x, cq, cv, wq, wv, qf, vf, q1, q2, v1, v2)


def finish(
    f_ref,
    ratio_ref,
    scale_ref,
    w_ref,
    wq_ref,
    wv_ref,
    qf_ref,
    vf_ref,
    proj_ref,
    q1_ref,
    q2_ref,
    v1_ref,
    v2_ref,
    qd_out,
    vd_out,
    qm_out,
    vm_out,
    q1_out,
    q2_out,
    v1_out,
    v2_out,
    qcopy_out,
    vcopy_out,
):
    qc = wq_ref.shape[1]
    sets = (
        (0, pl.ds(0, qc), wq_ref, qf_ref, q1_ref, q2_ref, qd_out, qm_out, q1_out, q2_out, qcopy_out),
        (
            1,
            pl.ds(qc, wv_ref.shape[1]),
            wv_ref,
            vf_ref,
            v1_ref,
            v2_ref,
            vd_out,
            vm_out,
            v1_out,
            v2_out,
            vcopy_out,
        ),
    )
    for n, at, w, f, m1, m2, d_out, m_out, m1_out, m2_out, c_out in sets:
        scale = scale_ref[n : n + 1, 0:1]
        ratio = ratio_ref[:, at]
        raw = jnp.dot(f_ref[n], ratio, preferred_element_type=F32)
        c_out[...] = (w_ref[:, at].astype(F32) - RATE * (raw * scale)).astype(BF)
        d = jnp.dot(f[...], ratio, preferred_element_type=F32) * scale
        d_out[...] = d
        m_out[...] = w[...] - RATE * d
        m1_out[...], m2_out[...], _ = moments(proj_ref[:, at], m1[...], m2[...])


def run_finish(factors, ratio, scale, weights, wq, wv, qf, vf, proj, q1, q2, v1, v2):
    rows, qc = wq.shape
    vc = wv.shape[1]
    width, cols = weights.shape
    rank, own = qf.shape[1], q1.shape[0]
    steps = 8 if rows % 128 == 0 else 4

    def tall(n, c):
        return pl.BlockSpec((n // steps, c), lambda i: (i, 0))

    def whole(a):
        return pl.BlockSpec(a.shape, lambda i: (0,) * a.ndim)

    shape = jax.ShapeDtypeStruct
    return pl.pallas_call(
        finish,
        grid=(steps,),
        in_specs=[
            pl.BlockSpec((2, width // steps, rank), lambda i: (0, i, 0)),
            whole(ratio),
            whole(scale),
            tall(width, cols),
            tall(rows, qc),
            tall(rows, vc),
            tall(rows, rank),
            tall(rows, rank),
            tall(own, cols),
            tall(own, qc),
            tall(own, qc),
            tall(own, vc),
            tall(own, vc),
        ],
        out_specs=[
            tall(rows, qc),
            tall(rows, vc),
            tall(rows, qc),
            tall(rows, vc),
            tall(own, qc),
            tall(own, qc),
            tall(own, vc),
            tall(own, vc),
            tall(width, qc),
            tall(width, vc),
        ],
        out_shape=[
            shape((rows, qc), F32),
            shape((rows, vc), F32),
            shape((rows, qc), F32),
            shape((rows, vc), F32),
            shape((own, qc), F32),
            shape((own, qc), F32),
            shape((own, vc), F32),
            shape((own, vc), F32),
            shape((width, qc), BF),
            shape((width, vc), BF),
        ],
        compiler_params=pltpu.CompilerParams(vmem_limit_bytes=60 * 1024 * 1024),
    )(factors, ratio, scale, weights, wq, wv, qf, vf, proj, q1, q2, v1, v2)


def line_exchange(
    quarter,
    chunks,
    rests,
    x_hbm,
    cq_hbm,
    cv_hbm,
    wq_hbm,
    wv_hbm,
    qf_hbm,
    vf_hbm,
    q1_hbm,
    q2_hbm,
    v1_hbm,
    v2_hbm,
    w_ref,
    f_ref,
    ratio_ref,
    wf_ref,
    m1_out,
    m2_out,
    scale_out,
    d_ref,
    x_ref,
    cq_ref,
    cv_ref,
    acc_ref,
    low_ref,
    part_ref,
    ra_ref,
    tb_ref,
    rb_ref,
    zs_ref,
    zo_ref,
    z_ref,
    zh_ref,
    m1_ref,
    m2_ref,
    g_ref,
    sq_ref,
    local_sem,
    out_s,
    fz_r,
    fp_r,
    wz_r,
    wp_r,
    wc_r,
    ra_r,
    rb_r,
    zs_r,
    zg_r,
    ag_r,
    ac_r,
    tp_s,
    tp_r,
):
    z = lax.axis_index("fs")
    r = lax.axis_index("rep")
    t = lax.axis_index("tp")
    nz, nr = 4, 4
    rows = qf_hbm.shape[0]
    part = rows // nr
    qc = cq_ref.shape[1]
    width, cols = w_ref.shape
    half = cols // 2
    rank = low_ref.shape[2]
    own = rank // nr
    share = own // nz
    tokens = x_ref.shape[0]
    px, py = lax.rem(r, 2), lax.div(r, 2)
    side = r + 1 - 2 * px
    over = lax.rem(r + 2, nr)
    corner = nr - 1 - r
    other = 1 - t
    upper = lax.div(z, 2)
    near = z + 1 - 2 * lax.rem(z, 2)
    mid = 2 - upper
    far = 3 - 3 * upper
    planes = [near, mid, far]
    inner = jnp.logical_and(z > 0, z < nz - 1)
    groups = {"plane": 0, "line": 1, "inner": 2}
    sent = dict.fromkeys(groups, 0)

    def remote(src, dst, ss, rs, dev):
        return pltpu.make_async_remote_copy(
            src_ref=src,
            dst_ref=dst,
            send_sem=ss,
            recv_sem=rs,
            device_id=dev,
            device_id_type=pl.DeviceIdType.MESH,
        )

    def count(ref, group):
        sent[group] += ref.size * ref.dtype.itemsize

    def send(src, dst, rs, dev, group="plane"):
        count(dst, group)
        remote(src, dst, out_s.at[groups[group]], rs, dev).start()

    def send_pair(src, dst, n):
        remote(src, dst, tp_s.at[n], tp_r.at[n], (z, r, other)).start()

    def send_inner(ref, rs, dev, wait=None):
        count(ref, "inner")

        @pl.when(inner)
        def _():
            if wait is not None:
                arrive(ref, wait)
            remote(ref, ref, out_s.at[2], rs, dev).start()

    def drain(group):
        size, line = sent[group], cols * 2
        while size:
            span = pl.ds(0, min(size // line, width))
            size -= min(size // line, width) * line
            ref = w_ref.at[span]
            remote(ref, ref, out_s.at[groups[group]], tp_r.at[0], (z, r, other)).wait_send()

    def arrive(dst, rs):
        remote(dst, dst, tp_s.at[0], rs, (z, r, other)).wait_recv()

    def at(start, size, step):
        return pl.ds(pl.multiple_of(start, step), size)

    def fac_copy(src):
        return pltpu.make_async_copy(src, f_ref.at[t, at(z * rows, rows, rows)], local_sem.at[0])

    @pl.when(t == 0)
    def _():
        fac_copy(qf_hbm).start()

    @pl.when(t == 1)
    def _():
        fac_copy(vf_hbm).start()

    left, right = pl.ds(0, qc), pl.ds(qc, cols - qc)
    x_in = pltpu.make_async_copy(x_hbm, x_ref, local_sem.at[1])
    cq_in = pltpu.make_async_copy(cq_hbm, cq_ref, local_sem.at[2])
    cv_in = pltpu.make_async_copy(cv_hbm, cv_ref, local_sem.at[3])
    pltpu.make_async_copy(wq_hbm, wf_ref.at[:, left], local_sem.at[4]).start()
    pltpu.make_async_copy(wv_hbm, wf_ref.at[:, right], local_sem.at[4]).start()
    for c in (x_in, cq_in, cv_in):
        c.start()
    for n, src, dst, span in (
        (5, q1_hbm, m1_ref, left),
        (5, v1_hbm, m1_ref, right),
        (6, q2_hbm, m2_ref, left),
        (6, v2_hbm, m2_ref, right),
    ):
        pltpu.make_async_copy(src, dst.at[:, span], local_sem.at[n]).start()

    def loaded(ref, n):
        pltpu.make_async_copy(ref, ref, local_sem.at[n]).wait()

    barrier = pltpu.get_barrier_semaphore()
    peers = [(p, r, t) for p in planes]
    peers += [(z, p, t) for p in (side, over, corner)]
    peers += [(z, r, other)]
    for dev in peers:
        pl.semaphore_signal(
            barrier, inc=1, device_id=dev, device_id_type=pl.DeviceIdType.MESH
        )
    pl.semaphore_wait(barrier, len(peers))

    class Spread:
        def __init__(self, view, split, rs, rest):
            self.view, self.split, self.rs, self.rest = view, split, rs, rest

        def start(self):
            here = self.view(r)
            for n, dev in ((0, side), (1, over)):
                send(here, here, self.rs.at[n], (z, dev, t))

        def relay(self):
            for n, src, dev in ((0, side, over), (1, over, side)):
                whole = self.view(src)
                arrive(whole, self.rs.at[n])
                there = self.split(whole, n)
                send(there, there, self.rest, (z, dev, t))

    def halves(ref, n):
        return ref.at[:, pl.ds(n * half, half)]

    def fac_rows(plane, rr):
        return f_ref.at[t, at(plane * rows + rr * part, part, part)]

    fac_copy(qf_hbm).wait()
    for i, p in enumerate(planes):
        here = fac_rows(z, r)
        send(here, here, fz_r.at[z], (p, r, t), "line")

    spans = [(n, s, True) for n, s in zip([sum(chunks[:c]) for c in range(len(chunks))], chunks)]
    spans += [(n, s, False) for n, s in zip([sum(rests[:c]) for c in range(len(rests))], rests)]

    def w_rows(plane, rr, c):
        begin, size, split = spans[c]
        begin = plane * rows + begin + (rr * quarter if split else nr * quarter)
        return w_ref.at[at(begin, size, 8)]

    def w_own(c):
        here = w_rows(z, r, c)
        send(here, here, wz_r.at[z, c], (near, r, t), "line")
        send_inner(here, wz_r.at[z, c], (mid, r, t))

    def w_pass(i, c):
        sem = wz_r.at[planes[i], c]
        send_inner(w_rows(planes[i], r, c), sem, (near if i else mid, r, t), sem)

    def w_land(i, c):
        @pl.when(jnp.logical_not(inner))
        def _():
            arrive(w_rows(planes[i], r, c), wz_r.at[planes[i], c])

    def w_start(i, c):
        w_land(i, c)
        w_in[i][c].start()

    w_in = [
        [
            Spread(functools.partial(lambda p, c, rr: w_rows(p, rr, c), p, c), halves, wp_r.at[i, c], wc_r.at[i])
            for c in range(len(chunks))
        ]
        for i, p in enumerate(planes)
    ]

    def low_add(plane, first):
        tile = tokens // 3

        @pl.loop(0, 3)
        def _(n):
            span = at(n * tile, tile, 16)
            a = jnp.dot(
                x_ref[span, at(plane * rows, rows, rows)],
                f_ref[t, at(plane * rows, rows, rows)],
                preferred_element_type=F32,
            )
            acc_ref[span, :] = a if first else acc_ref[span, :] + a

    fac = [
        Spread(
            functools.partial(fac_rows, p),
            lambda ref, n: ref.at[pl.ds(n * (part // 2), part // 2)],
            fp_r.at[i],
            fp_r.at[i, 2],
        )
        for i, p in enumerate(planes)
    ]

    def fac_start(i):
        arrive(fac_rows(planes[i], r), fz_r.at[planes[i]])
        fac[i].start()

    def fac_finish(i):
        arrive(fac_rows(planes[i], corner), fp_r.at[i, 2])
        low_add(planes[i], False)

    def share_rows(plane):
        return at(plane * share, share, share)

    def low_rows(rr, plane):
        return at(rr * own + plane * share, share, share)

    lo, hi = pl.ds(0, half), pl.ds(half, half)
    order = [far, mid, near, z]

    def sum_start(i):
        span = share_rows(order[i])
        for n, src, dev in (
            (0, part_ref.at[:, 1 - px, span, lo], side),
            (1, part_ref.at[1 - py, :, span, hi], over),
        ):
            send(src, ra_ref.at[n, :, span], ra_r.at[i, n], (z, dev, t))

    def sum_relay(i):
        span = share_rows(order[i])
        for n in range(2):
            arrive(ra_ref.at[n, :, span], ra_r.at[i, n])
        for n, mine, theirs, dev in (
            (0, part_ref[1 - py, px, span, lo], ra_ref[0, 1 - py, span, :], over),
            (1, part_ref[py, 1 - px, span, hi], ra_ref[1, 1 - px, span, :], side),
        ):
            tb_ref[n, span, :] = (mine.astype(F32) + theirs.astype(F32)).astype(BF)
            send(tb_ref.at[n, span], rb_ref.at[n, span], rb_r.at[i, n], (z, dev, t))

    def sum_finish(i):
        span = share_rows(order[i])
        for n in range(2):
            arrive(rb_ref.at[n, span], rb_r.at[i, n])
        out = []
        for n, cut, theirs in ((0, lo, ra_ref[0, py, span, :]), (1, hi, ra_ref[1, px, span, :])):
            a = part_ref[py, px, span, cut].astype(F32) + theirs.astype(F32)
            out.append(a + rb_ref[n, span, :].astype(F32))
        if i == 3:
            zo_ref[:, lo], zo_ref[:, hi] = out
        else:
            zs_ref[span, lo] = out[0].astype(BF)
            zs_ref[span, hi] = out[1].astype(BF)
            send(zs_ref.at[span], z_ref.at[z], zs_r.at[z], (order[i], r, t), "line")

    def line_sum():
        proj = zo_ref[...]
        for p in planes:
            arrive(z_ref.at[p], zs_r.at[p])
            proj = proj + z_ref[p].astype(F32)
        here = zh_ref.at[share_rows(z)]
        zh_ref[share_rows(z), :] = proj.astype(BF)
        for p in (far, mid, near):
            send(here, here, zg_r.at[z], (p, r, t), "line")

    ratio_in = [
        Spread(
            functools.partial(lambda p, rr: ratio_ref.at[low_rows(rr, p)], p),
            halves,
            ag_r.at[i],
            ac_r.at[0],
        )
        for i, p in enumerate([z] + planes)
    ]

    def ratio_start(i):
        p = z
        if i:
            p = planes[i - 1]
            arrive(zh_ref.at[share_rows(p)], zg_r.at[p])
        span = share_rows(p)
        first, second, ratio = moments(
            zh_ref[span, :].astype(F32), m1_ref[span, :], m2_ref[span, :]
        )
        m1_out[span, :] = first
        m2_out[span, :] = second
        ratio_ref[low_rows(r, p), :] = ratio.astype(BF)
        ratio_in[i].start()

    dims = (((0,), (0,)), ((), ()))

    def low_parts():
        for n, c_ref, span in ((0, cq_ref, slice(0, qc)), (1, cv_ref, slice(qc, cols))):
            a = lax.dot_general(
                low_ref[n], c_ref[...], dims, preferred_element_type=F32
            ).astype(BF)
            for k in range(nr):
                part_ref[k // 2, k % 2, :, span] = a[k * own : (k + 1) * own]

    def gram():
        arrive(f_ref.at[other], tp_r.at[0])
        for n in range(2):
            g = lax.dot_general(f_ref[n], f_ref[n], dims, preferred_element_type=F32)
            top = g.astype(BF)
            g_ref[n, 0] = top
            g_ref[n, 1] = (g - top.astype(F32)).astype(BF)

    def squares(n, span):
        ratio = ratio_ref[:, span]
        a = jnp.dot(g_ref[n, 0], ratio, preferred_element_type=F32)
        a = a + jnp.dot(g_ref[n, 1], ratio, preferred_element_type=F32)
        a = jnp.sum(a * ratio.astype(F32), axis=0, keepdims=True)
        return jnp.sum(a, axis=1, keepdims=True)

    def own_rows():
        tile = rows // 8

        @pl.loop(0, 8)
        def _(i):
            mine = at(z * rows + i * tile, tile, tile)
            span = at(i * tile, tile, tile)
            for n, cut in ((0, slice(0, qc)), (1, slice(qc, cols))):
                d = jnp.dot(f_ref[n, mine], ratio_ref[:, cut], preferred_element_type=F32)
                d = d * scale_out[n : n + 1, 0:1]
                d_ref[span, cut] = d
                wf_ref[span, cut] = wf_ref[span, cut] - RATE * d

    loaded(wf_ref, 4)
    w_ref[at(z * rows, rows, rows), :] = wf_ref[...].astype(BF)
    x_in.wait()
    low_add(z, True)
    fac_start(0)
    w_own(0)
    w_own(1)
    fac_start(1)
    fac_start(2)
    fac[0].relay()
    fac[1].relay()
    w_pass(0, 0)
    w_pass(1, 0)
    fac[2].relay()
    w_start(0, 0)
    fac_finish(0)
    w_pass(0, 1)
    w_pass(1, 1)
    w_start(0, 1)
    fac_finish(1)
    fac_finish(2)
    low_ref[t] = acc_ref[...].astype(BF)
    send_pair(low_ref.at[t], low_ref.at[t], 1)
    send_pair(f_ref.at[t], f_ref.at[t], 0)
    w_pass(2, 0)
    cq_in.wait()
    cv_in.wait()
    arrive(low_ref.at[other], tp_r.at[1])
    low_parts()
    for i in range(4):
        sum_start(i)
    w_in[0][0].relay()
    w_in[0][1].relay()
    w_pass(2, 1)
    w_own(2)
    sum_relay(0)
    sum_relay(1)
    sum_relay(2)
    sum_relay(3)
    w_start(1, 0)
    w_pass(0, 2)
    w_pass(1, 2)
    sum_finish(0)
    sum_finish(1)
    sum_finish(2)
    sum_finish(3)
    w_start(1, 1)
    w_pass(2, 2)
    loaded(m1_ref, 5)
    loaded(m2_ref, 6)
    line_sum()
    w_in[1][0].relay()
    ratio_start(0)
    w_start(2, 0)
    ratio_start(1)
    ratio_start(2)
    ratio_start(3)
    w_own(3)
    w_in[1][1].relay()
    w_start(2, 1)
    ratio_in[0].relay()
    ratio_in[1].relay()
    ratio_in[2].relay()
    ratio_in[3].relay()
    w_pass(0, 3)
    w_pass(1, 3)
    gram()
    w_in[2][0].relay()
    w_pass(2, 3)
    arrive(ratio_ref.at[at(corner * own, own, own)], ac_r.at[0])
    qs = squares(0, slice(0, qc)) / (width * qc * 2)
    vs = squares(1, slice(qc, cols)) / (width * (cols - qc) * 2)
    line = lax.broadcasted_iota(jnp.int32, sq_ref.shape[1:], 0)
    sq_ref[t] = jnp.where(line == 0, qs, vs)
    send_pair(sq_ref.at[t], sq_ref.at[t], 2)
    w_in[2][1].relay()
    arrive(sq_ref.at[other], tp_r.at[2])
    scale_out[...] = lax.rsqrt(jnp.maximum(sq_ref[0] + sq_ref[1], 0.0) + EPS_NORM)
    own_rows()
    for c in range(len(chunks), len(spans)):
        for i in range(3):
            w_land(i, c)
    for i in range(3):
        arrive(w_ref.at[at(planes[i] * rows + corner * quarter, quarter, 8)], wc_r.at[i])
    for n, ref in enumerate((f_ref.at[t], low_ref.at[t], sq_ref.at[t])):
        remote(ref, ref, tp_s.at[n], tp_r.at[n], (z, r, other)).wait_send()
    drain("plane")
    drain("line")

    @pl.when(inner)
    def _():
        drain("inner")


def run_line_exchange(x, cq, cv, wq, wv, qf, vf, q1, q2, v1, v2):
    tokens, width = x.shape
    qc = cq.shape[1]
    cols = qc + cv.shape[1]
    rows, rank = qf.shape
    own = rank // 4
    share = own // 4
    unit = rows // 64
    quarter = 13 * unit
    chunks = (7 * unit, 6 * unit)
    rests = (6 * unit, 6 * unit)
    any_spec = pl.BlockSpec(memory_space=pltpu.HBM)
    vmem = pl.BlockSpec(memory_space=pltpu.VMEM)
    dma = pltpu.SemaphoreType.DMA
    n = len(chunks)
    m = n + len(rests)
    return pl.pallas_call(
        functools.partial(line_exchange, quarter, chunks, rests),
        out_shape=(
            pltpu.VMEM((width, cols), BF),
            pltpu.VMEM((2, width, rank), BF),
            pltpu.VMEM((rank, cols), BF),
            pltpu.VMEM((rows, cols), F32),
            pltpu.VMEM((own, cols), F32),
            pltpu.VMEM((own, cols), F32),
            pltpu.VMEM((8, 128), F32),
            pltpu.VMEM((rows, cols), F32),
        ),
        in_specs=[any_spec] * 11,
        out_specs=(vmem,) * 8,
        scratch_shapes=[
            pltpu.VMEM((tokens, width), BF),
            pltpu.VMEM(cq.shape, BF),
            pltpu.VMEM(cv.shape, BF),
            pltpu.VMEM((tokens, rank), F32),
            pltpu.VMEM((2, tokens, rank), BF),
            pltpu.VMEM((2, 2, own, cols), BF),
            pltpu.VMEM((2, 2, own, cols // 2), BF),
            pltpu.VMEM((2, own, cols // 2), BF),
            pltpu.VMEM((2, own, cols // 2), BF),
            pltpu.VMEM((own, cols), BF),
            pltpu.VMEM((share, cols), F32),
            pltpu.VMEM((4, share, cols), BF),
            pltpu.VMEM((own, cols), BF),
            pltpu.VMEM((own, cols), F32),
            pltpu.VMEM((own, cols), F32),
            pltpu.VMEM((2, 2, rank, rank), BF),
            pltpu.VMEM((2, 8, 128), F32),
            dma((7,)),
            dma((3,)),
            dma((4,)),
            dma((3, 3)),
            dma((4, m)),
            dma((3, n, 2)),
            dma((3,)),
            dma((4, 2)),
            dma((4, 2)),
            dma((4,)),
            dma((4,)),
            dma((4, 2)),
            dma((1,)),
            dma((3,)),
            dma((3,)),
        ],
        compiler_params=pltpu.CompilerParams(
            collective_id=0, has_side_effects=True, vmem_limit_bytes=48 * 1024 * 1024
        ),
    )(x, cq, cv, wq, wv, qf, vf, q1, q2, v1, v2)


def line_finish(
    steps,
    w_ref,
    f_ref,
    ratio_ref,
    m_ref,
    m1_ref,
    m2_ref,
    scale_ref,
    d_ref,
    qd_out,
    vd_out,
    qm_out,
    vm_out,
    q1_out,
    q2_out,
    v1_out,
    v2_out,
    qcopy_out,
    vcopy_out,
    c_ref,
    sem,
):
    width, cols = w_ref.shape
    qc = qd_out.shape[1]
    left, right = pl.ds(0, qc), pl.ds(qc, cols - qc)
    outs = (
        (d_ref, left, qd_out),
        (d_ref, right, vd_out),
        (m_ref, left, qm_out),
        (m_ref, right, vm_out),
        (m1_ref, left, q1_out),
        (m1_ref, right, v1_out),
        (m2_ref, left, q2_out),
        (m2_ref, right, v2_out),
    )
    copies = [
        pltpu.make_async_copy(src.at[:, cut], dst, sem.at[n])
        for n, (src, cut, dst) in enumerate(outs)
    ]
    for c in copies:
        c.start()
    tall = width // steps

    @pl.loop(0, steps)
    def _(i):
        span = pl.ds(pl.multiple_of(i * tall, tall), tall)
        for n, cut, dst in ((0, left, qcopy_out), (1, right, vcopy_out)):
            raw = jnp.dot(f_ref[n, span], ratio_ref[:, cut], preferred_element_type=F32)
            raw = raw * scale_ref[n : n + 1, 0:1]
            c_ref[span, cut] = (w_ref[span, cut].astype(F32) - RATE * raw).astype(BF)
            pltpu.make_async_copy(c_ref.at[span, cut], dst.at[span], sem.at[8 + n]).start()

    for c in copies:
        c.wait()
    for n, cut, dst in ((0, left, qcopy_out), (1, right, vcopy_out)):
        pltpu.make_async_copy(c_ref.at[:, cut], dst, sem.at[8 + n]).wait()


def run_line_finish(weights, factors, ratio, masters, m1, m2, scale, directions, qc):
    rows, cols = masters.shape
    vc = cols - qc
    width, own = weights.shape[0], m1.shape[0]
    vmem = pl.BlockSpec(memory_space=pltpu.VMEM)
    shape = jax.ShapeDtypeStruct
    return pl.pallas_call(
        functools.partial(line_finish, 8),
        in_specs=[vmem] * 8,
        out_specs=[pl.BlockSpec(memory_space=pltpu.HBM)] * 10,
        out_shape=[
            shape((rows, qc), F32),
            shape((rows, vc), F32),
            shape((rows, qc), F32),
            shape((rows, vc), F32),
            shape((own, qc), F32),
            shape((own, qc), F32),
            shape((own, vc), F32),
            shape((own, vc), F32),
            shape((width, qc), BF),
            shape((width, vc), BF),
        ],
        scratch_shapes=[pltpu.VMEM((width, cols), BF), pltpu.SemaphoreType.DMA((10,))],
        compiler_params=pltpu.CompilerParams(vmem_limit_bytes=16 * 1024 * 1024),
    )(weights, factors, ratio, masters, m1, m2, scale, directions)


def suits_line(nz, nr, qf, cq, cv):
    rows, rank = qf.shape
    cols = cq.shape[1] + cv.shape[1]
    return nz == 4 and nr == 4 and rows % 512 == 0 and rank % 256 == 0 and cols % 256 == 0


def local(nz, nr, *args):
    _, cq, cv, wq, wv, qf, vf, q1, q2, v1, v2 = args
    if suits_line(nz, nr, qf, cq, cv):
        return tuple(run_line_finish(*run_line_exchange(*args), cq.shape[1]))
    weights, factors, ratio, proj, scale = run_exchange(nz, nr, *args)
    return tuple(
        run_finish(factors, ratio, scale, weights, wq, wv, qf, vf, proj, q1, q2, v1, v2)
    )


def solution(mesh):
    return jax.shard_map(
        functools.partial(local, mesh.shape["fs"], mesh.shape["rep"]),
        mesh=mesh,
        in_specs=(
            P(("fs", "rep"), None),
            P(("fs", "rep"), "tp"),
            P(("fs", "rep"), "tp"),
            P("fs", "tp"),
            P("fs", "tp"),
            P("fs", None),
            P("fs", None),
            P("rep", "tp"),
            P("rep", "tp"),
            P("rep", "tp"),
            P("rep", "tp"),
        ),
        out_specs=(
            P("fs", "tp"),
            P("fs", "tp"),
            P("fs", "tp"),
            P("fs", "tp"),
            P("rep", "tp"),
            P("rep", "tp"),
            P("rep", "tp"),
            P("rep", "tp"),
            P(None, "tp"),
            P(None, "tp"),
        ),
        check_vma=False,
    )
```

```python
import functools

import jax
import jax.numpy as jnp
from jax import lax
from jax.experimental import pallas as pl
from jax.experimental.pallas import tpu as pltpu
from jax.sharding import PartitionSpec as P

BETA_ONE = 0.8
BETA_TWO = 0.9
EPS_RATIO = 1e-08
EPS_NORM = 1e-06
RATE = 0.02
BF = jnp.bfloat16
F32 = jnp.float32


def moments(projected, first, second):
    first_new = BETA_ONE * first + (1.0 - BETA_ONE) * projected
    second_new = BETA_TWO * second + (1.0 - BETA_TWO) * projected * projected
    ratio = first_new / (jnp.sqrt(second_new) + EPS_RATIO)
    return (first_new, second_new, ratio)


def exchange(
    nz,
    nr,
    x_hbm,
    cq_hbm,
    cv_hbm,
    wq_hbm,
    wv_hbm,
    qf_hbm,
    vf_hbm,
    q1_hbm,
    q2_hbm,
    v1_hbm,
    v2_hbm,
    w_out,
    f_ref,
    ratio_ref,
    proj_out,
    scale_out,
    x_ref,
    cq_ref,
    cv_ref,
    wf_ref,
    wb_ref,
    low_ref,
    part_ref,
    rs_ref,
    z_ref,
    zg_ref,
    zh_ref,
    m1_ref,
    m2_ref,
    sq_ref,
    local_sem,
    f1_s,
    f1_r,
    w1_s,
    w1_r,
    f2_s,
    f2_r,
    w2_s,
    w2_r,
    rs_s,
    rs_r,
    zs_s,
    zs_r,
    zg_s,
    zg_r,
    ag_s,
    ag_r,
    tp_s,
    tp_r,
):
    z = lax.axis_index("fs")
    r = lax.axis_index("rep")
    t = lax.axis_index("tp")
    rows = qf_hbm.shape[0]
    part = rows // nr
    qc = cq_ref.shape[1]
    cols = w_out.shape[1]
    half = cols // 2
    width = w_out.shape[0]
    rank = low_ref.shape[2]
    own = rank // nr
    tokens = x_ref.shape[0]
    z_of = [lax.rem(z + k, nz) for k in range(nz)]
    z_from = [lax.rem(z + nz - k, nz) for k in range(nz)]
    r_of = [lax.rem(r + j, nr) for j in range(nr)]
    side = r + 1 - 2 * lax.rem(r, 2)
    over = lax.rem(r + 2, nr)
    corner = nr - 1 - r
    other = 1 - t

    def remote(src, dst, ss, rs, dev):
        return pltpu.make_async_remote_copy(
            src_ref=src,
            dst_ref=dst,
            send_sem=ss,
            recv_sem=rs,
            device_id=dev,
            device_id_type=pl.DeviceIdType.MESH,
        )

    def slab(zz, rr):
        return pl.ds(pl.multiple_of(zz * rows + rr * part, part), part)

    def fac_copy(src):
        return pltpu.make_async_copy(
            src,
            f_ref.at[t, pl.ds(pl.multiple_of(z * rows, rows), rows)],
            local_sem.at[0],
        )

    @pl.when(t == 0)
    def _():
        fac_copy(qf_hbm).start()

    @pl.when(t == 1)
    def _():
        fac_copy(vf_hbm).start()

    wq_in = pltpu.make_async_copy(wq_hbm, wf_ref.at[:, pl.ds(0, qc)], local_sem.at[1])
    wv_in = pltpu.make_async_copy(wv_hbm, wf_ref.at[:, pl.ds(qc, cols - qc)], local_sem.at[2])
    x_in = pltpu.make_async_copy(x_hbm, x_ref, local_sem.at[3])
    cq_in = pltpu.make_async_copy(cq_hbm, cq_ref, local_sem.at[4])
    cv_in = pltpu.make_async_copy(cv_hbm, cv_ref, local_sem.at[5])
    left, right = pl.ds(0, qc), pl.ds(qc, cols - qc)
    mom = [
        pltpu.make_async_copy(src, dst.at[:, at], local_sem.at[7 + n])
        for n, (src, dst, at) in enumerate(
            (
                (q1_hbm, m1_ref, left),
                (v1_hbm, m1_ref, right),
                (q2_hbm, m2_ref, left),
                (v2_hbm, m2_ref, right),
            )
        )
    ]
    for c in [wq_in, wv_in, x_in, cq_in, cv_in] + mom:
        c.start()

    barrier = pltpu.get_barrier_semaphore()
    peers = [(z_of[k], r, t) for k in range(1, nz)]
    peers += [(z, r_of[j], t) for j in range(1, nr)]
    peers += [(z, r, other)]
    for dev in peers:
        pl.semaphore_signal(
            barrier, inc=1, device_id=dev, device_id_type=pl.DeviceIdType.MESH
        )
    pl.semaphore_wait(barrier, len(peers))

    fac_copy(qf_hbm).wait()
    sends = []
    f1 = []
    for k in range(1, nz):
        here = f_ref.at[t, slab(z, r)]
        c = remote(here, here, f1_s.at[k - 1], f1_r.at[k - 1], (z_of[k], r, t))
        c.start()
        f1.append(c)
    wq_in.wait()
    wv_in.wait()
    wb_ref[...] = wf_ref[...].astype(BF)
    order = sorted(range(1, nz), key=lambda k: min(k, nz - k))
    w1 = {}
    for k in order:
        c = remote(
            wb_ref.at[pl.ds(pl.multiple_of(r * part, part), part)],
            w_out.at[slab(z, r)],
            w1_s.at[k - 1],
            w1_r.at[k - 1],
            (z_of[k], r, t),
        )
        c.start()
        w1[k] = c
    w_own = pltpu.make_async_copy(
        wb_ref, w_out.at[pl.ds(pl.multiple_of(z * rows, rows), rows)], local_sem.at[6]
    )
    w_own.start()

    f2 = []
    for k in range(1, nz):
        f1[k - 1].wait_recv()
        there = f_ref.at[t, slab(z_from[k], r)]
        for j in range(1, nr):
            n = (k - 1) * (nr - 1) + j - 1
            c = remote(there, there, f2_s.at[n], f2_r.at[n], (z, r_of[j], t))
            c.start()
            f2.append(c)
    for c in f2:
        c.wait_recv()
    w2 = {}

    def spread(k):
        w1[k].wait_recv()
        there = w_out.at[slab(z_from[k], r)]
        for n, dev in ((0, side), (1, over)):
            c = remote(there, there, w2_s.at[k - 1, n], w2_r.at[k - 1, n], (z, dev, t))
            c.start()
            w2[k, n] = c

    def relay(k):
        for n, src, dev, at in ((0, side, over, 0), (1, over, side, half)):
            w2[k, n].wait_recv()
            there = w_out.at[slab(z_from[k], src), pl.ds(at, half)]
            c = remote(
                there, there, w2_s.at[k - 1, 2 + n], w2_r.at[k - 1, 2 + n], (z, dev, t)
            )
            c.start()
            w2[k, 2 + n] = c

    stages = [[], [], []]
    for n, k in enumerate(order):
        stages[min(n, 2)].append(k)
    x_in.wait()
    tile = tokens // 3

    @pl.loop(0, 3)
    def _(i):
        span = pl.ds(pl.multiple_of(i * tile, tile), tile)
        low_ref[t, span] = jnp.dot(
            x_ref[span, :], f_ref[t], preferred_element_type=F32
        ).astype(BF)

    lx = remote(low_ref.at[t], low_ref.at[t], tp_s.at[1], tp_r.at[1], (z, r, other))
    lx.start()
    fx = remote(f_ref.at[t], f_ref.at[t], tp_s.at[0], tp_r.at[0], (z, r, other))
    fx.start()
    for k in stages[0]:
        spread(k)
    cq_in.wait()
    cv_in.wait()
    lx.wait_recv()
    dims = (((0,), (0,)), ((), ()))
    part_ref[:, :qc] = lax.dot_general(
        low_ref[0], cq_ref[...], dims, preferred_element_type=F32
    ).astype(BF)
    part_ref[:, qc:] = lax.dot_general(
        low_ref[1], cv_ref[...], dims, preferred_element_type=F32
    ).astype(BF)

    def low_rows(rr):
        return pl.ds(pl.multiple_of(rr * own, own), own)

    rsc = []
    for j in range(1, nr):
        c = remote(
            part_ref.at[low_rows(r_of[j])],
            rs_ref.at[j - 1],
            rs_s.at[j - 1],
            rs_r.at[j - 1],
            (z, r_of[j], t),
        )
        c.start()
        rsc.append(c)

    for k in stages[0]:
        relay(k)
    for c in rsc:
        c.wait_recv()
    total = part_ref[low_rows(r), :].astype(F32)
    for j in range(1, nr):
        total = total + rs_ref[j - 1].astype(F32)
    share = own // nz
    scatter = share % 16 == 0
    zc = []
    if scatter:
        zg_ref[...] = total.astype(BF)
    else:
        z_ref[z] = total.astype(BF)

    def z_rows(zz):
        return pl.ds(pl.multiple_of(zz * share, share), share)

    for k in range(1, nz):
        src = zg_ref.at[z_rows(z_of[k])] if scatter else z_ref.at[z]
        c = remote(src, z_ref.at[z], zs_s.at[k - 1], zs_r.at[k - 1], (z_of[k], r, t))
        c.start()
        zc.append(c)
    if scatter:
        z_ref[z] = zg_ref[z_rows(z), :]
    for k in stages[1]:
        spread(k)
    for c in zc:
        c.wait_recv()
    proj = z_ref[0].astype(F32)
    for k in range(1, nz):
        proj = proj + z_ref[k].astype(F32)
    gc = []
    if scatter:
        for c in zc:
            c.wait_send()
        zh = zh_ref
        zh[z_rows(z), :] = proj.astype(BF)
        for k in range(1, nz):
            here = zh.at[z_rows(z)]
            c = remote(here, here, zg_s.at[k - 1], zg_r.at[k - 1], (z_of[k], r, t))
            c.start()
            gc.append(c)
    for k in stages[1]:
        relay(k)
    for k in stages[2]:
        spread(k)
    for c in mom:
        c.wait()
    if scatter:
        for c in gc:
            c.wait_recv()
        proj = zh[...].astype(F32)
    proj_out[...] = proj
    _, _, ratio = moments(proj, m1_ref[...], m2_ref[...])
    ratio_ref[low_rows(r), :] = ratio.astype(BF)
    agc = []
    for j in range(1, nr):
        here = ratio_ref.at[low_rows(r)]
        c = remote(here, here, ag_s.at[j - 1], ag_r.at[j - 1], (z, r_of[j], t))
        c.start()
        agc.append(c)
    for k in stages[2]:
        relay(k)
    fx.wait_recv()
    for c in agc:
        c.wait_recv()
    step = min(256, width)

    def squares(i, acc):
        span = pl.ds(pl.multiple_of(i * step, step), step)
        a = jnp.dot(f_ref[0, span], ratio_ref[:, :qc], preferred_element_type=F32)
        b = jnp.dot(f_ref[1, span], ratio_ref[:, qc:], preferred_element_type=F32)
        a = jnp.sum(a * a, axis=0, keepdims=True)
        b = jnp.sum(b * b, axis=0, keepdims=True)
        return (acc[0] + a, acc[1] + b)

    qs, vs = lax.fori_loop(
        0,
        width // step,
        squares,
        (jnp.zeros((1, qc), F32), jnp.zeros((1, cols - qc), F32)),
    )
    qs = jnp.sum(qs, axis=1, keepdims=True)
    vs = jnp.sum(vs, axis=1, keepdims=True)
    row = lax.broadcasted_iota(jnp.int32, sq_ref.shape[1:], 0)
    sq_ref[t] = jnp.where(row == 0, qs / (width * qc * 2), vs / (width * (cols - qc) * 2))
    sx = remote(sq_ref.at[t], sq_ref.at[t], tp_s.at[2], tp_r.at[2], (z, r, other))
    sx.start()
    sx.wait_recv()
    scale_out[...] = lax.rsqrt(sq_ref[0] + sq_ref[1] + EPS_NORM)
    for k in range(1, nz):
        w2[k, 2].wait_recv()
        w2[k, 3].wait_recv()
    for c in f1 + list(w1.values()) + f2 + rsc + ([] if scatter else zc) + gc + agc + [fx, lx, sx] + list(w2.values()):
        c.wait_send()
    w_own.wait()


def run_exchange(nz, nr, x, cq, cv, wq, wv, qf, vf, q1, q2, v1, v2):
    tokens, width = x.shape
    qc = cq.shape[1]
    cols = qc + cv.shape[1]
    rows, rank = qf.shape
    own = rank // nr
    share = own // nz if (own // nz) % 16 == 0 else own
    any_spec = pl.BlockSpec(memory_space=pltpu.HBM)
    vmem = pl.BlockSpec(memory_space=pltpu.VMEM)
    dma = pltpu.SemaphoreType.DMA
    shape = jax.ShapeDtypeStruct
    return pl.pallas_call(
        functools.partial(exchange, nz, nr),
        out_shape=(
            shape((width, cols), BF),
            shape((2, width, rank), BF),
            shape((rank, cols), BF),
            shape((own, cols), F32),
            shape((8, 128), F32),
        ),
        in_specs=[any_spec] * 11,
        out_specs=(any_spec, vmem, vmem, vmem, vmem),
        scratch_shapes=[
            pltpu.VMEM((tokens, width), BF),
            pltpu.VMEM(cq.shape, BF),
            pltpu.VMEM(cv.shape, BF),
            pltpu.VMEM((rows, cols), F32),
            pltpu.VMEM((rows, cols), BF),
            pltpu.VMEM((2, tokens, rank), BF),
            pltpu.VMEM((rank, cols), BF),
            pltpu.VMEM((nr - 1, own, cols), BF),
            pltpu.VMEM((nz, share, cols), BF),
            pltpu.VMEM((own, cols), BF),
            pltpu.VMEM((own, cols), BF),
            pltpu.VMEM((own, cols), F32),
            pltpu.VMEM((own, cols), F32),
            pltpu.VMEM((2, 8, 128), F32),
            dma((11,)),
            dma((nz - 1,)),
            dma((nz - 1,)),
            dma((nz - 1,)),
            dma((nz - 1,)),
            dma(((nz - 1) * (nr - 1),)),
            dma(((nz - 1) * (nr - 1),)),
            dma((nz - 1, 4)),
            dma((nz - 1, 4)),
            dma((nr - 1,)),
            dma((nr - 1,)),
            dma((nz - 1,)),
            dma((nz - 1,)),
            dma((nz - 1,)),
            dma((nz - 1,)),
            dma((nr - 1,)),
            dma((nr - 1,)),
            dma((3,)),
            dma((3,)),
        ],
        compiler_params=pltpu.CompilerParams(
            collective_id=0, has_side_effects=True, vmem_limit_bytes=60 * 1024 * 1024
        ),
    )(x, cq, cv, wq, wv, qf, vf, q1, q2, v1, v2)


def finish(
    f_ref,
    ratio_ref,
    scale_ref,
    w_ref,
    wq_ref,
    wv_ref,
    qf_ref,
    vf_ref,
    proj_ref,
    q1_ref,
    q2_ref,
    v1_ref,
    v2_ref,
    qd_out,
    vd_out,
    qm_out,
    vm_out,
    q1_out,
    q2_out,
    v1_out,
    v2_out,
    qcopy_out,
    vcopy_out,
):
    qc = wq_ref.shape[1]
    sets = (
        (0, pl.ds(0, qc), wq_ref, qf_ref, q1_ref, q2_ref, qd_out, qm_out, q1_out, q2_out, qcopy_out),
        (
            1,
            pl.ds(qc, wv_ref.shape[1]),
            wv_ref,
            vf_ref,
            v1_ref,
            v2_ref,
            vd_out,
            vm_out,
            v1_out,
            v2_out,
            vcopy_out,
        ),
    )
    for n, at, w, f, m1, m2, d_out, m_out, m1_out, m2_out, c_out in sets:
        scale = scale_ref[n : n + 1, 0:1]
        ratio = ratio_ref[:, at]
        raw = jnp.dot(f_ref[n], ratio, preferred_element_type=F32)
        c_out[...] = (w_ref[:, at].astype(F32) - RATE * (raw * scale)).astype(BF)
        d = jnp.dot(f[...], ratio, preferred_element_type=F32) * scale
        d_out[...] = d
        m_out[...] = w[...] - RATE * d
        m1_out[...], m2_out[...], _ = moments(proj_ref[:, at], m1[...], m2[...])


def run_finish(factors, ratio, scale, weights, wq, wv, qf, vf, proj, q1, q2, v1, v2):
    rows, qc = wq.shape
    vc = wv.shape[1]
    width, cols = weights.shape
    rank, own = qf.shape[1], q1.shape[0]
    steps = 8 if rows % 128 == 0 else 4

    def tall(n, c):
        return pl.BlockSpec((n // steps, c), lambda i: (i, 0))

    def whole(a):
        return pl.BlockSpec(a.shape, lambda i: (0,) * a.ndim)

    shape = jax.ShapeDtypeStruct
    return pl.pallas_call(
        finish,
        grid=(steps,),
        in_specs=[
            pl.BlockSpec((2, width // steps, rank), lambda i: (0, i, 0)),
            whole(ratio),
            whole(scale),
            tall(width, cols),
            tall(rows, qc),
            tall(rows, vc),
            tall(rows, rank),
            tall(rows, rank),
            tall(own, cols),
            tall(own, qc),
            tall(own, qc),
            tall(own, vc),
            tall(own, vc),
        ],
        out_specs=[
            tall(rows, qc),
            tall(rows, vc),
            tall(rows, qc),
            tall(rows, vc),
            tall(own, qc),
            tall(own, qc),
            tall(own, vc),
            tall(own, vc),
            tall(width, qc),
            tall(width, vc),
        ],
        out_shape=[
            shape((rows, qc), F32),
            shape((rows, vc), F32),
            shape((rows, qc), F32),
            shape((rows, vc), F32),
            shape((own, qc), F32),
            shape((own, qc), F32),
            shape((own, vc), F32),
            shape((own, vc), F32),
            shape((width, qc), BF),
            shape((width, vc), BF),
        ],
        compiler_params=pltpu.CompilerParams(vmem_limit_bytes=60 * 1024 * 1024),
    )(factors, ratio, scale, weights, wq, wv, qf, vf, proj, q1, q2, v1, v2)


def line_exchange(
    quarter,
    chunks,
    rests,
    x_hbm,
    cq_hbm,
    cv_hbm,
    wq_hbm,
    wv_hbm,
    qf_hbm,
    vf_hbm,
    q1_hbm,
    q2_hbm,
    v1_hbm,
    v2_hbm,
    w_ref,
    f_ref,
    ratio_ref,
    wf_ref,
    m1_out,
    m2_out,
    scale_out,
    d_ref,
    x_ref,
    cq_ref,
    cv_ref,
    acc_ref,
    low_ref,
    part_ref,
    ra_ref,
    tb_ref,
    rb_ref,
    zs_ref,
    zo_ref,
    z_ref,
    zh_ref,
    m1_ref,
    m2_ref,
    g_ref,
    sq_ref,
    local_sem,
    out_s,
    fz_r,
    fp_r,
    wz_r,
    wp_r,
    wc_r,
    ra_r,
    rb_r,
    zs_r,
    zg_r,
    ag_r,
    ac_r,
    tp_s,
    tp_r,
):
    z = lax.axis_index("fs")
    r = lax.axis_index("rep")
    t = lax.axis_index("tp")
    nz, nr = 4, 4
    rows = qf_hbm.shape[0]
    part = rows // nr
    qc = cq_ref.shape[1]
    width, cols = w_ref.shape
    half = cols // 2
    rank = low_ref.shape[2]
    own = rank // nr
    share = own // nz
    tokens = x_ref.shape[0]
    px, py = lax.rem(r, 2), lax.div(r, 2)
    side = r + 1 - 2 * px
    over = lax.rem(r + 2, nr)
    corner = nr - 1 - r
    other = 1 - t
    upper = lax.div(z, 2)
    near = z + 1 - 2 * lax.rem(z, 2)
    mid = 2 - upper
    far = 3 - 3 * upper
    planes = [near, mid, far]
    inner = jnp.logical_and(z > 0, z < nz - 1)
    groups = {"plane": 0, "line": 1, "inner": 2}
    sent = dict.fromkeys(groups, 0)

    def remote(src, dst, ss, rs, dev):
        return pltpu.make_async_remote_copy(
            src_ref=src,
            dst_ref=dst,
            send_sem=ss,
            recv_sem=rs,
            device_id=dev,
            device_id_type=pl.DeviceIdType.MESH,
        )

    def count(ref, group):
        sent[group] += ref.size * ref.dtype.itemsize

    def send(src, dst, rs, dev, group="plane"):
        count(dst, group)
        remote(src, dst, out_s.at[groups[group]], rs, dev).start()

    def send_pair(src, dst, n):
        remote(src, dst, tp_s.at[n], tp_r.at[n], (z, r, other)).start()

    def send_inner(ref, rs, dev, wait=None):
        count(ref, "inner")

        @pl.when(inner)
        def _():
            if wait is not None:
                arrive(ref, wait)
            remote(ref, ref, out_s.at[2], rs, dev).start()

    def drain(group):
        size, line = sent[group], cols * 2
        while size:
            span = pl.ds(0, min(size // line, width))
            size -= min(size // line, width) * line
            ref = w_ref.at[span]
            remote(ref, ref, out_s.at[groups[group]], tp_r.at[0], (z, r, other)).wait_send()

    def arrive(dst, rs):
        remote(dst, dst, tp_s.at[0], rs, (z, r, other)).wait_recv()

    def at(start, size, step):
        return pl.ds(pl.multiple_of(start, step), size)

    def fac_copy(src):
        return pltpu.make_async_copy(src, f_ref.at[t, at(z * rows, rows, rows)], local_sem.at[0])

    @pl.when(t == 0)
    def _():
        fac_copy(qf_hbm).start()

    @pl.when(t == 1)
    def _():
        fac_copy(vf_hbm).start()

    left, right = pl.ds(0, qc), pl.ds(qc, cols - qc)
    x_in = pltpu.make_async_copy(x_hbm, x_ref, local_sem.at[1])
    cq_in = pltpu.make_async_copy(cq_hbm, cq_ref, local_sem.at[2])
    cv_in = pltpu.make_async_copy(cv_hbm, cv_ref, local_sem.at[3])
    pltpu.make_async_copy(wq_hbm, wf_ref.at[:, left], local_sem.at[4]).start()
    pltpu.make_async_copy(wv_hbm, wf_ref.at[:, right], local_sem.at[4]).start()
    for c in (x_in, cq_in, cv_in):
        c.start()
    for n, src, dst, span in (
        (5, q1_hbm, m1_ref, left),
        (5, v1_hbm, m1_ref, right),
        (6, q2_hbm, m2_ref, left),
        (6, v2_hbm, m2_ref, right),
    ):
        pltpu.make_async_copy(src, dst.at[:, span], local_sem.at[n]).start()

    def loaded(ref, n):
        pltpu.make_async_copy(ref, ref, local_sem.at[n]).wait()

    barrier = pltpu.get_barrier_semaphore()
    peers = [(p, r, t) for p in planes]
    peers += [(z, p, t) for p in (side, over, corner)]
    peers += [(z, r, other)]
    for dev in peers:
        pl.semaphore_signal(
            barrier, inc=1, device_id=dev, device_id_type=pl.DeviceIdType.MESH
        )
    pl.semaphore_wait(barrier, len(peers))

    class Spread:
        def __init__(self, view, split, rs, rest):
            self.view, self.split, self.rs, self.rest = view, split, rs, rest

        def start(self):
            here = self.view(r)
            for n, dev in ((0, side), (1, over)):
                send(here, here, self.rs.at[n], (z, dev, t))

        def relay(self):
            for n, src, dev in ((0, side, over), (1, over, side)):
                whole = self.view(src)
                arrive(whole, self.rs.at[n])
                there = self.split(whole, n)
                send(there, there, self.rest, (z, dev, t))

    def halves(ref, n):
        return ref.at[:, pl.ds(n * half, half)]

    def fac_rows(plane, rr):
        return f_ref.at[t, at(plane * rows + rr * part, part, part)]

    fac_copy(qf_hbm).wait()
    for i, p in enumerate(planes):
        here = fac_rows(z, r)
        send(here, here, fz_r.at[z], (p, r, t), "line")

    spans = [(n, s, True) for n, s in zip([sum(chunks[:c]) for c in range(len(chunks))], chunks)]
    spans += [(n, s, False) for n, s in zip([sum(rests[:c]) for c in range(len(rests))], rests)]

    def w_rows(plane, rr, c):
        begin, size, split = spans[c]
        begin = plane * rows + begin + (rr * quarter if split else nr * quarter)
        return w_ref.at[at(begin, size, 8)]

    def w_own(c):
        here = w_rows(z, r, c)
        send(here, here, wz_r.at[z, c], (near, r, t), "line")
        send_inner(here, wz_r.at[z, c], (mid, r, t))

    def w_pass(i, c):
        sem = wz_r.at[planes[i], c]
        send_inner(w_rows(planes[i], r, c), sem, (near if i else mid, r, t), sem)

    def w_land(i, c):
        @pl.when(jnp.logical_not(inner))
        def _():
            arrive(w_rows(planes[i], r, c), wz_r.at[planes[i], c])

    def w_start(i, c):
        w_land(i, c)
        w_in[i][c].start()

    w_in = [
        [
            Spread(functools.partial(lambda p, c, rr: w_rows(p, rr, c), p, c), halves, wp_r.at[i, c], wc_r.at[i])
            for c in range(len(chunks))
        ]
        for i, p in enumerate(planes)
    ]

    def low_add(plane, first):
        a = jnp.dot(
            x_ref[:, at(plane * rows, rows, rows)],
            f_ref[t, at(plane * rows, rows, rows)],
            preferred_element_type=F32,
        )
        acc_ref[...] = a if first else acc_ref[...] + a

    fac = [
        Spread(
            functools.partial(fac_rows, p),
            lambda ref, n: ref.at[pl.ds(n * (part // 2), part // 2)],
            fp_r.at[i],
            fp_r.at[i, 2],
        )
        for i, p in enumerate(planes)
    ]

    def fac_start(i):
        arrive(fac_rows(planes[i], r), fz_r.at[planes[i]])
        fac[i].start()

    def fac_finish(i):
        arrive(fac_rows(planes[i], corner), fp_r.at[i, 2])
        low_add(planes[i], False)

    def share_rows(plane):
        return at(plane * share, share, share)

    def low_rows(rr, plane):
        return at(rr * own + plane * share, share, share)

    lo, hi = pl.ds(0, half), pl.ds(half, half)
    order = [far, mid, near, z]

    def sum_start(i):
        span = share_rows(order[i])
        for n, src, dev in (
            (0, part_ref.at[:, 1 - px, span, lo], side),
            (1, part_ref.at[1 - py, :, span, hi], over),
        ):
            send(src, ra_ref.at[n, :, span], ra_r.at[i, n], (z, dev, t))

    def sum_relay(i):
        span = share_rows(order[i])
        for n in range(2):
            arrive(ra_ref.at[n, :, span], ra_r.at[i, n])
        for n, mine, theirs, dev in (
            (0, part_ref[1 - py, px, span, lo], ra_ref[0, 1 - py, span, :], over),
            (1, part_ref[py, 1 - px, span, hi], ra_ref[1, 1 - px, span, :], side),
        ):
            tb_ref[n, span, :] = (mine.astype(F32) + theirs.astype(F32)).astype(BF)
            send(tb_ref.at[n, span], rb_ref.at[n, span], rb_r.at[i, n], (z, dev, t))

    def sum_finish(i):
        span = share_rows(order[i])
        for n in range(2):
            arrive(rb_ref.at[n, span], rb_r.at[i, n])
        out = []
        for n, cut, theirs in ((0, lo, ra_ref[0, py, span, :]), (1, hi, ra_ref[1, px, span, :])):
            a = part_ref[py, px, span, cut].astype(F32) + theirs.astype(F32)
            out.append(a + rb_ref[n, span, :].astype(F32))
        if i == 3:
            zo_ref[:, lo], zo_ref[:, hi] = out
        else:
            zs_ref[span, lo] = out[0].astype(BF)
            zs_ref[span, hi] = out[1].astype(BF)
            send(zs_ref.at[span], z_ref.at[z], zs_r.at[z], (order[i], r, t), "line")

    def line_sum():
        proj = zo_ref[...]
        for p in planes:
            arrive(z_ref.at[p], zs_r.at[p])
            proj = proj + z_ref[p].astype(F32)
        here = zh_ref.at[share_rows(z)]
        zh_ref[share_rows(z), :] = proj.astype(BF)
        for p in (far, mid, near):
            send(here, here, zg_r.at[z], (p, r, t), "line")

    ratio_in = [
        Spread(
            functools.partial(lambda p, rr: ratio_ref.at[low_rows(rr, p)], p),
            halves,
            ag_r.at[i],
            ac_r.at[0],
        )
        for i, p in enumerate([z] + planes)
    ]

    def ratio_start(i):
        p = z
        if i:
            p = planes[i - 1]
            arrive(zh_ref.at[share_rows(p)], zg_r.at[p])
        span = share_rows(p)
        first, second, ratio = moments(
            zh_ref[span, :].astype(F32), m1_ref[span, :], m2_ref[span, :]
        )
        m1_out[span, :] = first
        m2_out[span, :] = second
        ratio_ref[low_rows(r, p), :] = ratio.astype(BF)
        ratio_in[i].start()

    dims = (((0,), (0,)), ((), ()))

    def low_parts():
        for n, c_ref, span in ((0, cq_ref, slice(0, qc)), (1, cv_ref, slice(qc, cols))):
            a = lax.dot_general(
                low_ref[n], c_ref[...], dims, preferred_element_type=F32
            ).astype(BF)
            for k in range(nr):
                part_ref[k // 2, k % 2, :, span] = a[k * own : (k + 1) * own]

    def gram():
        arrive(f_ref.at[other], tp_r.at[0])
        for n in range(2):
            g = lax.dot_general(f_ref[n], f_ref[n], dims, preferred_element_type=F32)
            top = g.astype(BF)
            g_ref[n, 0] = top
            g_ref[n, 1] = (g - top.astype(F32)).astype(BF)

    def squares(n, span):
        ratio = ratio_ref[:, span]
        a = jnp.dot(g_ref[n, 0], ratio, preferred_element_type=F32)
        a = a + jnp.dot(g_ref[n, 1], ratio, preferred_element_type=F32)
        a = jnp.sum(a * ratio.astype(F32), axis=0, keepdims=True)
        return jnp.sum(a, axis=1, keepdims=True)

    def own_rows():
        mine = at(z * rows, rows, rows)
        tile = min(256, qc)

        def columns(n, begin):
            cut = pl.ds(begin, tile)
            d = jnp.dot(f_ref[n, mine], ratio_ref[:, cut], preferred_element_type=F32)
            d = d * scale_out[n : n + 1, 0:1]
            d_ref[:, cut] = d
            wf_ref[:, cut] = wf_ref[:, cut] - RATE * d

        for begin in range(0, cols, tile):
            columns(0 if begin < qc else 1, begin)

    loaded(wf_ref, 4)
    w_ref[at(z * rows, rows, rows), :] = wf_ref[...].astype(BF)
    w_own(2)
    fac_start(0)
    w_own(1)
    x_in.wait()
    low_add(z, True)
    fac_start(1)
    fac_start(2)
    w_own(0)
    fac[0].relay()
    fac[1].relay()
    w_own(4)
    w_pass(1, 2)
    w_pass(0, 2)
    fac[2].relay()
    w_start(0, 2)
    w_own(3)
    fac_finish(0)
    w_pass(0, 1)
    fac_finish(1)
    w_start(0, 1)
    fac_finish(2)
    send_pair(f_ref.at[t], f_ref.at[t], 0)
    w_own(5)
    low_ref[t] = acc_ref[...].astype(BF)
    send_pair(low_ref.at[t], low_ref.at[t], 1)
    w_pass(0, 0)
    w_start(1, 2)
    cq_in.wait()
    cv_in.wait()
    arrive(low_ref.at[other], tp_r.at[1])
    low_parts()
    sum_start(2)
    sum_start(0)
    w_pass(1, 0)
    sum_start(1)
    w_pass(1, 1)
    sum_start(3)
    sum_relay(2)
    sum_relay(0)
    w_pass(0, 5)
    w_start(0, 0)
    w_pass(2, 1)
    sum_relay(3)
    sum_relay(1)
    w_in[1][2].relay()
    sum_finish(2)
    w_in[0][1].relay()
    w_pass(1, 5)
    sum_finish(0)
    w_start(1, 0)
    gram()
    w_pass(2, 0)
    sum_finish(3)
    w_in[0][0].relay()
    w_start(2, 1)
    sum_finish(1)
    w_start(1, 1)
    loaded(m1_ref, 5)
    loaded(m2_ref, 6)
    line_sum()
    ratio_start(0)
    w_pass(0, 4)
    w_pass(2, 5)
    w_pass(2, 2)
    w_in[1][0].relay()
    w_pass(1, 3)
    w_start(2, 0)
    ratio_in[0].relay()
    w_pass(0, 3)
    ratio_start(3)
    ratio_start(1)
    ratio_start(2)
    w_in[2][1].relay()
    w_start(2, 2)
    w_pass(2, 4)
    w_pass(1, 4)
    w_pass(2, 3)
    ratio_in[1].relay()
    ratio_in[2].relay()
    ratio_in[3].relay()
    w_in[0][2].relay()
    w_in[2][2].relay()
    w_in[2][0].relay()
    w_in[1][1].relay()
    arrive(ratio_ref.at[at(corner * own, own, own)], ac_r.at[0])
    qs = squares(0, slice(0, qc)) / (width * qc * 2)
    vs = squares(1, slice(qc, cols)) / (width * (cols - qc) * 2)
    line = lax.broadcasted_iota(jnp.int32, sq_ref.shape[1:], 0)
    sq_ref[t] = jnp.where(line == 0, qs, vs)
    send_pair(sq_ref.at[t], sq_ref.at[t], 2)
    arrive(sq_ref.at[other], tp_r.at[2])
    scale_out[...] = lax.rsqrt(jnp.maximum(sq_ref[0] + sq_ref[1], 0.0) + EPS_NORM)
    own_rows()
    for c in range(len(chunks), len(spans)):
        for i in range(3):
            w_land(i, c)
    for i in range(3):
        arrive(w_ref.at[at(planes[i] * rows + corner * quarter, quarter, 8)], wc_r.at[i])
    for n, ref in enumerate((f_ref.at[t], low_ref.at[t], sq_ref.at[t])):
        remote(ref, ref, tp_s.at[n], tp_r.at[n], (z, r, other)).wait_send()
    drain("plane")
    drain("line")

    @pl.when(inner)
    def _():
        drain("inner")


def run_line_exchange(x, cq, cv, wq, wv, qf, vf, q1, q2, v1, v2):
    tokens, width = x.shape
    qc = cq.shape[1]
    cols = qc + cv.shape[1]
    rows, rank = qf.shape
    own = rank // 4
    share = own // 4
    unit = rows // 64
    quarter = 12 * unit
    chunks = (4 * unit, 4 * unit, 4 * unit)
    rests = (6 * unit, 5 * unit, 5 * unit)
    any_spec = pl.BlockSpec(memory_space=pltpu.HBM)
    vmem = pl.BlockSpec(memory_space=pltpu.VMEM)
    dma = pltpu.SemaphoreType.DMA
    n = len(chunks)
    m = n + len(rests)
    return pl.pallas_call(
        functools.partial(line_exchange, quarter, chunks, rests),
        out_shape=(
            pltpu.VMEM((width, cols), BF),
            pltpu.VMEM((2, width, rank), BF),
            pltpu.VMEM((rank, cols), BF),
            pltpu.VMEM((rows, cols), F32),
            pltpu.VMEM((own, cols), F32),
            pltpu.VMEM((own, cols), F32),
            pltpu.VMEM((8, 128), F32),
            pltpu.VMEM((rows, cols), F32),
        ),
        in_specs=[any_spec] * 11,
        out_specs=(vmem,) * 8,
        scratch_shapes=[
            pltpu.VMEM((tokens, width), BF),
            pltpu.VMEM(cq.shape, BF),
            pltpu.VMEM(cv.shape, BF),
            pltpu.VMEM((tokens, rank), F32),
            pltpu.VMEM((2, tokens, rank), BF),
            pltpu.VMEM((2, 2, own, cols), BF),
            pltpu.VMEM((2, 2, own, cols // 2), BF),
            pltpu.VMEM((2, own, cols // 2), BF),
            pltpu.VMEM((2, own, cols // 2), BF),
            pltpu.VMEM((own, cols), BF),
            pltpu.VMEM((share, cols), F32),
            pltpu.VMEM((4, share, cols), BF),
            pltpu.VMEM((own, cols), BF),
            pltpu.VMEM((own, cols), F32),
            pltpu.VMEM((own, cols), F32),
            pltpu.VMEM((2, 2, rank, rank), BF),
            pltpu.VMEM((2, 8, 128), F32),
            dma((7,)),
            dma((3,)),
            dma((4,)),
            dma((3, 3)),
            dma((4, m)),
            dma((3, n, 2)),
            dma((3,)),
            dma((4, 2)),
            dma((4, 2)),
            dma((4,)),
            dma((4,)),
            dma((4, 2)),
            dma((1,)),
            dma((3,)),
            dma((3,)),
        ],
        compiler_params=pltpu.CompilerParams(
            collective_id=0, has_side_effects=True, vmem_limit_bytes=48 * 1024 * 1024
        ),
    )(x, cq, cv, wq, wv, qf, vf, q1, q2, v1, v2)


def line_finish(
    steps,
    w_ref,
    f_ref,
    ratio_ref,
    m_ref,
    m1_ref,
    m2_ref,
    scale_ref,
    d_ref,
    qd_out,
    vd_out,
    qm_out,
    vm_out,
    q1_out,
    q2_out,
    v1_out,
    v2_out,
    qcopy_out,
    vcopy_out,
    c_ref,
    sem,
):
    width, cols = w_ref.shape
    qc = qd_out.shape[1]
    left, right = pl.ds(0, qc), pl.ds(qc, cols - qc)
    outs = (
        (d_ref, left, qd_out),
        (d_ref, right, vd_out),
        (m_ref, left, qm_out),
        (m_ref, right, vm_out),
        (m1_ref, left, q1_out),
        (m1_ref, right, v1_out),
        (m2_ref, left, q2_out),
        (m2_ref, right, v2_out),
    )
    copies = [
        pltpu.make_async_copy(src.at[:, cut], dst, sem.at[n])
        for n, (src, cut, dst) in enumerate(outs)
    ]
    for c in copies:
        c.start()
    tall = width // steps

    @pl.loop(0, steps)
    def _(i):
        span = pl.ds(pl.multiple_of(i * tall, tall), tall)
        for n, cut, dst in ((0, left, qcopy_out), (1, right, vcopy_out)):
            raw = jnp.dot(f_ref[n, span], ratio_ref[:, cut], preferred_element_type=F32)
            raw = raw * scale_ref[n : n + 1, 0:1]
            c_ref[span, cut] = (w_ref[span, cut].astype(F32) - RATE * raw).astype(BF)
            pltpu.make_async_copy(c_ref.at[span, cut], dst.at[span], sem.at[8 + n]).start()

    for c in copies:
        c.wait()
    for n, cut, dst in ((0, left, qcopy_out), (1, right, vcopy_out)):
        pltpu.make_async_copy(c_ref.at[:, cut], dst, sem.at[8 + n]).wait()


def run_line_finish(weights, factors, ratio, masters, m1, m2, scale, directions, qc):
    rows, cols = masters.shape
    vc = cols - qc
    width, own = weights.shape[0], m1.shape[0]
    vmem = pl.BlockSpec(memory_space=pltpu.VMEM)
    shape = jax.ShapeDtypeStruct
    return pl.pallas_call(
        functools.partial(line_finish, 8),
        in_specs=[vmem] * 8,
        out_specs=[pl.BlockSpec(memory_space=pltpu.HBM)] * 10,
        out_shape=[
            shape((rows, qc), F32),
            shape((rows, vc), F32),
            shape((rows, qc), F32),
            shape((rows, vc), F32),
            shape((own, qc), F32),
            shape((own, qc), F32),
            shape((own, vc), F32),
            shape((own, vc), F32),
            shape((width, qc), BF),
            shape((width, vc), BF),
        ],
        scratch_shapes=[pltpu.VMEM((width, cols), BF), pltpu.SemaphoreType.DMA((10,))],
        compiler_params=pltpu.CompilerParams(vmem_limit_bytes=16 * 1024 * 1024),
    )(weights, factors, ratio, masters, m1, m2, scale, directions)


def suits_line(nz, nr, qf, cq, cv):
    rows, rank = qf.shape
    cols = cq.shape[1] + cv.shape[1]
    return nz == 4 and nr == 4 and rows % 512 == 0 and rank % 256 == 0 and cols % 256 == 0


def local(nz, nr, *args):
    _, cq, cv, wq, wv, qf, vf, q1, q2, v1, v2 = args
    if suits_line(nz, nr, qf, cq, cv):
        return tuple(run_line_finish(*run_line_exchange(*args), cq.shape[1]))
    weights, factors, ratio, proj, scale = run_exchange(nz, nr, *args)
    return tuple(
        run_finish(factors, ratio, scale, weights, wq, wv, qf, vf, proj, q1, q2, v1, v2)
    )


def solution(mesh):
    return jax.shard_map(
        functools.partial(local, mesh.shape["fs"], mesh.shape["rep"]),
        mesh=mesh,
        in_specs=(
            P(("fs", "rep"), None),
            P(("fs", "rep"), "tp"),
            P(("fs", "rep"), "tp"),
            P("fs", "tp"),
            P("fs", "tp"),
            P("fs", None),
            P("fs", None),
            P("rep", "tp"),
            P("rep", "tp"),
            P("rep", "tp"),
            P("rep", "tp"),
        ),
        out_specs=(
            P("fs", "tp"),
            P("fs", "tp"),
            P("fs", "tp"),
            P("fs", "tp"),
            P("rep", "tp"),
            P("rep", "tp"),
            P("rep", "tp"),
            P("rep", "tp"),
            P(None, "tp"),
            P(None, "tp"),
        ),
        check_vma=False,
    )
```

```python
import functools

import jax
import jax.numpy as jnp
from jax import lax
from jax.experimental import pallas as pl
from jax.experimental.pallas import tpu as pltpu
from jax.sharding import PartitionSpec as P

BETA_ONE = 0.8
BETA_TWO = 0.9
EPS_RATIO = 1e-08
EPS_NORM = 1e-06
RATE = 0.02
BF = jnp.bfloat16
F32 = jnp.float32


def moments(projected, first, second):
    first_new = BETA_ONE * first + (1.0 - BETA_ONE) * projected
    second_new = BETA_TWO * second + (1.0 - BETA_TWO) * projected * projected
    ratio = first_new / (jnp.sqrt(second_new) + EPS_RATIO)
    return (first_new, second_new, ratio)


def exchange(
    nz,
    nr,
    x_hbm,
    cq_hbm,
    cv_hbm,
    wq_hbm,
    wv_hbm,
    qf_hbm,
    vf_hbm,
    q1_hbm,
    q2_hbm,
    v1_hbm,
    v2_hbm,
    w_out,
    f_ref,
    ratio_ref,
    proj_out,
    scale_out,
    x_ref,
    cq_ref,
    cv_ref,
    wf_ref,
    wb_ref,
    low_ref,
    part_ref,
    rs_ref,
    z_ref,
    zg_ref,
    zh_ref,
    m1_ref,
    m2_ref,
    sq_ref,
    local_sem,
    f1_s,
    f1_r,
    w1_s,
    w1_r,
    f2_s,
    f2_r,
    w2_s,
    w2_r,
    rs_s,
    rs_r,
    zs_s,
    zs_r,
    zg_s,
    zg_r,
    ag_s,
    ag_r,
    tp_s,
    tp_r,
):
    z = lax.axis_index("fs")
    r = lax.axis_index("rep")
    t = lax.axis_index("tp")
    rows = qf_hbm.shape[0]
    part = rows // nr
    qc = cq_ref.shape[1]
    cols = w_out.shape[1]
    half = cols // 2
    width = w_out.shape[0]
    rank = low_ref.shape[2]
    own = rank // nr
    tokens = x_ref.shape[0]
    z_of = [lax.rem(z + k, nz) for k in range(nz)]
    z_from = [lax.rem(z + nz - k, nz) for k in range(nz)]
    r_of = [lax.rem(r + j, nr) for j in range(nr)]
    side = r + 1 - 2 * lax.rem(r, 2)
    over = lax.rem(r + 2, nr)
    corner = nr - 1 - r
    other = 1 - t

    def remote(src, dst, ss, rs, dev):
        return pltpu.make_async_remote_copy(
            src_ref=src,
            dst_ref=dst,
            send_sem=ss,
            recv_sem=rs,
            device_id=dev,
            device_id_type=pl.DeviceIdType.MESH,
        )

    def slab(zz, rr):
        return pl.ds(pl.multiple_of(zz * rows + rr * part, part), part)

    def fac_copy(src):
        return pltpu.make_async_copy(
            src,
            f_ref.at[t, pl.ds(pl.multiple_of(z * rows, rows), rows)],
            local_sem.at[0],
        )

    @pl.when(t == 0)
    def _():
        fac_copy(qf_hbm).start()

    @pl.when(t == 1)
    def _():
        fac_copy(vf_hbm).start()

    wq_in = pltpu.make_async_copy(wq_hbm, wf_ref.at[:, pl.ds(0, qc)], local_sem.at[1])
    wv_in = pltpu.make_async_copy(wv_hbm, wf_ref.at[:, pl.ds(qc, cols - qc)], local_sem.at[2])
    x_in = pltpu.make_async_copy(x_hbm, x_ref, local_sem.at[3])
    cq_in = pltpu.make_async_copy(cq_hbm, cq_ref, local_sem.at[4])
    cv_in = pltpu.make_async_copy(cv_hbm, cv_ref, local_sem.at[5])
    left, right = pl.ds(0, qc), pl.ds(qc, cols - qc)
    mom = [
        pltpu.make_async_copy(src, dst.at[:, at], local_sem.at[7 + n])
        for n, (src, dst, at) in enumerate(
            (
                (q1_hbm, m1_ref, left),
                (v1_hbm, m1_ref, right),
                (q2_hbm, m2_ref, left),
                (v2_hbm, m2_ref, right),
            )
        )
    ]
    for c in [wq_in, wv_in, x_in, cq_in, cv_in] + mom:
        c.start()

    barrier = pltpu.get_barrier_semaphore()
    peers = [(z_of[k], r, t) for k in range(1, nz)]
    peers += [(z, r_of[j], t) for j in range(1, nr)]
    peers += [(z, r, other)]
    for dev in peers:
        pl.semaphore_signal(
            barrier, inc=1, device_id=dev, device_id_type=pl.DeviceIdType.MESH
        )
    pl.semaphore_wait(barrier, len(peers))

    fac_copy(qf_hbm).wait()
    sends = []
    f1 = []
    for k in range(1, nz):
        here = f_ref.at[t, slab(z, r)]
        c = remote(here, here, f1_s.at[k - 1], f1_r.at[k - 1], (z_of[k], r, t))
        c.start()
        f1.append(c)
    wq_in.wait()
    wv_in.wait()
    wb_ref[...] = wf_ref[...].astype(BF)
    order = sorted(range(1, nz), key=lambda k: min(k, nz - k))
    w1 = {}
    for k in order:
        c = remote(
            wb_ref.at[pl.ds(pl.multiple_of(r * part, part), part)],
            w_out.at[slab(z, r)],
            w1_s.at[k - 1],
            w1_r.at[k - 1],
            (z_of[k], r, t),
        )
        c.start()
        w1[k] = c
    w_own = pltpu.make_async_copy(
        wb_ref, w_out.at[pl.ds(pl.multiple_of(z * rows, rows), rows)], local_sem.at[6]
    )
    w_own.start()

    f2 = []
    for k in range(1, nz):
        f1[k - 1].wait_recv()
        there = f_ref.at[t, slab(z_from[k], r)]
        for j in range(1, nr):
            n = (k - 1) * (nr - 1) + j - 1
            c = remote(there, there, f2_s.at[n], f2_r.at[n], (z, r_of[j], t))
            c.start()
            f2.append(c)
    for c in f2:
        c.wait_recv()
    w2 = {}

    def spread(k):
        w1[k].wait_recv()
        there = w_out.at[slab(z_from[k], r)]
        for n, dev in ((0, side), (1, over)):
            c = remote(there, there, w2_s.at[k - 1, n], w2_r.at[k - 1, n], (z, dev, t))
            c.start()
            w2[k, n] = c

    def relay(k):
        for n, src, dev, at in ((0, side, over, 0), (1, over, side, half)):
            w2[k, n].wait_recv()
            there = w_out.at[slab(z_from[k], src), pl.ds(at, half)]
            c = remote(
                there, there, w2_s.at[k - 1, 2 + n], w2_r.at[k - 1, 2 + n], (z, dev, t)
            )
            c.start()
            w2[k, 2 + n] = c

    stages = [[], [], []]
    for n, k in enumerate(order):
        stages[min(n, 2)].append(k)
    x_in.wait()
    tile = tokens // 3

    @pl.loop(0, 3)
    def _(i):
        span = pl.ds(pl.multiple_of(i * tile, tile), tile)
        low_ref[t, span] = jnp.dot(
            x_ref[span, :], f_ref[t], preferred_element_type=F32
        ).astype(BF)

    lx = remote(low_ref.at[t], low_ref.at[t], tp_s.at[1], tp_r.at[1], (z, r, other))
    lx.start()
    fx = remote(f_ref.at[t], f_ref.at[t], tp_s.at[0], tp_r.at[0], (z, r, other))
    fx.start()
    for k in stages[0]:
        spread(k)
    cq_in.wait()
    cv_in.wait()
    lx.wait_recv()
    dims = (((0,), (0,)), ((), ()))
    part_ref[:, :qc] = lax.dot_general(
        low_ref[0], cq_ref[...], dims, preferred_element_type=F32
    ).astype(BF)
    part_ref[:, qc:] = lax.dot_general(
        low_ref[1], cv_ref[...], dims, preferred_element_type=F32
    ).astype(BF)

    def low_rows(rr):
        return pl.ds(pl.multiple_of(rr * own, own), own)

    rsc = []
    for j in range(1, nr):
        c = remote(
            part_ref.at[low_rows(r_of[j])],
            rs_ref.at[j - 1],
            rs_s.at[j - 1],
            rs_r.at[j - 1],
            (z, r_of[j], t),
        )
        c.start()
        rsc.append(c)

    for k in stages[0]:
        relay(k)
    for c in rsc:
        c.wait_recv()
    total = part_ref[low_rows(r), :].astype(F32)
    for j in range(1, nr):
        total = total + rs_ref[j - 1].astype(F32)
    share = own // nz
    scatter = share % 16 == 0
    zc = []
    if scatter:
        zg_ref[...] = total.astype(BF)
    else:
        z_ref[z] = total.astype(BF)

    def z_rows(zz):
        return pl.ds(pl.multiple_of(zz * share, share), share)

    for k in range(1, nz):
        src = zg_ref.at[z_rows(z_of[k])] if scatter else z_ref.at[z]
        c = remote(src, z_ref.at[z], zs_s.at[k - 1], zs_r.at[k - 1], (z_of[k], r, t))
        c.start()
        zc.append(c)
    if scatter:
        z_ref[z] = zg_ref[z_rows(z), :]
    for k in stages[1]:
        spread(k)
    for c in zc:
        c.wait_recv()
    proj = z_ref[0].astype(F32)
    for k in range(1, nz):
        proj = proj + z_ref[k].astype(F32)
    gc = []
    if scatter:
        for c in zc:
            c.wait_send()
        zh = zh_ref
        zh[z_rows(z), :] = proj.astype(BF)
        for k in range(1, nz):
            here = zh.at[z_rows(z)]
            c = remote(here, here, zg_s.at[k - 1], zg_r.at[k - 1], (z_of[k], r, t))
            c.start()
            gc.append(c)
    for k in stages[1]:
        relay(k)
    for k in stages[2]:
        spread(k)
    for c in mom:
        c.wait()
    if scatter:
        for c in gc:
            c.wait_recv()
        proj = zh[...].astype(F32)
    proj_out[...] = proj
    _, _, ratio = moments(proj, m1_ref[...], m2_ref[...])
    ratio_ref[low_rows(r), :] = ratio.astype(BF)
    agc = []
    for j in range(1, nr):
        here = ratio_ref.at[low_rows(r)]
        c = remote(here, here, ag_s.at[j - 1], ag_r.at[j - 1], (z, r_of[j], t))
        c.start()
        agc.append(c)
    for k in stages[2]:
        relay(k)
    fx.wait_recv()
    for c in agc:
        c.wait_recv()
    step = min(256, width)

    def squares(i, acc):
        span = pl.ds(pl.multiple_of(i * step, step), step)
        a = jnp.dot(f_ref[0, span], ratio_ref[:, :qc], preferred_element_type=F32)
        b = jnp.dot(f_ref[1, span], ratio_ref[:, qc:], preferred_element_type=F32)
        a = jnp.sum(a * a, axis=0, keepdims=True)
        b = jnp.sum(b * b, axis=0, keepdims=True)
        return (acc[0] + a, acc[1] + b)

    qs, vs = lax.fori_loop(
        0,
        width // step,
        squares,
        (jnp.zeros((1, qc), F32), jnp.zeros((1, cols - qc), F32)),
    )
    qs = jnp.sum(qs, axis=1, keepdims=True)
    vs = jnp.sum(vs, axis=1, keepdims=True)
    row = lax.broadcasted_iota(jnp.int32, sq_ref.shape[1:], 0)
    sq_ref[t] = jnp.where(row == 0, qs / (width * qc * 2), vs / (width * (cols - qc) * 2))
    sx = remote(sq_ref.at[t], sq_ref.at[t], tp_s.at[2], tp_r.at[2], (z, r, other))
    sx.start()
    sx.wait_recv()
    scale_out[...] = lax.rsqrt(sq_ref[0] + sq_ref[1] + EPS_NORM)
    for k in range(1, nz):
        w2[k, 2].wait_recv()
        w2[k, 3].wait_recv()
    for c in f1 + list(w1.values()) + f2 + rsc + ([] if scatter else zc) + gc + agc + [fx, lx, sx] + list(w2.values()):
        c.wait_send()
    w_own.wait()


def run_exchange(nz, nr, x, cq, cv, wq, wv, qf, vf, q1, q2, v1, v2):
    tokens, width = x.shape
    qc = cq.shape[1]
    cols = qc + cv.shape[1]
    rows, rank = qf.shape
    own = rank // nr
    share = own // nz if (own // nz) % 16 == 0 else own
    any_spec = pl.BlockSpec(memory_space=pltpu.HBM)
    vmem = pl.BlockSpec(memory_space=pltpu.VMEM)
    dma = pltpu.SemaphoreType.DMA
    shape = jax.ShapeDtypeStruct
    return pl.pallas_call(
        functools.partial(exchange, nz, nr),
        out_shape=(
            shape((width, cols), BF),
            shape((2, width, rank), BF),
            shape((rank, cols), BF),
            shape((own, cols), F32),
            shape((8, 128), F32),
        ),
        in_specs=[any_spec] * 11,
        out_specs=(any_spec, vmem, vmem, vmem, vmem),
        scratch_shapes=[
            pltpu.VMEM((tokens, width), BF),
            pltpu.VMEM(cq.shape, BF),
            pltpu.VMEM(cv.shape, BF),
            pltpu.VMEM((rows, cols), F32),
            pltpu.VMEM((rows, cols), BF),
            pltpu.VMEM((2, tokens, rank), BF),
            pltpu.VMEM((rank, cols), BF),
            pltpu.VMEM((nr - 1, own, cols), BF),
            pltpu.VMEM((nz, share, cols), BF),
            pltpu.VMEM((own, cols), BF),
            pltpu.VMEM((own, cols), BF),
            pltpu.VMEM((own, cols), F32),
            pltpu.VMEM((own, cols), F32),
            pltpu.VMEM((2, 8, 128), F32),
            dma((11,)),
            dma((nz - 1,)),
            dma((nz - 1,)),
            dma((nz - 1,)),
            dma((nz - 1,)),
            dma(((nz - 1) * (nr - 1),)),
            dma(((nz - 1) * (nr - 1),)),
            dma((nz - 1, 4)),
            dma((nz - 1, 4)),
            dma((nr - 1,)),
            dma((nr - 1,)),
            dma((nz - 1,)),
            dma((nz - 1,)),
            dma((nz - 1,)),
            dma((nz - 1,)),
            dma((nr - 1,)),
            dma((nr - 1,)),
            dma((3,)),
            dma((3,)),
        ],
        compiler_params=pltpu.CompilerParams(
            collective_id=0, has_side_effects=True, vmem_limit_bytes=60 * 1024 * 1024
        ),
    )(x, cq, cv, wq, wv, qf, vf, q1, q2, v1, v2)


def finish(
    f_ref,
    ratio_ref,
    scale_ref,
    w_ref,
    wq_ref,
    wv_ref,
    qf_ref,
    vf_ref,
    proj_ref,
    q1_ref,
    q2_ref,
    v1_ref,
    v2_ref,
    qd_out,
    vd_out,
    qm_out,
    vm_out,
    q1_out,
    q2_out,
    v1_out,
    v2_out,
    qcopy_out,
    vcopy_out,
):
    qc = wq_ref.shape[1]
    sets = (
        (0, pl.ds(0, qc), wq_ref, qf_ref, q1_ref, q2_ref, qd_out, qm_out, q1_out, q2_out, qcopy_out),
        (
            1,
            pl.ds(qc, wv_ref.shape[1]),
            wv_ref,
            vf_ref,
            v1_ref,
            v2_ref,
            vd_out,
            vm_out,
            v1_out,
            v2_out,
            vcopy_out,
        ),
    )
    for n, at, w, f, m1, m2, d_out, m_out, m1_out, m2_out, c_out in sets:
        scale = scale_ref[n : n + 1, 0:1]
        ratio = ratio_ref[:, at]
        raw = jnp.dot(f_ref[n], ratio, preferred_element_type=F32)
        c_out[...] = (w_ref[:, at].astype(F32) - RATE * (raw * scale)).astype(BF)
        d = jnp.dot(f[...], ratio, preferred_element_type=F32) * scale
        d_out[...] = d
        m_out[...] = w[...] - RATE * d
        m1_out[...], m2_out[...], _ = moments(proj_ref[:, at], m1[...], m2[...])


def run_finish(factors, ratio, scale, weights, wq, wv, qf, vf, proj, q1, q2, v1, v2):
    rows, qc = wq.shape
    vc = wv.shape[1]
    width, cols = weights.shape
    rank, own = qf.shape[1], q1.shape[0]
    steps = 8 if rows % 128 == 0 else 4

    def tall(n, c):
        return pl.BlockSpec((n // steps, c), lambda i: (i, 0))

    def whole(a):
        return pl.BlockSpec(a.shape, lambda i: (0,) * a.ndim)

    shape = jax.ShapeDtypeStruct
    return pl.pallas_call(
        finish,
        grid=(steps,),
        in_specs=[
            pl.BlockSpec((2, width // steps, rank), lambda i: (0, i, 0)),
            whole(ratio),
            whole(scale),
            tall(width, cols),
            tall(rows, qc),
            tall(rows, vc),
            tall(rows, rank),
            tall(rows, rank),
            tall(own, cols),
            tall(own, qc),
            tall(own, qc),
            tall(own, vc),
            tall(own, vc),
        ],
        out_specs=[
            tall(rows, qc),
            tall(rows, vc),
            tall(rows, qc),
            tall(rows, vc),
            tall(own, qc),
            tall(own, qc),
            tall(own, vc),
            tall(own, vc),
            tall(width, qc),
            tall(width, vc),
        ],
        out_shape=[
            shape((rows, qc), F32),
            shape((rows, vc), F32),
            shape((rows, qc), F32),
            shape((rows, vc), F32),
            shape((own, qc), F32),
            shape((own, qc), F32),
            shape((own, vc), F32),
            shape((own, vc), F32),
            shape((width, qc), BF),
            shape((width, vc), BF),
        ],
        compiler_params=pltpu.CompilerParams(vmem_limit_bytes=60 * 1024 * 1024),
    )(factors, ratio, scale, weights, wq, wv, qf, vf, proj, q1, q2, v1, v2)


def line_exchange(
    quarter,
    chunks,
    rests,
    x_hbm,
    cq_hbm,
    cv_hbm,
    wq_hbm,
    wv_hbm,
    qf_hbm,
    vf_hbm,
    q1_hbm,
    q2_hbm,
    v1_hbm,
    v2_hbm,
    w_ref,
    f_ref,
    ratio_ref,
    wf_ref,
    m1_out,
    m2_out,
    scale_out,
    d_ref,
    x_ref,
    cq_ref,
    cv_ref,
    acc_ref,
    low_ref,
    part_ref,
    ra_ref,
    tb_ref,
    rb_ref,
    zs_ref,
    zo_ref,
    z_ref,
    zh_ref,
    m1_ref,
    m2_ref,
    g_ref,
    sq_ref,
    local_sem,
    out_s,
    fz_r,
    fp_r,
    wz_r,
    wp_r,
    wc_r,
    ra_r,
    rb_r,
    zs_r,
    zg_r,
    ag_r,
    ac_r,
    tp_s,
    tp_r,
):
    z = lax.axis_index("fs")
    r = lax.axis_index("rep")
    t = lax.axis_index("tp")
    nz, nr = 4, 4
    rows = qf_hbm.shape[0]
    part = rows // nr
    qc = cq_ref.shape[1]
    width, cols = w_ref.shape
    half = cols // 2
    rank = low_ref.shape[2]
    own = rank // nr
    share = own // nz
    tokens = x_ref.shape[0]
    px, py = lax.rem(r, 2), lax.div(r, 2)
    side = r + 1 - 2 * px
    over = lax.rem(r + 2, nr)
    corner = nr - 1 - r
    other = 1 - t
    upper = lax.div(z, 2)
    near = z + 1 - 2 * lax.rem(z, 2)
    mid = 2 - upper
    far = 3 - 3 * upper
    planes = [near, mid, far]
    inner = jnp.logical_and(z > 0, z < nz - 1)
    groups = {"plane": 0, "line": 1, "inner": 2}
    sent = dict.fromkeys(groups, 0)

    def remote(src, dst, ss, rs, dev):
        return pltpu.make_async_remote_copy(
            src_ref=src,
            dst_ref=dst,
            send_sem=ss,
            recv_sem=rs,
            device_id=dev,
            device_id_type=pl.DeviceIdType.MESH,
        )

    def count(ref, group):
        sent[group] += ref.size * ref.dtype.itemsize

    def send(src, dst, rs, dev, group="plane"):
        count(dst, group)
        remote(src, dst, out_s.at[groups[group]], rs, dev).start()

    def send_pair(src, dst, n):
        remote(src, dst, tp_s.at[n], tp_r.at[n], (z, r, other)).start()

    def send_inner(ref, rs, dev, wait=None):
        count(ref, "inner")

        @pl.when(inner)
        def _():
            if wait is not None:
                arrive(ref, wait)
            remote(ref, ref, out_s.at[2], rs, dev).start()

    def drain(group):
        size, line = sent[group], cols * 2
        while size:
            span = pl.ds(0, min(size // line, width))
            size -= min(size // line, width) * line
            ref = w_ref.at[span]
            remote(ref, ref, out_s.at[groups[group]], tp_r.at[0], (z, r, other)).wait_send()

    def arrive(dst, rs):
        remote(dst, dst, tp_s.at[0], rs, (z, r, other)).wait_recv()

    def at(start, size, step):
        return pl.ds(pl.multiple_of(start, step), size)

    def fac_copy(src):
        return pltpu.make_async_copy(src, f_ref.at[t, at(z * rows, rows, rows)], local_sem.at[0])

    @pl.when(t == 0)
    def _():
        fac_copy(qf_hbm).start()

    @pl.when(t == 1)
    def _():
        fac_copy(vf_hbm).start()

    left, right = pl.ds(0, qc), pl.ds(qc, cols - qc)
    x_in = pltpu.make_async_copy(x_hbm, x_ref, local_sem.at[1])
    cq_in = pltpu.make_async_copy(cq_hbm, cq_ref, local_sem.at[2])
    cv_in = pltpu.make_async_copy(cv_hbm, cv_ref, local_sem.at[3])
    pltpu.make_async_copy(wq_hbm, wf_ref.at[:, left], local_sem.at[4]).start()
    pltpu.make_async_copy(wv_hbm, wf_ref.at[:, right], local_sem.at[4]).start()
    for c in (x_in, cq_in, cv_in):
        c.start()
    for n, src, dst, span in (
        (5, q1_hbm, m1_ref, left),
        (5, v1_hbm, m1_ref, right),
        (6, q2_hbm, m2_ref, left),
        (6, v2_hbm, m2_ref, right),
    ):
        pltpu.make_async_copy(src, dst.at[:, span], local_sem.at[n]).start()

    def loaded(ref, n):
        pltpu.make_async_copy(ref, ref, local_sem.at[n]).wait()

    barrier = pltpu.get_barrier_semaphore()
    peers = [(p, r, t) for p in planes]
    peers += [(z, p, t) for p in (side, over, corner)]
    peers += [(z, r, other)]
    for dev in peers:
        pl.semaphore_signal(
            barrier, inc=1, device_id=dev, device_id_type=pl.DeviceIdType.MESH
        )
    pl.semaphore_wait(barrier, len(peers))

    class Spread:
        def __init__(self, view, split, both, rs, rest):
            self.view, self.split, self.both, self.rs, self.rest = view, split, both, rs, rest

        def start(self):
            here = self.view(r)
            for dev in (side, over):
                send(here, here, self.rs, (z, dev, t))

        def relay(self):
            arrive(self.both, self.rs)
            for n, src, dev in ((0, side, over), (1, over, side)):
                there = self.split(self.view(src), n)
                send(there, there, self.rest, (z, dev, t))

    def halves(ref, n):
        return ref.at[:, pl.ds(n * half, half)]

    def fac_rows(plane, rr):
        return f_ref.at[t, at(plane * rows + rr * part, part, part)]

    fac_copy(qf_hbm).wait()
    for i, p in enumerate(planes):
        here = fac_rows(z, r)
        send(here, here, fz_r.at[z], (p, r, t), "line")

    spans = [(n, s, True) for n, s in zip([sum(chunks[:c]) for c in range(len(chunks))], chunks)]
    spans += [(n, s, False) for n, s in zip([sum(rests[:c]) for c in range(len(rests))], rests)]

    def w_rows(plane, rr, c):
        begin, size, split = spans[c]
        begin = plane * rows + begin + (rr * quarter if split else nr * quarter)
        return w_ref.at[at(begin, size, 8)]

    def w_own(c):
        here = w_rows(z, r, c)
        send(here, here, wz_r.at[0, c], (near, r, t), "line")
        send_inner(here, wz_r.at[1, c], (mid, r, t))

    def w_pass(i, c):
        to, sem = (near, wz_r.at[i, c]) if i else (mid, wz_r.at[2, c])
        send_inner(w_rows(planes[i], r, c), sem, (to, r, t), wz_r.at[i, c])

    def w_land(i, c):
        @pl.when(jnp.logical_not(inner))
        def _():
            arrive(w_rows(planes[i], r, c), wz_r.at[i, c])

    def w_start(i, c):
        w_land(i, c)
        w_in[i][c].start()

    w_in = [
        [
            Spread(functools.partial(lambda p, c, rr: w_rows(p, rr, c), p, c), halves, w_ref.at[pl.ds(0, 2 * chunks[c])], wp_r.at[i, c], wc_r.at[i])
            for c in range(len(chunks))
        ]
        for i, p in enumerate(planes)
    ]

    def low_add(plane, first):
        a = jnp.dot(
            x_ref[:, at(plane * rows, rows, rows)],
            f_ref[t, at(plane * rows, rows, rows)],
            preferred_element_type=F32,
        )
        acc_ref[...] = a if first else acc_ref[...] + a

    fac = [
        Spread(
            functools.partial(fac_rows, p),
            lambda ref, n: ref.at[pl.ds(n * (part // 2), part // 2)],
            f_ref.at[t, pl.ds(0, 2 * part)],
            fp_r.at[i, 0],
            fp_r.at[i, 1],
        )
        for i, p in enumerate(planes)
    ]

    def fac_start(i):
        arrive(fac_rows(planes[i], r), fz_r.at[planes[i]])
        fac[i].start()

    def fac_finish(i):
        arrive(fac_rows(planes[i], corner), fp_r.at[i, 1])
        low_add(planes[i], False)

    def share_rows(plane):
        return at(plane * share, share, share)

    def low_rows(rr, plane):
        return at(rr * own + plane * share, share, share)

    lo, hi = pl.ds(0, half), pl.ds(half, half)
    order = [far, mid, near, z]

    def sum_start(i):
        span = share_rows(order[i])
        for n, src, dev in (
            (0, part_ref.at[:, 1 - px, span, lo], side),
            (1, part_ref.at[1 - py, :, span, hi], over),
        ):
            send(src, ra_ref.at[n, :, span], ra_r.at[i], (z, dev, t))

    def sum_relay(i):
        span = share_rows(order[i])
        arrive(ra_ref.at[:, :, span], ra_r.at[i])
        for n, mine, theirs, dev in (
            (0, part_ref[1 - py, px, span, lo], ra_ref[0, 1 - py, span, :], over),
            (1, part_ref[py, 1 - px, span, hi], ra_ref[1, 1 - px, span, :], side),
        ):
            tb_ref[n, span, :] = (mine.astype(F32) + theirs.astype(F32)).astype(BF)
            send(tb_ref.at[n, span], rb_ref.at[n, span], rb_r.at[i], (z, dev, t))

    def sum_finish(i):
        span = share_rows(order[i])
        arrive(rb_ref.at[:, span], rb_r.at[i])
        out = []
        for n, cut, theirs in ((0, lo, ra_ref[0, py, span, :]), (1, hi, ra_ref[1, px, span, :])):
            a = part_ref[py, px, span, cut].astype(F32) + theirs.astype(F32)
            out.append(a + rb_ref[n, span, :].astype(F32))
        if i == 3:
            zo_ref[:, lo], zo_ref[:, hi] = out
        else:
            zs_ref[span, lo] = out[0].astype(BF)
            zs_ref[span, hi] = out[1].astype(BF)
            send(zs_ref.at[span], z_ref.at[z], zs_r.at[z], (order[i], r, t), "line")

    def line_sum():
        proj = zo_ref[...]
        for p in planes:
            arrive(z_ref.at[p], zs_r.at[p])
            proj = proj + z_ref[p].astype(F32)
        here = zh_ref.at[share_rows(z)]
        zh_ref[share_rows(z), :] = proj.astype(BF)
        for p in (far, mid, near):
            send(here, here, zg_r.at[z], (p, r, t), "line")

    ratio_in = [
        Spread(
            functools.partial(lambda p, rr: ratio_ref.at[low_rows(rr, p)], p),
            halves,
            ratio_ref.at[pl.ds(0, 2 * share)],
            ag_r.at[i],
            ac_r.at[0],
        )
        for i, p in enumerate([z] + planes)
    ]

    def ratio_start(i):
        p = z
        if i:
            p = planes[i - 1]
            arrive(zh_ref.at[share_rows(p)], zg_r.at[p])
        span = share_rows(p)
        first, second, ratio = moments(
            zh_ref[span, :].astype(F32), m1_ref[span, :], m2_ref[span, :]
        )
        m1_out[span, :] = first
        m2_out[span, :] = second
        ratio_ref[low_rows(r, p), :] = ratio.astype(BF)
        ratio_in[i].start()

    dims = (((0,), (0,)), ((), ()))

    def low_parts():
        for n, c_ref, span in ((0, cq_ref, slice(0, qc)), (1, cv_ref, slice(qc, cols))):
            a = lax.dot_general(
                low_ref[n], c_ref[...], dims, preferred_element_type=F32
            ).astype(BF)
            for k in range(nr):
                part_ref[k // 2, k % 2, :, span] = a[k * own : (k + 1) * own]

    def gram():
        arrive(f_ref.at[other], tp_r.at[0])
        for n in range(2):
            g = lax.dot_general(f_ref[n], f_ref[n], dims, preferred_element_type=F32)
            top = g.astype(BF)
            g_ref[n, 0] = top
            g_ref[n, 1] = (g - top.astype(F32)).astype(BF)

    def squares(n, span):
        ratio = ratio_ref[:, span]
        a = jnp.dot(g_ref[n, 0], ratio, preferred_element_type=F32)
        a = a + jnp.dot(g_ref[n, 1], ratio, preferred_element_type=F32)
        a = jnp.sum(a * ratio.astype(F32), axis=0, keepdims=True)
        return jnp.sum(a, axis=1, keepdims=True)

    def own_rows():
        mine = at(z * rows, rows, rows)
        tile = min(256, qc)

        def columns(n, begin):
            cut = pl.ds(begin, tile)
            d = jnp.dot(f_ref[n, mine], ratio_ref[:, cut], preferred_element_type=F32)
            d = d * scale_out[n : n + 1, 0:1]
            d_ref[:, cut] = d
            wf_ref[:, cut] = wf_ref[:, cut] - RATE * d

        for begin in range(0, cols, tile):
            columns(0 if begin < qc else 1, begin)

    loaded(wf_ref, 4)
    w_ref[at(z * rows, rows, rows), :] = wf_ref[...].astype(BF)
    w_own(2)
    fac_start(0)
    w_own(1)
    x_in.wait()
    low_add(z, True)
    fac_start(1)
    fac_start(2)
    w_own(0)
    fac[0].relay()
    w_pass(1, 2)
    fac[1].relay()
    w_own(4)
    w_pass(0, 2)
    fac[2].relay()
    w_start(0, 2)
    w_own(3)
    fac_finish(0)
    w_pass(0, 1)
    fac_finish(1)
    w_start(0, 1)
    fac_finish(2)
    send_pair(f_ref.at[t], f_ref.at[t], 0)
    low_ref[t] = acc_ref[...].astype(BF)
    send_pair(low_ref.at[t], low_ref.at[t], 1)
    w_own(5)
    w_pass(0, 0)
    w_start(1, 2)
    cq_in.wait()
    cv_in.wait()
    arrive(low_ref.at[other], tp_r.at[1])
    low_parts()
    sum_start(2)
    w_pass(1, 0)
    sum_start(0)
    sum_start(1)
    w_pass(1, 1)
    sum_start(3)
    sum_relay(2)
    sum_relay(0)
    w_start(0, 0)
    w_pass(2, 1)
    w_pass(0, 5)
    sum_relay(3)
    w_in[1][2].relay()
    sum_relay(1)
    sum_finish(2)
    w_pass(2, 0)
    sum_finish(0)
    w_pass(1, 5)
    w_start(1, 0)
    w_in[0][1].relay()
    sum_finish(3)
    w_in[0][0].relay()
    w_start(2, 1)
    sum_finish(1)
    gram()
    w_start(1, 1)
    loaded(m1_ref, 5)
    loaded(m2_ref, 6)
    line_sum()
    ratio_start(0)
    w_pass(0, 4)
    w_pass(2, 5)
    w_pass(2, 2)
    w_pass(1, 3)
    w_in[1][0].relay()
    w_start(2, 0)
    ratio_in[0].relay()
    ratio_start(1)
    w_pass(0, 3)
    ratio_start(3)
    ratio_start(2)
    w_in[2][1].relay()
    w_start(2, 2)
    w_pass(2, 4)
    w_pass(2, 3)
    ratio_in[1].relay()
    ratio_in[2].relay()
    ratio_in[3].relay()
    w_pass(1, 4)
    w_in[0][2].relay()
    w_in[2][2].relay()
    w_in[1][1].relay()
    w_in[2][0].relay()
    arrive(ratio_ref.at[at(corner * own, own, own)], ac_r.at[0])
    qs = squares(0, slice(0, qc)) / (width * qc * 2)
    vs = squares(1, slice(qc, cols)) / (width * (cols - qc) * 2)
    line = lax.broadcasted_iota(jnp.int32, sq_ref.shape[1:], 0)
    sq_ref[t] = jnp.where(line == 0, qs, vs)
    send_pair(sq_ref.at[t], sq_ref.at[t], 2)
    arrive(sq_ref.at[other], tp_r.at[2])
    scale_out[...] = lax.rsqrt(jnp.maximum(sq_ref[0] + sq_ref[1], 0.0) + EPS_NORM)
    own_rows()
    for c in range(len(chunks), len(spans)):
        for i in range(3):
            w_land(i, c)
    for i in range(3):
        arrive(w_ref.at[at(planes[i] * rows + corner * quarter, quarter, 8)], wc_r.at[i])
    for n, ref in enumerate((f_ref.at[t], low_ref.at[t], sq_ref.at[t])):
        remote(ref, ref, tp_s.at[n], tp_r.at[n], (z, r, other)).wait_send()
    drain("plane")
    drain("line")

    @pl.when(inner)
    def _():
        drain("inner")


def run_line_exchange(x, cq, cv, wq, wv, qf, vf, q1, q2, v1, v2):
    tokens, width = x.shape
    qc = cq.shape[1]
    cols = qc + cv.shape[1]
    rows, rank = qf.shape
    own = rank // 4
    share = own // 4
    unit = rows // 64
    quarter = 12 * unit
    chunks = (4 * unit, 4 * unit, 4 * unit)
    rests = (6 * unit, 5 * unit, 5 * unit)
    any_spec = pl.BlockSpec(memory_space=pltpu.HBM)
    vmem = pl.BlockSpec(memory_space=pltpu.VMEM)
    dma = pltpu.SemaphoreType.DMA
    n = len(chunks)
    m = n + len(rests)
    return pl.pallas_call(
        functools.partial(line_exchange, quarter, chunks, rests),
        out_shape=(
            pltpu.VMEM((width, cols), BF),
            pltpu.VMEM((2, width, rank), BF),
            pltpu.VMEM((rank, cols), BF),
            pltpu.VMEM((rows, cols), F32),
            pltpu.VMEM((own, cols), F32),
            pltpu.VMEM((own, cols), F32),
            pltpu.VMEM((8, 128), F32),
            pltpu.VMEM((rows, cols), F32),
        ),
        in_specs=[any_spec] * 11,
        out_specs=(vmem,) * 8,
        scratch_shapes=[
            pltpu.VMEM((tokens, width), BF),
            pltpu.VMEM(cq.shape, BF),
            pltpu.VMEM(cv.shape, BF),
            pltpu.VMEM((tokens, rank), F32),
            pltpu.VMEM((2, tokens, rank), BF),
            pltpu.VMEM((2, 2, own, cols), BF),
            pltpu.VMEM((2, 2, own, cols // 2), BF),
            pltpu.VMEM((2, own, cols // 2), BF),
            pltpu.VMEM((2, own, cols // 2), BF),
            pltpu.VMEM((own, cols), BF),
            pltpu.VMEM((share, cols), F32),
            pltpu.VMEM((4, share, cols), BF),
            pltpu.VMEM((own, cols), BF),
            pltpu.VMEM((own, cols), F32),
            pltpu.VMEM((own, cols), F32),
            pltpu.VMEM((2, 2, rank, rank), BF),
            pltpu.VMEM((2, 8, 128), F32),
            dma((7,)),
            dma((3,)),
            dma((4,)),
            dma((3, 2)),
            dma((3, m)),
            dma((3, n)),
            dma((3,)),
            dma((4,)),
            dma((4,)),
            dma((4,)),
            dma((4,)),
            dma((4,)),
            dma((1,)),
            dma((3,)),
            dma((3,)),
        ],
        compiler_params=pltpu.CompilerParams(
            collective_id=0, has_side_effects=True, vmem_limit_bytes=48 * 1024 * 1024
        ),
    )(x, cq, cv, wq, wv, qf, vf, q1, q2, v1, v2)


def line_finish(
    steps,
    w_ref,
    f_ref,
    ratio_ref,
    m_ref,
    m1_ref,
    m2_ref,
    scale_ref,
    d_ref,
    qd_out,
    vd_out,
    qm_out,
    vm_out,
    q1_out,
    q2_out,
    v1_out,
    v2_out,
    qcopy_out,
    vcopy_out,
    c_ref,
    sem,
):
    width, cols = w_ref.shape
    qc = qd_out.shape[1]
    left, right = pl.ds(0, qc), pl.ds(qc, cols - qc)
    outs = (
        (d_ref, left, qd_out),
        (d_ref, right, vd_out),
        (m_ref, left, qm_out),
        (m_ref, right, vm_out),
        (m1_ref, left, q1_out),
        (m1_ref, right, v1_out),
        (m2_ref, left, q2_out),
        (m2_ref, right, v2_out),
    )
    copies = [
        pltpu.make_async_copy(src.at[:, cut], dst, sem.at[n])
        for n, (src, cut, dst) in enumerate(outs)
    ]
    for c in copies:
        c.start()
    tall = width // steps

    @pl.loop(0, steps)
    def _(i):
        span = pl.ds(pl.multiple_of(i * tall, tall), tall)
        for n, cut, dst in ((0, left, qcopy_out), (1, right, vcopy_out)):
            raw = jnp.dot(f_ref[n, span], ratio_ref[:, cut], preferred_element_type=F32)
            raw = raw * scale_ref[n : n + 1, 0:1]
            c_ref[span, cut] = (w_ref[span, cut].astype(F32) - RATE * raw).astype(BF)
            pltpu.make_async_copy(c_ref.at[span, cut], dst.at[span], sem.at[8 + n]).start()

    for c in copies:
        c.wait()
    for n, cut, dst in ((0, left, qcopy_out), (1, right, vcopy_out)):
        pltpu.make_async_copy(c_ref.at[:, cut], dst, sem.at[8 + n]).wait()


def run_line_finish(weights, factors, ratio, masters, m1, m2, scale, directions, qc):
    rows, cols = masters.shape
    vc = cols - qc
    width, own = weights.shape[0], m1.shape[0]
    vmem = pl.BlockSpec(memory_space=pltpu.VMEM)
    shape = jax.ShapeDtypeStruct
    return pl.pallas_call(
        functools.partial(line_finish, 8),
        in_specs=[vmem] * 8,
        out_specs=[pl.BlockSpec(memory_space=pltpu.HBM)] * 10,
        out_shape=[
            shape((rows, qc), F32),
            shape((rows, vc), F32),
            shape((rows, qc), F32),
            shape((rows, vc), F32),
            shape((own, qc), F32),
            shape((own, qc), F32),
            shape((own, vc), F32),
            shape((own, vc), F32),
            shape((width, qc), BF),
            shape((width, vc), BF),
        ],
        scratch_shapes=[pltpu.VMEM((width, cols), BF), pltpu.SemaphoreType.DMA((10,))],
        compiler_params=pltpu.CompilerParams(vmem_limit_bytes=16 * 1024 * 1024),
    )(weights, factors, ratio, masters, m1, m2, scale, directions)


def suits_line(nz, nr, qf, cq, cv):
    rows, rank = qf.shape
    cols = cq.shape[1] + cv.shape[1]
    return nz == 4 and nr == 4 and rows % 512 == 0 and rank % 256 == 0 and cols % 256 == 0


def local(nz, nr, *args):
    _, cq, cv, wq, wv, qf, vf, q1, q2, v1, v2 = args
    if suits_line(nz, nr, qf, cq, cv):
        return tuple(run_line_finish(*run_line_exchange(*args), cq.shape[1]))
    weights, factors, ratio, proj, scale = run_exchange(nz, nr, *args)
    return tuple(
        run_finish(factors, ratio, scale, weights, wq, wv, qf, vf, proj, q1, q2, v1, v2)
    )


def solution(mesh):
    return jax.shard_map(
        functools.partial(local, mesh.shape["fs"], mesh.shape["rep"]),
        mesh=mesh,
        in_specs=(
            P(("fs", "rep"), None),
            P(("fs", "rep"), "tp"),
            P(("fs", "rep"), "tp"),
            P("fs", "tp"),
            P("fs", "tp"),
            P("fs", None),
            P("fs", None),
            P("rep", "tp"),
            P("rep", "tp"),
            P("rep", "tp"),
            P("rep", "tp"),
        ),
        out_specs=(
            P("fs", "tp"),
            P("fs", "tp"),
            P("fs", "tp"),
            P("fs", "tp"),
            P("rep", "tp"),
            P("rep", "tp"),
            P("rep", "tp"),
            P("rep", "tp"),
            P(None, "tp"),
            P(None, "tp"),
        ),
        check_vma=False,
    )
```

```python
import functools

import jax
import jax.numpy as jnp
from jax import lax
from jax.experimental import pallas as pl
from jax.experimental.pallas import tpu as pltpu
from jax.sharding import PartitionSpec as P

BETA_ONE = 0.8
BETA_TWO = 0.9
EPS_RATIO = 1e-08
EPS_NORM = 1e-06
RATE = 0.02
BF = jnp.bfloat16
F32 = jnp.float32


def moments(projected, first, second):
    first_new = BETA_ONE * first + (1.0 - BETA_ONE) * projected
    second_new = BETA_TWO * second + (1.0 - BETA_TWO) * projected * projected
    ratio = first_new / (jnp.sqrt(second_new) + EPS_RATIO)
    return (first_new, second_new, ratio)


def exchange(
    nz,
    nr,
    x_hbm,
    cq_hbm,
    cv_hbm,
    wq_hbm,
    wv_hbm,
    qf_hbm,
    vf_hbm,
    q1_hbm,
    q2_hbm,
    v1_hbm,
    v2_hbm,
    w_out,
    f_ref,
    ratio_ref,
    proj_out,
    scale_out,
    x_ref,
    cq_ref,
    cv_ref,
    wf_ref,
    wb_ref,
    low_ref,
    part_ref,
    rs_ref,
    z_ref,
    zg_ref,
    zh_ref,
    m1_ref,
    m2_ref,
    sq_ref,
    local_sem,
    f1_s,
    f1_r,
    w1_s,
    w1_r,
    f2_s,
    f2_r,
    w2_s,
    w2_r,
    rs_s,
    rs_r,
    zs_s,
    zs_r,
    zg_s,
    zg_r,
    ag_s,
    ag_r,
    tp_s,
    tp_r,
):
    z = lax.axis_index("fs")
    r = lax.axis_index("rep")
    t = lax.axis_index("tp")
    rows = qf_hbm.shape[0]
    part = rows // nr
    qc = cq_ref.shape[1]
    cols = w_out.shape[1]
    half = cols // 2
    width = w_out.shape[0]
    rank = low_ref.shape[2]
    own = rank // nr
    tokens = x_ref.shape[0]
    z_of = [lax.rem(z + k, nz) for k in range(nz)]
    z_from = [lax.rem(z + nz - k, nz) for k in range(nz)]
    r_of = [lax.rem(r + j, nr) for j in range(nr)]
    side = r + 1 - 2 * lax.rem(r, 2)
    over = lax.rem(r + 2, nr)
    corner = nr - 1 - r
    other = 1 - t

    def remote(src, dst, ss, rs, dev):
        return pltpu.make_async_remote_copy(
            src_ref=src,
            dst_ref=dst,
            send_sem=ss,
            recv_sem=rs,
            device_id=dev,
            device_id_type=pl.DeviceIdType.MESH,
        )

    def slab(zz, rr):
        return pl.ds(pl.multiple_of(zz * rows + rr * part, part), part)

    def fac_copy(src):
        return pltpu.make_async_copy(
            src,
            f_ref.at[t, pl.ds(pl.multiple_of(z * rows, rows), rows)],
            local_sem.at[0],
        )

    @pl.when(t == 0)
    def _():
        fac_copy(qf_hbm).start()

    @pl.when(t == 1)
    def _():
        fac_copy(vf_hbm).start()

    wq_in = pltpu.make_async_copy(wq_hbm, wf_ref.at[:, pl.ds(0, qc)], local_sem.at[1])
    wv_in = pltpu.make_async_copy(wv_hbm, wf_ref.at[:, pl.ds(qc, cols - qc)], local_sem.at[2])
    x_in = pltpu.make_async_copy(x_hbm, x_ref, local_sem.at[3])
    cq_in = pltpu.make_async_copy(cq_hbm, cq_ref, local_sem.at[4])
    cv_in = pltpu.make_async_copy(cv_hbm, cv_ref, local_sem.at[5])
    left, right = pl.ds(0, qc), pl.ds(qc, cols - qc)
    mom = [
        pltpu.make_async_copy(src, dst.at[:, at], local_sem.at[7 + n])
        for n, (src, dst, at) in enumerate(
            (
                (q1_hbm, m1_ref, left),
                (v1_hbm, m1_ref, right),
                (q2_hbm, m2_ref, left),
                (v2_hbm, m2_ref, right),
            )
        )
    ]
    for c in [wq_in, wv_in, x_in, cq_in, cv_in] + mom:
        c.start()

    barrier = pltpu.get_barrier_semaphore()
    peers = [(z_of[k], r, t) for k in range(1, nz)]
    peers += [(z, r_of[j], t) for j in range(1, nr)]
    peers += [(z, r, other)]
    for dev in peers:
        pl.semaphore_signal(
            barrier, inc=1, device_id=dev, device_id_type=pl.DeviceIdType.MESH
        )
    pl.semaphore_wait(barrier, len(peers))

    fac_copy(qf_hbm).wait()
    sends = []
    f1 = []
    for k in range(1, nz):
        here = f_ref.at[t, slab(z, r)]
        c = remote(here, here, f1_s.at[k - 1], f1_r.at[k - 1], (z_of[k], r, t))
        c.start()
        f1.append(c)
    wq_in.wait()
    wv_in.wait()
    wb_ref[...] = wf_ref[...].astype(BF)
    order = sorted(range(1, nz), key=lambda k: min(k, nz - k))
    w1 = {}
    for k in order:
        c = remote(
            wb_ref.at[pl.ds(pl.multiple_of(r * part, part), part)],
            w_out.at[slab(z, r)],
            w1_s.at[k - 1],
            w1_r.at[k - 1],
            (z_of[k], r, t),
        )
        c.start()
        w1[k] = c
    w_own = pltpu.make_async_copy(
        wb_ref, w_out.at[pl.ds(pl.multiple_of(z * rows, rows), rows)], local_sem.at[6]
    )
    w_own.start()

    f2 = []
    for k in range(1, nz):
        f1[k - 1].wait_recv()
        there = f_ref.at[t, slab(z_from[k], r)]
        for j in range(1, nr):
            n = (k - 1) * (nr - 1) + j - 1
            c = remote(there, there, f2_s.at[n], f2_r.at[n], (z, r_of[j], t))
            c.start()
            f2.append(c)
    for c in f2:
        c.wait_recv()
    w2 = {}

    def spread(k):
        w1[k].wait_recv()
        there = w_out.at[slab(z_from[k], r)]
        for n, dev in ((0, side), (1, over)):
            c = remote(there, there, w2_s.at[k - 1, n], w2_r.at[k - 1, n], (z, dev, t))
            c.start()
            w2[k, n] = c

    def relay(k):
        for n, src, dev, at in ((0, side, over, 0), (1, over, side, half)):
            w2[k, n].wait_recv()
            there = w_out.at[slab(z_from[k], src), pl.ds(at, half)]
            c = remote(
                there, there, w2_s.at[k - 1, 2 + n], w2_r.at[k - 1, 2 + n], (z, dev, t)
            )
            c.start()
            w2[k, 2 + n] = c

    stages = [[], [], []]
    for n, k in enumerate(order):
        stages[min(n, 2)].append(k)
    x_in.wait()
    tile = tokens // 3

    @pl.loop(0, 3)
    def _(i):
        span = pl.ds(pl.multiple_of(i * tile, tile), tile)
        low_ref[t, span] = jnp.dot(
            x_ref[span, :], f_ref[t], preferred_element_type=F32
        ).astype(BF)

    lx = remote(low_ref.at[t], low_ref.at[t], tp_s.at[1], tp_r.at[1], (z, r, other))
    lx.start()
    fx = remote(f_ref.at[t], f_ref.at[t], tp_s.at[0], tp_r.at[0], (z, r, other))
    fx.start()
    for k in stages[0]:
        spread(k)
    cq_in.wait()
    cv_in.wait()
    lx.wait_recv()
    dims = (((0,), (0,)), ((), ()))
    part_ref[:, :qc] = lax.dot_general(
        low_ref[0], cq_ref[...], dims, preferred_element_type=F32
    ).astype(BF)
    part_ref[:, qc:] = lax.dot_general(
        low_ref[1], cv_ref[...], dims, preferred_element_type=F32
    ).astype(BF)

    def low_rows(rr):
        return pl.ds(pl.multiple_of(rr * own, own), own)

    rsc = []
    for j in range(1, nr):
        c = remote(
            part_ref.at[low_rows(r_of[j])],
            rs_ref.at[j - 1],
            rs_s.at[j - 1],
            rs_r.at[j - 1],
            (z, r_of[j], t),
        )
        c.start()
        rsc.append(c)

    for k in stages[0]:
        relay(k)
    for c in rsc:
        c.wait_recv()
    total = part_ref[low_rows(r), :].astype(F32)
    for j in range(1, nr):
        total = total + rs_ref[j - 1].astype(F32)
    share = own // nz
    scatter = share % 16 == 0
    zc = []
    if scatter:
        zg_ref[...] = total.astype(BF)
    else:
        z_ref[z] = total.astype(BF)

    def z_rows(zz):
        return pl.ds(pl.multiple_of(zz * share, share), share)

    for k in range(1, nz):
        src = zg_ref.at[z_rows(z_of[k])] if scatter else z_ref.at[z]
        c = remote(src, z_ref.at[z], zs_s.at[k - 1], zs_r.at[k - 1], (z_of[k], r, t))
        c.start()
        zc.append(c)
    if scatter:
        z_ref[z] = zg_ref[z_rows(z), :]
    for k in stages[1]:
        spread(k)
    for c in zc:
        c.wait_recv()
    proj = z_ref[0].astype(F32)
    for k in range(1, nz):
        proj = proj + z_ref[k].astype(F32)
    gc = []
    if scatter:
        for c in zc:
            c.wait_send()
        zh = zh_ref
        zh[z_rows(z), :] = proj.astype(BF)
        for k in range(1, nz):
            here = zh.at[z_rows(z)]
            c = remote(here, here, zg_s.at[k - 1], zg_r.at[k - 1], (z_of[k], r, t))
            c.start()
            gc.append(c)
    for k in stages[1]:
        relay(k)
    for k in stages[2]:
        spread(k)
    for c in mom:
        c.wait()
    if scatter:
        for c in gc:
            c.wait_recv()
        proj = zh[...].astype(F32)
    proj_out[...] = proj
    _, _, ratio = moments(proj, m1_ref[...], m2_ref[...])
    ratio_ref[low_rows(r), :] = ratio.astype(BF)
    agc = []
    for j in range(1, nr):
        here = ratio_ref.at[low_rows(r)]
        c = remote(here, here, ag_s.at[j - 1], ag_r.at[j - 1], (z, r_of[j], t))
        c.start()
        agc.append(c)
    for k in stages[2]:
        relay(k)
    fx.wait_recv()
    for c in agc:
        c.wait_recv()
    step = min(256, width)

    def squares(i, acc):
        span = pl.ds(pl.multiple_of(i * step, step), step)
        a = jnp.dot(f_ref[0, span], ratio_ref[:, :qc], preferred_element_type=F32)
        b = jnp.dot(f_ref[1, span], ratio_ref[:, qc:], preferred_element_type=F32)
        a = jnp.sum(a * a, axis=0, keepdims=True)
        b = jnp.sum(b * b, axis=0, keepdims=True)
        return (acc[0] + a, acc[1] + b)

    qs, vs = lax.fori_loop(
        0,
        width // step,
        squares,
        (jnp.zeros((1, qc), F32), jnp.zeros((1, cols - qc), F32)),
    )
    qs = jnp.sum(qs, axis=1, keepdims=True)
    vs = jnp.sum(vs, axis=1, keepdims=True)
    row = lax.broadcasted_iota(jnp.int32, sq_ref.shape[1:], 0)
    sq_ref[t] = jnp.where(row == 0, qs / (width * qc * 2), vs / (width * (cols - qc) * 2))
    sx = remote(sq_ref.at[t], sq_ref.at[t], tp_s.at[2], tp_r.at[2], (z, r, other))
    sx.start()
    sx.wait_recv()
    scale_out[...] = lax.rsqrt(sq_ref[0] + sq_ref[1] + EPS_NORM)
    for k in range(1, nz):
        w2[k, 2].wait_recv()
        w2[k, 3].wait_recv()
    for c in f1 + list(w1.values()) + f2 + rsc + ([] if scatter else zc) + gc + agc + [fx, lx, sx] + list(w2.values()):
        c.wait_send()
    w_own.wait()


def run_exchange(nz, nr, x, cq, cv, wq, wv, qf, vf, q1, q2, v1, v2):
    tokens, width = x.shape
    qc = cq.shape[1]
    cols = qc + cv.shape[1]
    rows, rank = qf.shape
    own = rank // nr
    share = own // nz if (own // nz) % 16 == 0 else own
    any_spec = pl.BlockSpec(memory_space=pltpu.HBM)
    vmem = pl.BlockSpec(memory_space=pltpu.VMEM)
    dma = pltpu.SemaphoreType.DMA
    shape = jax.ShapeDtypeStruct
    return pl.pallas_call(
        functools.partial(exchange, nz, nr),
        out_shape=(
            shape((width, cols), BF),
            shape((2, width, rank), BF),
            shape((rank, cols), BF),
            shape((own, cols), F32),
            shape((8, 128), F32),
        ),
        in_specs=[any_spec] * 11,
        out_specs=(any_spec, vmem, vmem, vmem, vmem),
        scratch_shapes=[
            pltpu.VMEM((tokens, width), BF),
            pltpu.VMEM(cq.shape, BF),
            pltpu.VMEM(cv.shape, BF),
            pltpu.VMEM((rows, cols), F32),
            pltpu.VMEM((rows, cols), BF),
            pltpu.VMEM((2, tokens, rank), BF),
            pltpu.VMEM((rank, cols), BF),
            pltpu.VMEM((nr - 1, own, cols), BF),
            pltpu.VMEM((nz, share, cols), BF),
            pltpu.VMEM((own, cols), BF),
            pltpu.VMEM((own, cols), BF),
            pltpu.VMEM((own, cols), F32),
            pltpu.VMEM((own, cols), F32),
            pltpu.VMEM((2, 8, 128), F32),
            dma((11,)),
            dma((nz - 1,)),
            dma((nz - 1,)),
            dma((nz - 1,)),
            dma((nz - 1,)),
            dma(((nz - 1) * (nr - 1),)),
            dma(((nz - 1) * (nr - 1),)),
            dma((nz - 1, 4)),
            dma((nz - 1, 4)),
            dma((nr - 1,)),
            dma((nr - 1,)),
            dma((nz - 1,)),
            dma((nz - 1,)),
            dma((nz - 1,)),
            dma((nz - 1,)),
            dma((nr - 1,)),
            dma((nr - 1,)),
            dma((3,)),
            dma((3,)),
        ],
        compiler_params=pltpu.CompilerParams(
            collective_id=0, has_side_effects=True, vmem_limit_bytes=60 * 1024 * 1024
        ),
    )(x, cq, cv, wq, wv, qf, vf, q1, q2, v1, v2)


def finish(
    f_ref,
    ratio_ref,
    scale_ref,
    w_ref,
    wq_ref,
    wv_ref,
    qf_ref,
    vf_ref,
    proj_ref,
    q1_ref,
    q2_ref,
    v1_ref,
    v2_ref,
    qd_out,
    vd_out,
    qm_out,
    vm_out,
    q1_out,
    q2_out,
    v1_out,
    v2_out,
    qcopy_out,
    vcopy_out,
):
    qc = wq_ref.shape[1]
    sets = (
        (0, pl.ds(0, qc), wq_ref, qf_ref, q1_ref, q2_ref, qd_out, qm_out, q1_out, q2_out, qcopy_out),
        (
            1,
            pl.ds(qc, wv_ref.shape[1]),
            wv_ref,
            vf_ref,
            v1_ref,
            v2_ref,
            vd_out,
            vm_out,
            v1_out,
            v2_out,
            vcopy_out,
        ),
    )
    for n, at, w, f, m1, m2, d_out, m_out, m1_out, m2_out, c_out in sets:
        scale = scale_ref[n : n + 1, 0:1]
        ratio = ratio_ref[:, at]
        raw = jnp.dot(f_ref[n], ratio, preferred_element_type=F32)
        c_out[...] = (w_ref[:, at].astype(F32) - RATE * (raw * scale)).astype(BF)
        d = jnp.dot(f[...], ratio, preferred_element_type=F32) * scale
        d_out[...] = d
        m_out[...] = w[...] - RATE * d
        m1_out[...], m2_out[...], _ = moments(proj_ref[:, at], m1[...], m2[...])


def run_finish(factors, ratio, scale, weights, wq, wv, qf, vf, proj, q1, q2, v1, v2):
    rows, qc = wq.shape
    vc = wv.shape[1]
    width, cols = weights.shape
    rank, own = qf.shape[1], q1.shape[0]
    steps = 8 if rows % 128 == 0 else 4

    def tall(n, c):
        return pl.BlockSpec((n // steps, c), lambda i: (i, 0))

    def whole(a):
        return pl.BlockSpec(a.shape, lambda i: (0,) * a.ndim)

    shape = jax.ShapeDtypeStruct
    return pl.pallas_call(
        finish,
        grid=(steps,),
        in_specs=[
            pl.BlockSpec((2, width // steps, rank), lambda i: (0, i, 0)),
            whole(ratio),
            whole(scale),
            tall(width, cols),
            tall(rows, qc),
            tall(rows, vc),
            tall(rows, rank),
            tall(rows, rank),
            tall(own, cols),
            tall(own, qc),
            tall(own, qc),
            tall(own, vc),
            tall(own, vc),
        ],
        out_specs=[
            tall(rows, qc),
            tall(rows, vc),
            tall(rows, qc),
            tall(rows, vc),
            tall(own, qc),
            tall(own, qc),
            tall(own, vc),
            tall(own, vc),
            tall(width, qc),
            tall(width, vc),
        ],
        out_shape=[
            shape((rows, qc), F32),
            shape((rows, vc), F32),
            shape((rows, qc), F32),
            shape((rows, vc), F32),
            shape((own, qc), F32),
            shape((own, qc), F32),
            shape((own, vc), F32),
            shape((own, vc), F32),
            shape((width, qc), BF),
            shape((width, vc), BF),
        ],
        compiler_params=pltpu.CompilerParams(vmem_limit_bytes=60 * 1024 * 1024),
    )(factors, ratio, scale, weights, wq, wv, qf, vf, proj, q1, q2, v1, v2)


def line_exchange(
    quarter,
    chunks,
    rests,
    x_hbm,
    cq_hbm,
    cv_hbm,
    wq_hbm,
    wv_hbm,
    qf_hbm,
    vf_hbm,
    q1_hbm,
    q2_hbm,
    v1_hbm,
    v2_hbm,
    w_ref,
    f_ref,
    ratio_ref,
    wf_ref,
    m1_out,
    m2_out,
    scale_out,
    d_ref,
    x_ref,
    cq_ref,
    cv_ref,
    acc_ref,
    low_ref,
    part_ref,
    ra_ref,
    tb_ref,
    rb_ref,
    zs_ref,
    zo_ref,
    z_ref,
    zh_ref,
    m1_ref,
    m2_ref,
    g_ref,
    sq_ref,
    local_sem,
    out_s,
    fz_r,
    fp_r,
    wz_r,
    wp_r,
    wc_r,
    ra_r,
    rb_r,
    zs_r,
    zg_r,
    ag_r,
    ac_r,
    tp_s,
    tp_r,
):
    z = lax.axis_index("fs")
    r = lax.axis_index("rep")
    t = lax.axis_index("tp")
    nz, nr = 4, 4
    rows = qf_hbm.shape[0]
    part = rows // nr
    qc = cq_ref.shape[1]
    width, cols = w_ref.shape
    half = cols // 2
    rank = low_ref.shape[2]
    own = rank // nr
    share = own // nz
    tokens = x_ref.shape[0]
    px, py = lax.rem(r, 2), lax.div(r, 2)
    side = r + 1 - 2 * px
    over = lax.rem(r + 2, nr)
    corner = nr - 1 - r
    other = 1 - t
    upper = lax.div(z, 2)
    near = z + 1 - 2 * lax.rem(z, 2)
    mid = 2 - upper
    far = 3 - 3 * upper
    planes = [near, mid, far]
    inner = jnp.logical_and(z > 0, z < nz - 1)
    groups = {"plane": 0, "line": 1, "inner": 2}
    sent = dict.fromkeys(groups, 0)

    def remote(src, dst, ss, rs, dev):
        return pltpu.make_async_remote_copy(
            src_ref=src,
            dst_ref=dst,
            send_sem=ss,
            recv_sem=rs,
            device_id=dev,
            device_id_type=pl.DeviceIdType.MESH,
        )

    def count(ref, group):
        sent[group] += ref.size * ref.dtype.itemsize

    def send(src, dst, rs, dev, group="plane"):
        count(dst, group)
        remote(src, dst, out_s.at[groups[group]], rs, dev).start()

    def send_pair(src, dst, n):
        remote(src, dst, tp_s.at[n], tp_r.at[n], (z, r, other)).start()

    def send_inner(ref, rs, dev, wait=None):
        count(ref, "inner")

        @pl.when(inner)
        def _():
            if wait is not None:
                arrive(ref, wait)
            remote(ref, ref, out_s.at[2], rs, dev).start()

    def drain(group):
        size, line = sent[group], cols * 2
        while size:
            span = pl.ds(0, min(size // line, width))
            size -= min(size // line, width) * line
            ref = w_ref.at[span]
            remote(ref, ref, out_s.at[groups[group]], tp_r.at[0], (z, r, other)).wait_send()

    def arrive(dst, rs):
        remote(dst, dst, tp_s.at[0], rs, (z, r, other)).wait_recv()

    def at(start, size, step):
        return pl.ds(pl.multiple_of(start, step), size)

    def fac_copy(src):
        return pltpu.make_async_copy(src, f_ref.at[t, at(z * rows, rows, rows)], local_sem.at[0])

    @pl.when(t == 0)
    def _():
        fac_copy(qf_hbm).start()

    @pl.when(t == 1)
    def _():
        fac_copy(vf_hbm).start()

    left, right = pl.ds(0, qc), pl.ds(qc, cols - qc)
    x_in = pltpu.make_async_copy(x_hbm, x_ref, local_sem.at[1])
    cq_in = pltpu.make_async_copy(cq_hbm, cq_ref, local_sem.at[2])
    cv_in = pltpu.make_async_copy(cv_hbm, cv_ref, local_sem.at[3])
    pltpu.make_async_copy(wq_hbm, wf_ref.at[:, left], local_sem.at[4]).start()
    pltpu.make_async_copy(wv_hbm, wf_ref.at[:, right], local_sem.at[4]).start()
    for c in (x_in, cq_in, cv_in):
        c.start()
    for n, src, dst, span in (
        (5, q1_hbm, m1_ref, left),
        (5, v1_hbm, m1_ref, right),
        (6, q2_hbm, m2_ref, left),
        (6, v2_hbm, m2_ref, right),
    ):
        pltpu.make_async_copy(src, dst.at[:, span], local_sem.at[n]).start()

    def loaded(ref, n):
        pltpu.make_async_copy(ref, ref, local_sem.at[n]).wait()

    barrier = pltpu.get_barrier_semaphore()
    peers = [(p, r, t) for p in planes]
    peers += [(z, p, t) for p in (side, over, corner)]
    peers += [(z, r, other)]
    for dev in peers:
        pl.semaphore_signal(
            barrier, inc=1, device_id=dev, device_id_type=pl.DeviceIdType.MESH
        )
    pl.semaphore_wait(barrier, len(peers))

    class Spread:
        def __init__(self, view, split, both, rs, rest):
            self.view, self.split, self.both, self.rs, self.rest = view, split, both, rs, rest

        def start(self):
            here = self.view(r)
            for dev in (side, over):
                send(here, here, self.rs, (z, dev, t))

        def relay(self):
            arrive(self.both, self.rs)
            for n, src, dev in ((0, side, over), (1, over, side)):
                there = self.split(self.view(src), n)
                send(there, there, self.rest, (z, dev, t))

    def halves(ref, n):
        return ref.at[:, pl.ds(n * half, half)]

    def fac_rows(plane, rr):
        return f_ref.at[t, at(plane * rows + rr * part, part, part)]

    fac_copy(qf_hbm).wait()
    for i, p in enumerate(planes):
        here = fac_rows(z, r)
        send(here, here, fz_r.at[z], (p, r, t), "line")

    spans = [(n, s, True) for n, s in zip([sum(chunks[:c]) for c in range(len(chunks))], chunks)]
    spans += [(n, s, False) for n, s in zip([sum(rests[:c]) for c in range(len(rests))], rests)]

    def w_rows(plane, rr, c):
        begin, size, split = spans[c]
        begin = plane * rows + begin + (rr * quarter if split else nr * quarter)
        return w_ref.at[at(begin, size, 8)]

    def w_own(c):
        here = w_rows(z, r, c)
        send(here, here, wz_r.at[0, c], (near, r, t), "line")
        send_inner(here, wz_r.at[1, c], (mid, r, t))

    def w_pass(i, c):
        to, sem = (near, wz_r.at[i, c]) if i else (mid, wz_r.at[2, c])
        send_inner(w_rows(planes[i], r, c), sem, (to, r, t), wz_r.at[i, c])

    def w_land(i, c):
        @pl.when(jnp.logical_not(inner))
        def _():
            arrive(w_rows(planes[i], r, c), wz_r.at[i, c])

    def w_start(i, c):
        w_land(i, c)
        w_in[i][c].start()

    w_in = [
        [
            Spread(functools.partial(lambda p, c, rr: w_rows(p, rr, c), p, c), halves, w_ref.at[pl.ds(0, 2 * chunks[c])], wp_r.at[i, c], wc_r.at[i])
            for c in range(len(chunks))
        ]
        for i, p in enumerate(planes)
    ]

    def low_add(plane, first):
        a = jnp.dot(
            x_ref[:, at(plane * rows, rows, rows)],
            f_ref[t, at(plane * rows, rows, rows)],
            preferred_element_type=F32,
        )
        acc_ref[...] = a if first else acc_ref[...] + a

    fac = [
        Spread(
            functools.partial(fac_rows, p),
            lambda ref, n: ref.at[pl.ds(n * (part // 2), part // 2)],
            f_ref.at[t, pl.ds(0, 2 * part)],
            fp_r.at[i, 0],
            fp_r.at[i, 1],
        )
        for i, p in enumerate(planes)
    ]

    def fac_start(i):
        arrive(fac_rows(planes[i], r), fz_r.at[planes[i]])
        fac[i].start()

    def fac_finish(i):
        arrive(fac_rows(planes[i], corner), fp_r.at[i, 1])
        low_add(planes[i], False)

    def share_rows(plane):
        return at(plane * share, share, share)

    def low_rows(rr, plane):
        return at(rr * own + plane * share, share, share)

    lo, hi = pl.ds(0, half), pl.ds(half, half)
    order = [far, mid, near, z]

    def sum_start(i):
        span = share_rows(order[i])
        for n, src, dev in (
            (0, part_ref.at[:, 1 - px, span, lo], side),
            (1, part_ref.at[1 - py, :, span, hi], over),
        ):
            send(src, ra_ref.at[n, :, span], ra_r.at[i], (z, dev, t))

    def sum_relay(i):
        span = share_rows(order[i])
        arrive(ra_ref.at[:, :, span], ra_r.at[i])
        for n, mine, theirs, dev in (
            (0, part_ref[1 - py, px, span, lo], ra_ref[0, 1 - py, span, :], over),
            (1, part_ref[py, 1 - px, span, hi], ra_ref[1, 1 - px, span, :], side),
        ):
            tb_ref[n, span, :] = (mine.astype(F32) + theirs.astype(F32)).astype(BF)
            send(tb_ref.at[n, span], rb_ref.at[n, span], rb_r.at[i], (z, dev, t))

    def sum_finish(i):
        span = share_rows(order[i])
        arrive(rb_ref.at[:, span], rb_r.at[i])
        out = []
        for n, cut, theirs in ((0, lo, ra_ref[0, py, span, :]), (1, hi, ra_ref[1, px, span, :])):
            a = part_ref[py, px, span, cut].astype(F32) + theirs.astype(F32)
            out.append(a + rb_ref[n, span, :].astype(F32))
        if i == 3:
            zo_ref[:, lo], zo_ref[:, hi] = out
        else:
            zs_ref[span, lo] = out[0].astype(BF)
            zs_ref[span, hi] = out[1].astype(BF)
            send(zs_ref.at[span], z_ref.at[z], zs_r.at[z], (order[i], r, t), "line")

    def line_sum():
        proj = zo_ref[...]
        for p in planes:
            arrive(z_ref.at[p], zs_r.at[p])
            proj = proj + z_ref[p].astype(F32)
        here = zh_ref.at[share_rows(z)]
        zh_ref[share_rows(z), :] = proj.astype(BF)
        for p in (far, mid, near):
            send(here, here, zg_r.at[z], (p, r, t), "line")

    ratio_in = [
        Spread(
            functools.partial(lambda p, rr: ratio_ref.at[low_rows(rr, p)], p),
            halves,
            ratio_ref.at[pl.ds(0, 2 * share)],
            ag_r.at[i],
            ac_r.at[0],
        )
        for i, p in enumerate([z] + planes)
    ]

    def ratio_start(i):
        p = z
        if i:
            p = planes[i - 1]
            arrive(zh_ref.at[share_rows(p)], zg_r.at[p])
        span = share_rows(p)
        first, second, ratio = moments(
            zh_ref[span, :].astype(F32), m1_ref[span, :], m2_ref[span, :]
        )
        m1_out[span, :] = first
        m2_out[span, :] = second
        ratio_ref[low_rows(r, p), :] = ratio.astype(BF)
        ratio_in[i].start()

    dims = (((0,), (0,)), ((), ()))

    def low_parts():
        for n, c_ref, span in ((0, cq_ref, slice(0, qc)), (1, cv_ref, slice(qc, cols))):
            a = lax.dot_general(
                low_ref[n], c_ref[...], dims, preferred_element_type=F32
            ).astype(BF)
            for k in range(nr):
                part_ref[k // 2, k % 2, :, span] = a[k * own : (k + 1) * own]

    def gram():
        arrive(f_ref.at[other], tp_r.at[0])
        for n in range(2):
            g = lax.dot_general(f_ref[n], f_ref[n], dims, preferred_element_type=F32)
            top = g.astype(BF)
            g_ref[n, 0] = top
            g_ref[n, 1] = (g - top.astype(F32)).astype(BF)

    def squares(n, span):
        ratio = ratio_ref[:, span]
        a = jnp.dot(g_ref[n, 0], ratio, preferred_element_type=F32)
        a = a + jnp.dot(g_ref[n, 1], ratio, preferred_element_type=F32)
        a = jnp.sum(a * ratio.astype(F32), axis=0, keepdims=True)
        return jnp.sum(a, axis=1, keepdims=True)

    def own_rows():
        mine = at(z * rows, rows, rows)
        tile = min(256, qc)

        def columns(n, begin):
            cut = pl.ds(begin, tile)
            d = jnp.dot(f_ref[n, mine], ratio_ref[:, cut], preferred_element_type=F32)
            d = d * scale_out[n : n + 1, 0:1]
            d_ref[:, cut] = d
            wf_ref[:, cut] = wf_ref[:, cut] - RATE * d

        for begin in range(0, cols, tile):
            columns(0 if begin < qc else 1, begin)

    loaded(wf_ref, 4)
    w_ref[at(z * rows, rows, rows), :] = wf_ref[...].astype(BF)
    w_own(2)
    fac_start(0)
    w_own(1)
    x_in.wait()
    low_add(z, True)
    fac_start(1)
    fac_start(2)
    w_own(0)
    fac[0].relay()
    w_pass(1, 2)
    fac[1].relay()
    w_own(4)
    w_pass(0, 2)
    fac[2].relay()
    w_start(0, 2)
    w_own(3)
    fac_finish(0)
    w_pass(0, 1)
    fac_finish(1)
    w_start(0, 1)
    fac_finish(2)
    send_pair(f_ref.at[t], f_ref.at[t], 0)
    low_ref[t] = acc_ref[...].astype(BF)
    send_pair(low_ref.at[t], low_ref.at[t], 1)
    w_own(5)
    w_pass(0, 0)
    w_start(1, 2)
    cq_in.wait()
    cv_in.wait()
    arrive(low_ref.at[other], tp_r.at[1])
    low_parts()
    sum_start(2)
    w_pass(1, 0)
    sum_start(0)
    sum_start(1)
    w_pass(1, 1)
    sum_start(3)
    sum_relay(2)
    sum_relay(0)
    w_start(0, 0)
    w_pass(2, 1)
    w_pass(0, 5)
    sum_relay(3)
    w_in[1][2].relay()
    sum_relay(1)
    sum_finish(2)
    w_pass(2, 0)
    sum_finish(0)
    w_pass(1, 5)
    w_start(1, 0)
    w_in[0][1].relay()
    sum_finish(3)
    w_in[0][0].relay()
    w_start(2, 1)
    sum_finish(1)
    gram()
    w_start(1, 1)
    loaded(m1_ref, 5)
    loaded(m2_ref, 6)
    line_sum()
    ratio_start(0)
    w_pass(0, 4)
    w_pass(2, 5)
    w_pass(2, 2)
    w_pass(1, 3)
    w_in[1][0].relay()
    w_start(2, 0)
    ratio_in[0].relay()
    ratio_start(1)
    w_pass(0, 3)
    ratio_start(3)
    ratio_start(2)
    w_in[2][1].relay()
    w_start(2, 2)
    w_pass(2, 4)
    w_pass(2, 3)
    ratio_in[1].relay()
    ratio_in[2].relay()
    ratio_in[3].relay()
    w_pass(1, 4)
    w_in[0][2].relay()
    w_in[2][2].relay()
    w_in[1][1].relay()
    w_in[2][0].relay()
    arrive(ratio_ref.at[at(corner * own, own, own)], ac_r.at[0])
    qs = squares(0, slice(0, qc)) / (width * qc * 2)
    vs = squares(1, slice(qc, cols)) / (width * (cols - qc) * 2)
    line = lax.broadcasted_iota(jnp.int32, sq_ref.shape[1:], 0)
    sq_ref[t] = jnp.where(line == 0, qs, vs)
    send_pair(sq_ref.at[t], sq_ref.at[t], 2)
    arrive(sq_ref.at[other], tp_r.at[2])
    scale_out[...] = lax.rsqrt(jnp.maximum(sq_ref[0] + sq_ref[1], 0.0) + EPS_NORM)
    own_rows()
    for c in range(len(chunks), len(spans)):
        for i in range(3):
            w_land(i, c)
    for i in range(3):
        arrive(w_ref.at[at(planes[i] * rows + corner * quarter, quarter, 8)], wc_r.at[i])
    for n, ref in enumerate((f_ref.at[t], low_ref.at[t], sq_ref.at[t])):
        remote(ref, ref, tp_s.at[n], tp_r.at[n], (z, r, other)).wait_send()
    drain("plane")
    drain("line")

    @pl.when(inner)
    def _():
        drain("inner")


def run_line_exchange(x, cq, cv, wq, wv, qf, vf, q1, q2, v1, v2):
    tokens, width = x.shape
    qc = cq.shape[1]
    cols = qc + cv.shape[1]
    rows, rank = qf.shape
    own = rank // 4
    share = own // 4
    unit = rows // 64
    quarter = 12 * unit
    chunks = (4 * unit, 4 * unit, 4 * unit)
    rests = (6 * unit, 5 * unit, 5 * unit)
    any_spec = pl.BlockSpec(memory_space=pltpu.HBM)
    vmem = pl.BlockSpec(memory_space=pltpu.VMEM)
    dma = pltpu.SemaphoreType.DMA
    n = len(chunks)
    m = n + len(rests)
    return pl.pallas_call(
        functools.partial(line_exchange, quarter, chunks, rests),
        out_shape=(
            pltpu.VMEM((width, cols), BF),
            pltpu.VMEM((2, width, rank), BF),
            pltpu.VMEM((rank, cols), BF),
            pltpu.VMEM((rows, cols), F32),
            pltpu.VMEM((own, cols), F32),
            pltpu.VMEM((own, cols), F32),
            pltpu.VMEM((8, 128), F32),
            pltpu.VMEM((rows, cols), F32),
        ),
        in_specs=[any_spec] * 11,
        out_specs=(vmem,) * 8,
        scratch_shapes=[
            pltpu.VMEM((tokens, width), BF),
            pltpu.VMEM(cq.shape, BF),
            pltpu.VMEM(cv.shape, BF),
            pltpu.VMEM((tokens, rank), F32),
            pltpu.VMEM((2, tokens, rank), BF),
            pltpu.VMEM((2, 2, own, cols), BF),
            pltpu.VMEM((2, 2, own, cols // 2), BF),
            pltpu.VMEM((2, own, cols // 2), BF),
            pltpu.VMEM((2, own, cols // 2), BF),
            pltpu.VMEM((own, cols), BF),
            pltpu.VMEM((share, cols), F32),
            pltpu.VMEM((4, share, cols), BF),
            pltpu.VMEM((own, cols), BF),
            pltpu.VMEM((own, cols), F32),
            pltpu.VMEM((own, cols), F32),
            pltpu.VMEM((2, 2, rank, rank), BF),
            pltpu.VMEM((2, 8, 128), F32),
            dma((7,)),
            dma((3,)),
            dma((4,)),
            dma((3, 2)),
            dma((3, m)),
            dma((3, n)),
            dma((3,)),
            dma((4,)),
            dma((4,)),
            dma((4,)),
            dma((4,)),
            dma((4,)),
            dma((1,)),
            dma((3,)),
            dma((3,)),
        ],
        compiler_params=pltpu.CompilerParams(
            collective_id=0, has_side_effects=True, vmem_limit_bytes=48 * 1024 * 1024
        ),
    )(x, cq, cv, wq, wv, qf, vf, q1, q2, v1, v2)


def line_finish(
    steps,
    w_ref,
    f_ref,
    ratio_ref,
    m_ref,
    m1_ref,
    m2_ref,
    scale_ref,
    d_ref,
    qd_out,
    vd_out,
    qm_out,
    vm_out,
    q1_out,
    q2_out,
    v1_out,
    v2_out,
    qcopy_out,
    vcopy_out,
    c_ref,
    sem,
):
    width, cols = w_ref.shape
    qc = qd_out.shape[1]
    left, right = pl.ds(0, qc), pl.ds(qc, cols - qc)
    outs = (
        (d_ref, left, qd_out),
        (d_ref, right, vd_out),
        (m_ref, left, qm_out),
        (m_ref, right, vm_out),
        (m1_ref, left, q1_out),
        (m1_ref, right, v1_out),
        (m2_ref, left, q2_out),
        (m2_ref, right, v2_out),
    )
    copies = [
        pltpu.make_async_copy(src.at[:, cut], dst, sem.at[n // 2])
        for n, (src, cut, dst) in enumerate(outs)
    ]
    for c in copies:
        c.start()
    tall = width // steps

    @pl.loop(0, steps)
    def _(i):
        span = pl.ds(pl.multiple_of(i * tall, tall), tall)
        for n, cut, dst in ((0, left, qcopy_out), (1, right, vcopy_out)):
            raw = jnp.dot(f_ref[n, span], ratio_ref[:, cut], preferred_element_type=F32)
            raw = raw * scale_ref[n : n + 1, 0:1]
            c_ref[span, cut] = (w_ref[span, cut].astype(F32) - RATE * raw).astype(BF)
            pltpu.make_async_copy(c_ref.at[span, cut], dst.at[span], sem.at[4]).start()

    for n, ref in enumerate((d_ref, m_ref, m1_ref, m2_ref, c_ref)):
        pltpu.make_async_copy(ref, ref, sem.at[n]).wait()


def run_line_finish(weights, factors, ratio, masters, m1, m2, scale, directions, qc):
    rows, cols = masters.shape
    vc = cols - qc
    width, own = weights.shape[0], m1.shape[0]
    vmem = pl.BlockSpec(memory_space=pltpu.VMEM)
    shape = jax.ShapeDtypeStruct
    return pl.pallas_call(
        functools.partial(line_finish, 8),
        in_specs=[vmem] * 8,
        out_specs=[pl.BlockSpec(memory_space=pltpu.HBM)] * 10,
        out_shape=[
            shape((rows, qc), F32),
            shape((rows, vc), F32),
            shape((rows, qc), F32),
            shape((rows, vc), F32),
            shape((own, qc), F32),
            shape((own, qc), F32),
            shape((own, vc), F32),
            shape((own, vc), F32),
            shape((width, qc), BF),
            shape((width, vc), BF),
        ],
        scratch_shapes=[pltpu.VMEM((width, cols), BF), pltpu.SemaphoreType.DMA((5,))],
        compiler_params=pltpu.CompilerParams(vmem_limit_bytes=16 * 1024 * 1024),
    )(weights, factors, ratio, masters, m1, m2, scale, directions)


def suits_line(nz, nr, qf, cq, cv):
    rows, rank = qf.shape
    cols = cq.shape[1] + cv.shape[1]
    return nz == 4 and nr == 4 and rows % 512 == 0 and rank % 256 == 0 and cols % 256 == 0


def local(nz, nr, *args):
    _, cq, cv, wq, wv, qf, vf, q1, q2, v1, v2 = args
    if suits_line(nz, nr, qf, cq, cv):
        return tuple(run_line_finish(*run_line_exchange(*args), cq.shape[1]))
    weights, factors, ratio, proj, scale = run_exchange(nz, nr, *args)
    return tuple(
        run_finish(factors, ratio, scale, weights, wq, wv, qf, vf, proj, q1, q2, v1, v2)
    )


def solution(mesh):
    return jax.shard_map(
        functools.partial(local, mesh.shape["fs"], mesh.shape["rep"]),
        mesh=mesh,
        in_specs=(
            P(("fs", "rep"), None),
            P(("fs", "rep"), "tp"),
            P(("fs", "rep"), "tp"),
            P("fs", "tp"),
            P("fs", "tp"),
            P("fs", None),
            P("fs", None),
            P("rep", "tp"),
            P("rep", "tp"),
            P("rep", "tp"),
            P("rep", "tp"),
        ),
        out_specs=(
            P("fs", "tp"),
            P("fs", "tp"),
            P("fs", "tp"),
            P("fs", "tp"),
            P("rep", "tp"),
            P("rep", "tp"),
            P("rep", "tp"),
            P("rep", "tp"),
            P(None, "tp"),
            P(None, "tp"),
        ),
        check_vma=False,
    )
```
